32 devices in a mesh: sp: 8 (over z, x), tp: 4 (over y, core).
Axes of the slice: x: 2, y: 2, z: 4, core: 2. Of those that a mesh axis runs over, the one named last changes fastest.
Arguments:
- x_in: bfloat16 [4096, 1024], P('sp', 'tp'), may hold values from -6 to 6
- gate_b: bfloat16 [4096, 1024], P('sp', 'tp'), may hold values from -6 to 6
- gate_c: bfloat16 [4096, 1024], P('sp', 'tp'), may hold values from -6 to 6
- conv_taps: bfloat16 [3, 1024], P(None, 'tp'), may hold values from -3.5 to 3.5
- out_proj: bfloat16 [1024, 2048], P('tp'), may hold values from -0.1875 to 0.1875
- mix_gain: bfloat16 [2048], replicated, may hold values from 0.099609375 to 1.8984375
- resid: bfloat16 [4096, 2048], P(('sp', 'tp')), may hold values from -6 to 6
- pre_gain: bfloat16 [2048], replicated, may hold values from 0.099609375 to 1.8984375
- expert_gate: bfloat16 [8, 2048, 512], P('sp'), may hold values from -0.125 to 0.125
- expert_up: bfloat16 [8, 2048, 512], P('sp'), may hold values from -0.125 to 0.125
- expert_down: bfloat16 [8, 512, 2048], P('sp'), may hold values from -7.1594562 to 7.1594562
- shared_gate: bfloat16 [2048, 256], replicated, may hold values from -0.125 to 0.125
- shared_up: bfloat16 [2048, 256], replicated, may hold values from -0.125 to 0.125
- shared_down: bfloat16 [256, 2048], replicated, may hold values from -10.125 to 10.125
- post_gain: bfloat16 [2048], replicated, may hold values from 0.099609375 to 1.8984375
- routes: int32 [4096, 4], P(('sp', 'tp')), may hold values from 0 to 7, all different within a row; in each aligned block of 128 rows (0 to 127, 128 to 255, ...) at most 96 rows name the same one
- route_weights: float32 [4096, 4], P(('sp', 'tp')), may hold values from 0.1 to 1
Outputs:
- layer_out: bfloat16 [4096, 2048], P(('sp', 'tp'))
The draws below stay inside these ranges and needn't reach their ends.
Inputs may be any that keep to these rules, and one draw needn't show every extreme that they name: `routes`: each row names 4 different experts. Within the rows of one device (aligned blocks), no expert is named by more than 96 rows, and in some block one expert is named by exactly 96 rows.
All inputs are finite; a program needn't handle non-finite values.
Results may differ from the reference program's by a relative error of at most 0.007.
Values may be sent and summed in bfloat16 or wider, within the bound.
A program may use at most 128 MiB of HBM per device.

```python
import math
import jax
import jax.numpy as jnp
import numpy as np
from jax import lax

D = 2048
CONV_CH = 1024
EXPERT_HIDDEN = 512
SHARED_HIDDEN = 256
CONV_WIDTH = 3
TOPK = 4
TOK_DEV = 512
EXPERTS = 8
CAP = 96
TOKENS = 4096
N_SP = 8
N_TP = 4


def column_scale(key, count):
    ramp = 3.0 ** (jnp.arange(count, dtype=jnp.float32) / count)
    rough = 10.0 ** jax.random.uniform(key, (count,), jnp.float32)
    return ramp * rough / 10.0


def draw_expert_down(key, part):
    first, second = jax.random.split(key)
    base = jnp.clip(jax.random.normal(first, (EXPERTS, EXPERT_HIDDEN, D), jnp.float32), -6.0, 6.0)
    return (base * EXPERT_HIDDEN ** (-0.5) * column_scale(second, D)[None, None, :]).astype(jnp.bfloat16)


def draw_shared_down(key, part):
    first, second = jax.random.split(key)
    base = jnp.clip(jax.random.normal(first, (SHARED_HIDDEN, D), jnp.float32), -6.0, 6.0)
    return (base * SHARED_HIDDEN ** (-0.5) * column_scale(second, D)[None, :]).astype(jnp.bfloat16)


def levels(rng, dims, shards, low, top_value):
    gain, own = 1.0, jax.random.fold_in(rng, 6)
    for dim, blocks in shards:
        steps = jnp.exp(jax.random.uniform(jax.random.fold_in(own, dim), (blocks,), jnp.float32, low / len(shards), top_value / len(shards)))
        gain = gain * jnp.repeat(steps, dims[dim] // blocks).reshape([-1 if axis == dim else 1 for axis in range(len(dims))])
    return gain


def assign_block(stream_key, own, number, rows, number_of, top, most, skew):
    order = jax.random.permutation(stream_key, number_of)
    packed, common = load_shares(number_of, rows * top, most, skew, True), load_shares(number_of, rows * top, most, skew, False)
    places = jnp.arange(number_of)

    def named(tallies, rotation):
        used = int((tallies > 0).sum())
        fixed = max(1, used // 4)
        moved = fixed + (places - fixed + rotation * (used - fixed)) % max(1, number_of - fixed)
        return jnp.zeros((number_of,), jnp.int32).at[order[jnp.where(places < fixed, places, moved)]].set(jnp.asarray(tallies, jnp.int32))

    tallies = jnp.where(number % 4 == 0, named(packed, number // 4), named(common, number - number // 4 - 1))
    mixed = jax.random.permutation(jax.random.fold_in(own, 3), number_of)
    giver, sink = mixed[0:number_of // 2 * 2:2], mixed[1:number_of // 2 * 2:2]
    margin = jnp.minimum(tallies[giver] - 1, most - tallies[sink]) // 2
    margin = jnp.where((giver == order[0]) | (sink == order[0]) | (tallies[sink] == 0), 0, jnp.maximum(margin, 0))
    moved = jax.random.randint(jax.random.fold_in(own, 4), (number_of // 2,), 0, 1 << 20) % (margin + 1)
    tallies = tallies.at[giver].add(-moved).at[sink].add(moved)
    members = jnp.searchsorted(jnp.cumsum(tallies), jnp.arange(rows * top), side="right").astype(jnp.int32)
    table = members.reshape(top, rows).T
    table = table[jax.random.permutation(jax.random.fold_in(own, 1), rows)]
    rotation = jax.random.randint(jax.random.fold_in(own, 2), (rows, 1), 0, top)
    return jnp.take_along_axis(table, (jnp.arange(top)[None, :] + rotation) % top, axis=1)


def load_shares(count, total, bound, lean, full):
    loads = [(1 << 20) // math.isqrt(grade ** lean) + 1 for grade in range(1, count + 1)]
    largest = bound if full else min(bound, max(-(-total // count), total * loads[0] // sum(loads)))
    least = 1 if total - largest >= count - 1 else 0
    holding, rest = [largest] + [least] * (count - 1), total - largest - least * (count - 1)
    while rest > 0:
        free = [i for i in range(1, count) if holding[i] < largest] or [i for i in range(1, count) if holding[i] < bound]
        whole, budget = sum([loads[i] for i in free]), rest
        for i in free:
            addition = min(bound - holding[i], max(1, budget * loads[i] // whole), rest)
            holding[i] = holding[i] + addition
            rest = rest - addition
    return np.array(holding)


def centred(own_key, extent, spread, most, pieces=(), kind=jnp.bfloat16):
    level = levels(own_key, extent, pieces, -0.22, 0.18) if pieces else 1.0
    array = jax.random.normal(own_key, extent, jnp.float32) * spread * level
    return jnp.minimum(jnp.maximum(array, -most), most).astype(kind)


def setup_inputs(seed: int = 0) -> dict:
    arg_keys = jax.random.split(jax.random.key(seed), 18)
    x_in = centred(arg_keys[0], (TOKENS, CONV_CH), 1.0, 6.0, ((0, 8), (1, 4)))
    gate_b = centred(arg_keys[1], (TOKENS, CONV_CH), 1.0, 6.0, ((0, 8), (1, 4)))
    gate_c = centred(arg_keys[2], (TOKENS, CONV_CH), 1.0, 6.0, ((0, 8), (1, 4)))
    conv_taps = centred(arg_keys[3], (CONV_WIDTH, CONV_CH), CONV_WIDTH ** -0.5, 3.5, ((1, 4),))
    out_proj = centred(arg_keys[4], (CONV_CH, D), CONV_CH ** -0.5, 0.1875, ((0, 4),))
    mix_gain = jnp.clip(1.0 + 0.18 * jax.random.normal(arg_keys[5], (D,), jnp.float32), 0.099609375, 1.8984375).astype(jnp.bfloat16)
    resid = centred(arg_keys[6], (TOKENS, D), 1.0, 6.0, ((0, 32),))
    pre_gain = jnp.clip(1.0 + 0.18 * jax.random.normal(arg_keys[7], (D,), jnp.float32), 0.099609375, 1.8984375).astype(jnp.bfloat16)
    expert_gate = centred(arg_keys[8], (EXPERTS, D, EXPERT_HIDDEN), D ** -0.5, 0.125, ((0, 8),))
    expert_up = centred(arg_keys[9], (EXPERTS, D, EXPERT_HIDDEN), D ** -0.5, 0.125, ((0, 8),))
    expert_down = draw_expert_down(jax.random.fold_in(arg_keys[17], 71), 0)
    shared_gate = centred(arg_keys[11], (D, SHARED_HIDDEN), D ** -0.5, 0.125)
    shared_up = centred(arg_keys[12], (D, SHARED_HIDDEN), D ** -0.5, 0.125)
    shared_down = draw_shared_down(jax.random.fold_in(arg_keys[17], 71), 0)
    post_gain = jnp.clip(1.0 + 0.18 * jax.random.normal(arg_keys[14], (D,), jnp.float32), 0.099609375, 1.8984375).astype(jnp.bfloat16)
    routes_keys = jax.random.split(jax.random.fold_in(arg_keys[15], 1), TOKENS // (TOK_DEV // N_TP))
    routes_turns = jax.random.permutation(jax.random.fold_in(arg_keys[15], 3), TOKENS // (TOK_DEV // N_TP))
    routes = jax.vmap(lambda own, number: assign_block(jax.random.fold_in(arg_keys[15], 2), own, number, TOK_DEV // N_TP, EXPERTS, TOPK, CAP, 2))(routes_keys, routes_turns).reshape((TOKENS, TOPK))
    route_weights = jnp.clip(0.1 + 0.9 * jax.random.uniform(arg_keys[16], (TOKENS, TOPK), jnp.float32) ** levels(arg_keys[16], (TOKENS, TOPK), ((0, 32),), -0.2, 0.2), 0.1, 1.0)
    return dict(x_in=x_in, gate_b=gate_b, gate_c=gate_c, conv_taps=conv_taps, out_proj=out_proj, mix_gain=mix_gain, resid=resid, pre_gain=pre_gain, expert_gate=expert_gate, expert_up=expert_up, expert_down=expert_down, shared_gate=shared_gate, shared_up=shared_up, shared_down=shared_down, post_gain=post_gain, routes=routes, route_weights=route_weights)


epsilon = 1e-06

def reference(x_in, gate_b, gate_c, conv_taps, out_proj, mix_gain, resid, pre_gain, expert_gate, expert_up, expert_down, shared_gate, shared_up, shared_down, post_gain, routes, route_weights):
    mixed_in = gate_c.astype(jnp.float32) * x_in.astype(jnp.float32)
    reach = CONV_WIDTH - 1
    padded = jnp.concatenate([jnp.zeros((reach, CONV_CH), jnp.float32), mixed_in], 0)
    taps = conv_taps.astype(jnp.float32)
    convolved = jnp.zeros((TOKENS, CONV_CH), jnp.float32)
    for index in range(CONV_WIDTH):
        convolved = convolved + taps[index][None, :] * padded[index:index + TOKENS]
    conv_out = (gate_b.astype(jnp.float32) * convolved).astype(jnp.bfloat16)
    projected = jnp.dot(conv_out, out_proj, preferred_element_type=jnp.float32)
    row_scale = lax.rsqrt(lax.optimization_barrier(jnp.mean(projected * projected, axis=1, keepdims=True)) + epsilon)
    resid1 = (resid.astype(jnp.float32) + projected * row_scale * mix_gain.astype(jnp.float32)).astype(jnp.bfloat16)
    wide_resid = resid1.astype(jnp.float32)
    normed = (wide_resid * lax.rsqrt(lax.optimization_barrier(jnp.mean(wide_resid * wide_resid, axis=1, keepdims=True)) + epsilon) * pre_gain.astype(jnp.float32)).astype(jnp.bfloat16)
    block_count = N_SP * N_TP
    quarter = TOK_DEV // N_TP
    flat_ids = routes.reshape(-1).astype(jnp.int32)
    onehot = (flat_ids[:, None] == jnp.arange(EXPERTS, dtype=jnp.int32)[None, :]).astype(jnp.int32)
    blocks = onehot.reshape(block_count, quarter * TOPK, EXPERTS)
    before = (jnp.cumsum(blocks, axis=1) - blocks).reshape(-1, EXPERTS)
    position = lax.optimization_barrier(jnp.sum(before * onehot, axis=1))
    source = jnp.arange(TOKENS * TOPK, dtype=jnp.int32) // (quarter * TOPK)
    slot_index = flat_ids * (block_count * CAP) + source * CAP + position
    dispatched = jnp.zeros((EXPERTS * block_count * CAP, D), jnp.bfloat16).at[slot_index].set(jnp.repeat(normed, TOPK, axis=0))

    def run_expert(operands):
        rows_in, w_gate, w_up, w_down = operands
        gate_h = jnp.dot(rows_in, w_gate, preferred_element_type=jnp.float32)
        up_h = jnp.dot(rows_in, w_up, preferred_element_type=jnp.float32)
        hidden = (jax.nn.silu(gate_h) * up_h).astype(jnp.bfloat16)
        return jnp.dot(hidden, w_down, preferred_element_type=jnp.float32).astype(jnp.bfloat16)
    expert_out = lax.map(run_expert, (dispatched.reshape(EXPERTS, block_count * CAP, D), expert_gate, expert_up, expert_down)).reshape(-1, D)
    picked = expert_out[slot_index].reshape(TOKENS, TOPK, D)
    routed = jnp.zeros((TOKENS, D), jnp.float32)
    for index in range(TOPK):
        routed = routed + route_weights[:, index:index + 1] * picked[:, index].astype(jnp.float32)
    shared_g = jnp.dot(normed, shared_gate, preferred_element_type=jnp.float32)
    shared_u = jnp.dot(normed, shared_up, preferred_element_type=jnp.float32)
    shared_hidden = (jax.nn.silu(shared_g) * shared_u).astype(jnp.bfloat16)
    shared_out = jnp.dot(shared_hidden, shared_down, preferred_element_type=jnp.float32)
    branch = routed + shared_out
    factor = lax.rsqrt(lax.optimization_barrier(jnp.mean(branch * branch, axis=1, keepdims=True)) + epsilon)
    return (wide_resid + branch * factor * post_gain.astype(jnp.float32)).astype(jnp.bfloat16)
```

```python
import functools

import jax
import jax.numpy as jnp
from jax import lax
from jax.experimental import pallas as pl
from jax.experimental.pallas import tpu as pltpu

P = jax.sharding.PartitionSpec
MESH = pl.DeviceIdType.MESH
epsilon = 1e-06
PIECES = 4
HALVES = 2
DIRECT = 2


def layer_kernel(
    line,
    x_ref,
    gate_b_ref,
    gate_c_ref,
    taps_ref,
    resid_ref,
    mix_ref,
    pre_ref,
    post_ref,
    routes_ref,
    weights_ref,
    proj_ref,
    eg_ref,
    eu_ref,
    ed_ref,
    sg_ref,
    su_ref,
    sd_ref,
    out_ref,
    edge_x,
    edge_c,
    mixed,
    conv,
    conv_near,
    proj,
    part_out,
    part_in,
    projected,
    resid1,
    w_gate,
    w_up,
    w_down,
    s_gate,
    s_up,
    s_down,
    blocks,
    sums,
    shared,
    from_low,
    from_high,
    outgoing,
    shares,
    hidden,
    load_sem,
    e_send,
    e_recv,
    p_send,
    p_recv,
    c_send,
    c_recv,
    f_send,
    f_recv,
    wx_send,
    wx_recv,
    wn_send,
    wn_recv,
    wf_send,
    wf_recv,
    wr_send,
    wr_recv,
    t_send,
    t_recv,
    gu_send,
    gu_recv,
    gd_send,
    gd_recv,
    ru_send,
    ru_recv,
    rd_send,
    rd_recv,
):
    sp = lax.axis_index("sp")
    tp = lax.axis_index("tp")
    sp_size = lax.axis_size("sp")
    tp_size = lax.axis_size("tp")
    z = sp // 2
    x = sp % 2
    last = line - 1
    mate = z * 2 + 1 - x
    near = (tp // 2) * 2 + 1 - tp % 2
    far = (tp + 2) % tp_size
    near_far = (near + 2) % tp_size
    rows, width = resid_ref.shape
    step_rows = rows // PIECES
    hid = w_gate.shape[2]
    shared_hid = s_gate.shape[1]

    barrier = pltpu.get_barrier_semaphore()
    for k in range(1, sp_size):
        pl.semaphore_signal(barrier, inc=1, device_id=((sp + k) % sp_size, tp), device_id_type=MESH)
    for k in range(1, tp_size):
        pl.semaphore_signal(barrier, inc=1, device_id=(sp, (tp + k) % tp_size), device_id_type=MESH)

    loads = [
        pltpu.make_async_copy(src, dst, load_sem.at[n])
        for n, (src, dst) in enumerate(
            (
                (eg_ref.at[0], w_gate.at[0]),
                (eu_ref.at[0], w_up.at[0]),
                (ed_ref.at[0], w_down.at[0]),
                (sg_ref, s_gate),
                (su_ref, s_up),
                (sd_ref, s_down),
                (proj_ref, proj.at[0]),
            )
        )
    ]
    loads[-1].start()
    for load in loads[:-1]:
        load.start()

    all_rows, channels = x_ref.shape
    reach = taps_ref.shape[0] - 1
    pad = edge_x.shape[0]
    mixed[pad:] = x_ref[...].astype(jnp.float32) * gate_c_ref[...].astype(jnp.float32)

    def edge_copy(n):
        source, landing = ((x_ref, edge_x), (gate_c_ref, edge_c))[n]
        return pltpu.make_async_remote_copy(
            src_ref=source.at[pl.ds(all_rows - pad, pad)],
            dst_ref=landing,
            send_sem=e_send.at[n],
            recv_sem=e_recv.at[n],
            device_id=((sp + 1) % sp_size, tp),
            device_id_type=MESH,
        )

    proj_copy = pltpu.make_async_remote_copy(
        src_ref=proj_ref,
        dst_ref=proj.at[1],
        send_sem=p_send.at[0],
        recv_sem=p_recv.at[0],
        device_id=(sp, near),
        device_id_type=MESH,
    )

    def block_rows(owner):
        return pl.ds(pl.multiple_of(owner * rows, rows), rows)

    def conv_copy(n):
        return pltpu.make_async_remote_copy(
            src_ref=conv.at[block_rows((near, near_far)[n])],
            dst_ref=conv_near.at[n],
            send_sem=c_send.at[n],
            recv_sem=c_recv.at[n],
            device_id=(sp, near),
            device_id_type=MESH,
        )

    part_cols = width // PIECES

    def part_copy(j):
        cols = pl.ds(pl.multiple_of(j * part_cols, part_cols), part_cols)
        return pltpu.make_async_remote_copy(
            src_ref=part_out.at[:, cols],
            dst_ref=part_in.at[:, cols],
            send_sem=f_send.at[j],
            recv_sem=f_recv.at[j],
            device_id=(sp, far),
            device_id_type=MESH,
        )

    pl.semaphore_wait(barrier, sp_size - 1 + tp_size - 1)

    @pl.when(sp < sp_size - 1)
    def _():
        edge_copy(0).start()
        edge_copy(1).start()

    proj_copy.start()

    pieces = []
    for ref, held in ((eg_ref, w_gate), (eu_ref, w_up), (ed_ref, w_down)):
        size = ref.shape[1] // tp_size // HALVES
        for h in range(HALVES):
            pieces.append((ref, held, size, h))

    def span(owner, n):
        _, _, size, h = pieces[n]
        return pl.ds(pl.multiple_of((owner * HALVES + h) * size, size), size)

    def hop(n, owner, target, send, recv, first=False):
        ref, held, _, _ = pieces[n]
        where = span(owner, n)
        return pltpu.make_async_remote_copy(
            src_ref=ref.at[0, where] if first else held.at[1, where],
            dst_ref=held.at[1, where],
            send_sem=send.at[n],
            recv_sem=recv.at[n],
            device_id=target,
            device_id_type=MESH,
        )

    def x_hop(n):
        return hop(n, tp, (mate, tp), wx_send, wx_recv, True)

    def near_hop(n, owner):
        return hop(n, owner, (sp, near), wn_send, wn_recv)

    def far_hop(n, owner):
        return hop(n, owner, (sp, far), wf_send, wf_recv)

    def direct_hop(n):
        return hop(n, far, (mate, tp), wf_send, wf_recv, True)

    def relay_hop(n, owner):
        return hop(n, owner, (sp, near), wr_send, wr_recv)

    count = len(pieces)

    def line_copy(source, landing, b, c, up, send, recv):
        part = pl.ds(pl.multiple_of(c * step_rows, step_rows), step_rows)
        return pltpu.make_async_remote_copy(
            src_ref=source.at[b, part],
            dst_ref=landing.at[b, part],
            send_sem=send.at[b, c],
            recv_sem=recv.at[b, c],
            device_id=((z + (1 if up else -1)) * 2 + x, tp),
            device_id_type=MESH,
        )

    def go_up(b, c):
        return line_copy(blocks, blocks, b, c, True, gu_send, gu_recv)

    def go_down(b, c):
        return line_copy(blocks, blocks, b, c, False, gd_send, gd_recv)

    def back_up(b, c):
        return line_copy(outgoing, from_low, b, c, True, ru_send, ru_recv)

    def back_down(b, c):
        return line_copy(outgoing, from_high, b, c, False, rd_send, rd_recv)

    def share_copy(k, source):
        return pltpu.make_async_remote_copy(
            src_ref=shares.at[source],
            dst_ref=shares.at[source],
            send_sem=t_send.at[k],
            recv_sem=t_recv.at[source],
            device_id=(((z + k) % line) * 2 + x, tp),
            device_id_type=MESH,
        )

    for n in range(count):
        x_hop(n).start()
    for n in range(count - DIRECT, count):
        direct_hop(n).start()

    lanes = lax.broadcasted_iota(jnp.int32, (rows, shares.shape[2]), 1)
    names = lax.broadcasted_iota(jnp.int32, (shares.shape[2], rows), 0)
    table = jnp.zeros((shares.shape[2], rows), jnp.float32)
    for k in range(routes_ref.shape[0]):
        table += jnp.where(names == routes_ref[k : k + 1], weights_ref[k : k + 1], 0.0)
    shares[z] = table.T

    @pl.when(sp > 0)
    def _():
        edge_copy(0).wait_recv()
        edge_copy(1).wait_recv()
        mixed[:pad] = edge_x[...].astype(jnp.float32) * edge_c[...].astype(jnp.float32)

    @pl.when(sp == 0)
    def _():
        mixed[:pad] = jnp.zeros((pad, channels), jnp.float32)

    convolved = jnp.zeros((all_rows, channels), jnp.float32)
    for k in range(reach + 1):
        begin = pad - reach + k
        convolved += taps_ref[k : k + 1].astype(jnp.float32) * mixed[begin : begin + all_rows]
    conv[...] = (gate_b_ref[...].astype(jnp.float32) * convolved).astype(jnp.bfloat16)
    conv_copy(1).start()
    conv_copy(0).start()
    for k in range(1, line):
        share_copy(k, z).start()
    loads[-1].wait()
    proj_copy.wait_recv()

    def project(n, owner, cols):
        return jnp.dot(
            conv[block_rows(owner)], proj[0, :, cols], preferred_element_type=jnp.float32
        ) + jnp.dot(conv_near[n], proj[1, :, cols], preferred_element_type=jnp.float32)

    conv_copy(1).wait_recv()

    @pl.loop(0, PIECES)
    def _(j):
        cols = pl.ds(pl.multiple_of(j * part_cols, part_cols), part_cols)
        part_out[:, cols] = project(1, far, cols).astype(jnp.bfloat16)
        part_copy(j).start()

    conv_copy(0).wait_recv()

    @pl.loop(0, PIECES)
    def _(j):
        cols = pl.ds(pl.multiple_of(j * part_cols, part_cols), part_cols)
        projected[:, cols] = project(0, tp, cols)

    sums[...] = jnp.zeros_like(sums)

    def spread(n):
        x_hop(n).wait_recv()
        if n < count - DIRECT:
            far_hop(n, tp).start()
        near_hop(n, tp).start()

    for n in range(count // 2):
        spread(n)

    @pl.loop(0, PIECES)
    def _(j):
        cols = pl.ds(pl.multiple_of(j * part_cols, part_cols), part_cols)
        part_copy(j).wait_recv()
        projected[:, cols] += part_in[:, cols].astype(jnp.float32)

    def send_block(c):
        @pl.when(z < last)
        def _():
            go_up(z, c).start()

        @pl.when(z > 0)
        def _():
            go_down(z, c).start()

    for c in range(PIECES):
        part = pl.ds(c * step_rows, step_rows)
        block = projected[part]
        scale = lax.rsqrt(jnp.mean(block * block, axis=1, keepdims=True) + epsilon)
        mid = (
            resid_ref[part].astype(jnp.float32)
            + block * scale * mix_ref[...].astype(jnp.float32).reshape(1, width)
        ).astype(jnp.bfloat16)
        resid1[part] = mid
        wide = mid.astype(jnp.float32)
        normal = lax.rsqrt(jnp.mean(wide * wide, axis=1, keepdims=True) + epsilon)
        blocks[z, part] = (wide * normal * pre_ref[...].astype(jnp.float32).reshape(1, width)).astype(jnp.bfloat16)
        if c > 0:
            send_block(c - 1)
    send_block(PIECES - 1)

    def apply(b, i):
        expert = z * 2 + x + i * (1 - 2 * x)

        @pl.loop(0, hid // 256)
        def _(j):
            cols = pl.ds(pl.multiple_of(j * 256, 256), 256)
            gate = jnp.dot(blocks[b], w_gate[i, :, cols], preferred_element_type=jnp.float32)
            up = jnp.dot(blocks[b], w_up[i, :, cols], preferred_element_type=jnp.float32)
            hidden[:, cols] = (jax.nn.silu(gate) * up).astype(jnp.bfloat16)

        share = jnp.sum(jnp.where(lanes == expert, shares[b], 0.0), axis=1, keepdims=True)

        @pl.loop(0, width // 512)
        def _(j):
            cols = pl.ds(pl.multiple_of(j * 512, 512), 512)
            made = jnp.dot(hidden[...], w_down[i, :, cols], preferred_element_type=jnp.float32)
            made = made.astype(jnp.bfloat16).astype(jnp.float32)
            sums[b, :, cols] += jnp.where(share > 0.0, share * made, 0.0)

    def receive(t):
        @pl.loop(0, PIECES)
        def _(c):
            @pl.when(z - t >= 0)
            def _():
                go_up(z - t, c).wait_recv()

                @pl.when(z < last)
                def _():
                    go_up(z - t, c).start()

            @pl.when(z + t <= last)
            def _():
                go_down(z + t, c).wait_recv()

                @pl.when(z > 0)
                def _():
                    go_down(z + t, c).start()

    def apply_pair(t, i):
        @pl.loop(0, 2)
        def _(side):
            b = z - t + side * 2 * t

            @pl.when((b >= 0) & (b <= last))
            def _():
                apply(b, i)

    def give_back(t):
        p_up = t - z
        p_down = t - (last - z)
        b_up = (p_up + last) % last + 1
        b_down = last - ((p_down + last) % last + 1)
        send_up = (p_up >= 1) & (p_up <= last) & (b_up > z)
        send_down = (p_down >= 1) & (p_down <= last) & (b_down < z)

        @pl.loop(0, PIECES)
        def _(c):
            part = pl.ds(pl.multiple_of(c * step_rows, step_rows), step_rows)

            @pl.when(send_up)
            def _():
                @pl.when(z > 0)
                def _():
                    back_up(b_up, c).wait_recv()
                    sums[b_up, part] += from_low[b_up, part].astype(jnp.float32)

                outgoing[b_up, part] = sums[b_up, part].astype(jnp.bfloat16)
                back_up(b_up, c).start()

            @pl.when(send_down)
            def _():
                @pl.when(z < last)
                def _():
                    back_down(b_down, c).wait_recv()
                    sums[b_down, part] += from_high[b_down, part].astype(jnp.float32)

                outgoing[b_down, part] = sums[b_down, part].astype(jnp.bfloat16)
                back_down(b_down, c).start()

    for load in loads[:3]:
        load.wait()
    apply(z, 0)
    for load in loads[3:-1]:
        load.wait()
    s_g = jnp.dot(blocks[z], s_gate[...], preferred_element_type=jnp.float32)
    s_u = jnp.dot(blocks[z], s_up[...], preferred_element_type=jnp.float32)
    s_h = (jax.nn.silu(s_g) * s_u).astype(jnp.bfloat16)
    hidden[:, :shared_hid] = s_h

    @pl.loop(0, width // 512)
    def _(j):
        cols = pl.ds(pl.multiple_of(j * 512, 512), 512)
        shared[:, cols] = jnp.dot(
            hidden[:, :shared_hid], s_down[:, cols], preferred_element_type=jnp.float32
        )

    for n in range(count // 2, count):
        spread(n)
    receive(1)
    for k in range(1, line):
        share_copy(k, (z + k) % line).wait_recv()
    apply_pair(1, 0)

    def relay(n):
        far_hop(n, far).wait_recv()
        relay_hop(n, far).start()

    for n in range(2 * count // 3):
        relay(n)
    for t in range(2, last):
        receive(t)
        apply_pair(t, 0)
    for n in range(2 * count // 3, count):
        relay(n)
    for n in range(count):
        near_hop(n, near).wait_recv()
        relay_hop(n, near_far).wait_recv()

    @pl.loop(2, last)
    def _(t):
        apply_pair(t, 1)

    give_back(1)
    apply_pair(1, 1)
    receive(last)
    apply_pair(last, 0)
    apply_pair(last, 1)
    give_back(2)
    apply(z, 1)

    @pl.loop(3, 2 * last - 1)
    def _(t):
        give_back(t)

    @pl.loop(0, PIECES)
    def _(c):
        part = pl.ds(pl.multiple_of(c * step_rows, step_rows), step_rows)

        @pl.when(z > 0)
        def _():
            back_up(z, c).wait_recv()
            sums[z, part] += from_low[z, part].astype(jnp.float32)

        @pl.when(z < last)
        def _():
            back_down(z, c).wait_recv()
            sums[z, part] += from_high[z, part].astype(jnp.float32)

        branch = sums[z, part] + shared[part]
        factor = lax.rsqrt(jnp.mean(branch * branch, axis=1, keepdims=True) + epsilon)
        out_ref[part] = (
            resid1[part].astype(jnp.float32)
            + branch * factor * post_ref[...].astype(jnp.float32).reshape(1, width)
        ).astype(jnp.bfloat16)

    @pl.when(sp < sp_size - 1)
    def _():
        edge_copy(0).wait_send()
        edge_copy(1).wait_send()

    proj_copy.wait_send()
    conv_copy(0).wait_send()
    conv_copy(1).wait_send()
    for j in range(PIECES):
        part_copy(j).wait_send()
    for n in range(count):
        x_hop(n).wait_send()
        near_hop(n, tp).wait_send()
        far_hop(n, tp).wait_send()
        relay_hop(n, far).wait_send()
    for k in range(1, line):
        share_copy(k, z).wait_send()

    @pl.loop(0, PIECES)
    def _(c):
        @pl.loop(0, line)
        def _(b):
            @pl.when((b <= z) & (z < last))
            def _():
                go_up(b, c).wait_send()

            @pl.when((b >= z) & (z > 0))
            def _():
                go_down(b, c).wait_send()

            @pl.when(b > z)
            def _():
                back_up(b, c).wait_send()

            @pl.when(b < z)
            def _():
                back_down(b, c).wait_send()


def fused_layer(
    x_in, gate_b, gate_c, conv_taps, out_proj, mix_gain, resid, pre_gain, expert_gate, expert_up,
    expert_down, shared_gate, shared_up, shared_down, post_gain, routes, route_weights,
):
    experts = lax.axis_size("sp")
    line = experts // 2
    all_rows, channels = x_in.shape
    rows, width = resid.shape
    hid = expert_gate.shape[2]
    shared_hid = shared_gate.shape[1]
    dma = pltpu.SemaphoreType.DMA
    count = 3 * HALVES
    bf, f32 = jnp.bfloat16, jnp.float32
    vmem = pl.BlockSpec(memory_space=pltpu.VMEM)
    hbm = pl.BlockSpec(memory_space=pltpu.HBM)
    lanes = 128 * (-(-experts // 128))
    pad = 16 * (-(-(conv_taps.shape[0] - 1) // 16))
    return pl.pallas_call(
        functools.partial(layer_kernel, line),
        out_shape=jax.ShapeDtypeStruct((rows, width), bf),
        in_specs=[vmem] * 10 + [hbm] * 7,
        out_specs=vmem,
        scratch_shapes=[
            pltpu.VMEM((pad, channels), bf),
            pltpu.VMEM((pad, channels), bf),
            pltpu.VMEM((pad + all_rows, channels), f32),
            pltpu.VMEM((all_rows, channels), bf),
            pltpu.VMEM((2, rows, channels), bf),
            pltpu.VMEM((2, channels, width), bf),
            pltpu.VMEM((rows, width), bf),
            pltpu.VMEM((rows, width), bf),
            pltpu.VMEM((rows, width), f32),
            pltpu.VMEM((rows, width), bf),
            pltpu.VMEM((2, width, hid), bf),
            pltpu.VMEM((2, width, hid), bf),
            pltpu.VMEM((2, hid, width), bf),
            pltpu.VMEM((width, shared_hid), bf),
            pltpu.VMEM((width, shared_hid), bf),
            pltpu.VMEM((shared_hid, width), bf),
            pltpu.VMEM((line, rows, width), bf),
            pltpu.VMEM((line, rows, width), f32),
            pltpu.VMEM((rows, width), f32),
            pltpu.VMEM((line, rows, width), bf),
            pltpu.VMEM((line, rows, width), bf),
            pltpu.VMEM((line, rows, width), bf),
            pltpu.VMEM((line, rows, lanes), f32),
            pltpu.VMEM((rows, max(hid, shared_hid)), bf),
            dma((7,)),
            dma((2,)),
            dma((2,)),
            dma((1,)),
            dma((1,)),
            dma((2,)),
            dma((2,)),
            dma((PIECES,)),
            dma((PIECES,)),
        ]
        + [dma((count,))] * 8
        + [dma((line,))] * 2
        + [dma((line, PIECES))] * 8,
        compiler_params=pltpu.CompilerParams(
            collective_id=0, has_side_effects=True, vmem_limit_bytes=60 * 1024 * 1024
        ),
    )(
        x_in, gate_b, gate_c, conv_taps, resid, mix_gain, pre_gain, post_gain,
        routes.T, route_weights.T, out_proj, expert_gate, expert_up, expert_down,
        shared_gate, shared_up, shared_down,
    )


def passed_along(shard, axis, by):
    size = lax.axis_size(axis)
    pairs = [(i, i + by) for i in range(size) if 0 <= i + by < size]
    return lax.ppermute(shard, axis, pairs)


def body(
    x_in,
    gate_b,
    gate_c,
    conv_taps,
    out_proj,
    mix_gain,
    resid,
    pre_gain,
    expert_gate,
    expert_up,
    expert_down,
    shared_gate,
    shared_up,
    shared_down,
    post_gain,
    routes,
    route_weights,
):
    group = lax.axis_size("sp")
    wide_slots = 3 * resid.shape[0] * routes.shape[1] // group
    if wide_slots > resid.shape[0] and group % 2 == 0 and lax.axis_size("tp") == 2 * 2:
        return fused_layer(
            x_in, gate_b, gate_c, conv_taps, out_proj, mix_gain, resid, pre_gain, expert_gate,
            expert_up, expert_down, shared_gate, shared_up, shared_down, post_gain, routes,
            route_weights,
        )
    row_count = x_in.shape[0]
    channels = x_in.shape[1]
    reach = conv_taps.shape[0] - 1
    edge_rows = jnp.concatenate([x_in[row_count - reach :], gate_c[row_count - reach :]], 1)
    arrived_edge = passed_along(edge_rows, "sp", 1)
    inputs = jnp.concatenate([arrived_edge[:, :channels], x_in], 0).astype(jnp.float32)
    gate_rows = jnp.concatenate([arrived_edge[:, channels:], gate_c], 0).astype(jnp.float32)
    mixed_in = inputs * gate_rows
    taps = conv_taps.astype(jnp.float32)
    convolved = jnp.zeros((row_count, channels), jnp.float32)
    for index in range(reach + 1):
        convolved = convolved + taps[index][None, :] * mixed_in[index : index + row_count]
    conv_out = (gate_b.astype(jnp.float32) * convolved).astype(jnp.bfloat16)
    width_all = out_proj.shape[1]
    full_rows = lax.all_to_all(conv_out, "tp", split_axis=0, concat_axis=1, tiled=True)
    projected = jnp.dot(
        full_rows,
        lax.all_gather(out_proj, "tp", axis=0, tiled=True),
        preferred_element_type=jnp.float32,
    )
    row_scale = lax.rsqrt(jnp.mean(projected * projected, axis=1, keepdims=True) + epsilon)
    resid1 = (
        resid.astype(jnp.float32) + projected * row_scale * mix_gain.astype(jnp.float32)
    ).astype(jnp.bfloat16)
    wide_resid = resid1.astype(jnp.float32)
    normed = (
        wide_resid
        * lax.rsqrt(jnp.mean(wide_resid * wide_resid, axis=1, keepdims=True) + epsilon)
        * pre_gain.astype(jnp.float32)
    ).astype(jnp.bfloat16)
    experts = lax.axis_size("sp")
    local_rows = resid.shape[0]
    top_count = routes.shape[1]
    capacity = 3 * local_rows * top_count // (2 * experts)
    flat_ids = routes.reshape(-1)
    onehot = (flat_ids[:, None] == jnp.arange(experts, dtype=jnp.int32)[None, :]).astype(jnp.int32)
    before = jnp.cumsum(onehot, axis=0) - onehot
    position = jnp.sum(before * onehot, axis=1)
    slot_index = flat_ids * capacity + position
    outgoing = (
        jnp.zeros((experts * capacity, width_all), jnp.bfloat16)
        .at[slot_index]
        .set(jnp.repeat(normed, top_count, axis=0))
    )
    received = lax.all_to_all(
        outgoing.reshape(experts, capacity, width_all),
        "sp",
        split_axis=0,
        concat_axis=0,
        tiled=True,
    )
    arrived = received.reshape(experts * capacity, width_all)
    gate_h = jnp.dot(arrived, expert_gate[0], preferred_element_type=jnp.float32)
    up_h = jnp.dot(arrived, expert_up[0], preferred_element_type=jnp.float32)
    hidden = (jax.nn.silu(gate_h) * up_h).astype(jnp.bfloat16)
    expert_out = jnp.dot(hidden, expert_down[0], preferred_element_type=jnp.float32).astype(
        jnp.bfloat16
    )
    returned = lax.all_to_all(
        expert_out.reshape(experts, capacity, width_all),
        "sp",
        split_axis=0,
        concat_axis=0,
        tiled=True,
    )
    returned = returned.reshape(experts * capacity, width_all)
    picked = returned[slot_index].astype(jnp.float32).reshape(local_rows, top_count, width_all)
    routed = jnp.einsum("tk,tkd->td", route_weights, picked)
    shared_g = jnp.dot(normed, shared_gate, preferred_element_type=jnp.float32)
    shared_u = jnp.dot(normed, shared_up, preferred_element_type=jnp.float32)
    shared_hidden = (jax.nn.silu(shared_g) * shared_u).astype(jnp.bfloat16)
    shared_out = jnp.dot(shared_hidden, shared_down, preferred_element_type=jnp.float32)
    branch = routed + shared_out
    factor = lax.rsqrt(jnp.mean(branch * branch, axis=1, keepdims=True) + epsilon)
    return (wide_resid + branch * factor * post_gain.astype(jnp.float32)[None, :]).astype(
        jnp.bfloat16
    )


def solution(mesh):
    return jax.shard_map(
        body,
        mesh=mesh,
        in_specs=(
            P("sp", "tp"),
            P("sp", "tp"),
            P("sp", "tp"),
            P(None, "tp"),
            P("tp", None),
            P(),
            P(("sp", "tp"), None),
            P(),
            P("sp", None, None),
            P("sp", None, None),
            P("sp", None, None),
            P(),
            P(),
            P(),
            P(),
            P(("sp", "tp"), None),
            P(("sp", "tp"), None),
        ),
        out_specs=P(("sp", "tp"), None),
        check_vma=False,
    )
```

```python
import functools

import jax
import jax.numpy as jnp
from jax import lax
from jax.experimental import pallas as pl
from jax.experimental.pallas import tpu as pltpu

P = jax.sharding.PartitionSpec
MESH = pl.DeviceIdType.MESH
epsilon = 1e-06
PIECES = 4
HALVES = 2
DIRECT = (3, 7)
TABLE = HALVES


def layer_kernel(
    line,
    x_hbm,
    gate_b_hbm,
    gate_c_hbm,
    taps_hbm,
    resid_hbm,
    mix_hbm,
    pre_hbm,
    post_hbm,
    routes_hbm,
    weights_hbm,
    proj_ref,
    eg_ref,
    eu_ref,
    ed_ref,
    sg_ref,
    su_ref,
    sd_ref,
    out_ref,
    x_ref,
    gate_b_ref,
    gate_c_ref,
    taps_ref,
    resid_ref,
    mix_ref,
    pre_ref,
    post_ref,
    routes_ref,
    weights_ref,
    edge_x,
    edge_c,
    mixed,
    conv,
    conv_near,
    proj,
    part_out,
    part_in,
    projected,
    resid1,
    w_gate,
    w_up,
    w_down,
    s_gate,
    s_up,
    s_down,
    blocks,
    shares,
    hidden,
    shared_hidden,
    branch,
    outgoing,
    from_out,
    from_in,
    load_sem,
    e_send,
    e_recv,
    p_send,
    p_recv,
    c_send,
    c_recv,
    f_send,
    f_recv,
    wx_send,
    wx_recv,
    wn_send,
    wn_recv,
    wf_send,
    wf_recv,
    wr_send,
    wr_recv,
    gi_send,
    go_send,
    gi_recv,
    go_recv,
    ri_send,
    ro_send,
    ri_recv,
    ro_recv,
):
    sp = lax.axis_index("sp")
    tp = lax.axis_index("tp")
    sp_size = lax.axis_size("sp")
    tp_size = lax.axis_size("tp")
    z = sp // 2
    x = sp % 2
    last = line - 1
    mate = z * 2 + 1 - x
    near = (tp // 2) * 2 + 1 - tp % 2
    far = (tp + 2) % tp_size
    near_far = (near + 2) % tp_size
    upper = z // (line // 2)
    inward_step = 1 - 2 * upper
    level = upper * last + inward_step * z
    inward = ((z + inward_step) * 2 + x, tp)
    outward = ((z - inward_step) * 2 + x, tp)

    def rel(k):
        return upper * last + inward_step * k

    rows, width = resid_ref.shape
    half_rows = rows // HALVES
    hid = w_gate.shape[2]
    shared_hid = s_gate.shape[1]
    part_cols = width // PIECES

    barrier = pltpu.get_barrier_semaphore()

    def greet(device):
        pl.semaphore_signal(barrier, inc=1, device_id=device, device_id_type=MESH)

    greet((mate, tp))
    greet((sp, near))
    greet((sp, far))

    @pl.when(z > 0)
    def _():
        greet((sp - 2, tp))

    @pl.when(z < last)
    def _():
        greet((sp + 2, tp))

    @pl.when((x == 1) & (z < last))
    def _():
        greet((sp + 1, tp))

    @pl.when((x == 0) & (z > 0))
    def _():
        greet((sp - 1, tp))

    pairs = (
        (x_hbm, x_ref),
        (gate_c_hbm, gate_c_ref),
        (proj_ref, proj.at[0]),
        (gate_b_hbm, gate_b_ref),
        (taps_hbm, taps_ref),
        (routes_hbm, routes_ref),
        (weights_hbm, weights_ref),
        (resid_hbm, resid_ref),
        (mix_hbm, mix_ref),
        (pre_hbm, pre_ref),
        (eg_ref.at[0], w_gate.at[0]),
        (eu_ref.at[0], w_up.at[0]),
        (sg_ref, s_gate),
        (su_ref, s_up),
        (ed_ref.at[0], w_down.at[pl.ds(0, hid)]),
        (sd_ref, s_down),
        (post_hbm, post_ref),
    )
    loads = [pltpu.make_async_copy(src, dst, load_sem.at[n]) for n, (src, dst) in enumerate(pairs)]
    for load in loads:
        load.start()

    all_rows, channels = x_ref.shape
    reach = taps_ref.shape[0] - 1
    pad = edge_x.shape[0]

    def edge_copy(n):
        source, landing = ((x_ref, edge_x), (gate_c_ref, edge_c))[n]
        return pltpu.make_async_remote_copy(
            src_ref=source.at[pl.ds(all_rows - pad, pad)],
            dst_ref=landing,
            send_sem=e_send.at[n],
            recv_sem=e_recv.at[n],
            device_id=((sp + 1) % sp_size, tp),
            device_id_type=MESH,
        )

    proj_copy = pltpu.make_async_remote_copy(
        src_ref=proj.at[0],
        dst_ref=proj.at[1],
        send_sem=p_send.at[0],
        recv_sem=p_recv.at[0],
        device_id=(sp, near),
        device_id_type=MESH,
    )

    def block_rows(owner):
        return pl.ds(pl.multiple_of(owner * rows, rows), rows)

    def conv_copy(n):
        return pltpu.make_async_remote_copy(
            src_ref=conv.at[block_rows((near, near_far)[n])],
            dst_ref=conv_near.at[n],
            send_sem=c_send.at[n],
            recv_sem=c_recv.at[n],
            device_id=(sp, near),
            device_id_type=MESH,
        )

    def chunk(j):
        return pl.ds(pl.multiple_of(j * part_cols, part_cols), part_cols)

    def half(r):
        return pl.ds(r * half_rows, half_rows)

    def part_copy(j):
        return pltpu.make_async_remote_copy(
            src_ref=part_out.at[:, chunk(j)],
            dst_ref=part_in.at[:, chunk(j)],
            send_sem=f_send.at[j],
            recv_sem=f_recv.at[j],
            device_id=(sp, far),
            device_id_type=MESH,
        )

    pieces = []
    for ref, held in ((eg_ref, w_gate), (eu_ref, w_up)):
        for h in range(HALVES):
            pieces.append((ref, held, h))
    for j in range(PIECES):
        pieces.append((ed_ref, w_down, j))
    count = len(pieces)

    def cut(n, owner):
        ref, held, h = pieces[n]
        if held is w_down:
            size = hid // tp_size
            begin = pl.multiple_of(owner * size, size)
            return (
                ref.at[0, pl.ds(begin, size), chunk(h)],
                held.at[pl.ds(pl.multiple_of(hid + begin, size), size), chunk(h)],
            )
        size = ref.shape[1] // tp_size // HALVES
        where = pl.ds(pl.multiple_of((owner * HALVES + h) * size, size), size)
        return ref.at[0, where], held.at[1, where]

    def hop(n, owner, target, send, recv, first=False):
        source, landing = cut(n, owner)
        return pltpu.make_async_remote_copy(
            src_ref=source if first else landing,
            dst_ref=landing,
            send_sem=send.at[n],
            recv_sem=recv.at[n],
            device_id=target,
            device_id_type=MESH,
        )

    def x_hop(n):
        return hop(n, tp, (mate, tp), wx_send, wx_recv, True)

    def near_hop(n, owner):
        return hop(n, owner, (sp, near), wn_send, wn_recv)

    def far_hop(n, owner):
        return hop(n, owner, (sp, far), wf_send, wf_recv)

    def direct_hop(n):
        return hop(n, far, (mate, tp), wf_send, wf_recv, True)

    def relay_hop(n, owner):
        return hop(n, owner, (sp, near), wr_send, wr_recv)

    def spread(n):
        with jax.named_scope("w_x"):
            x_hop(n).wait_recv()
        if n not in DIRECT:
            far_hop(n, tp).start()
        near_hop(n, tp).start()

    def relay(n):
        with jax.named_scope("w_far"):
            far_hop(n, far).wait_recv()
        relay_hop(n, far).start()

    def ready(n):
        with jax.named_scope("w_ready"):
            near_hop(n, near).wait_recv()
            relay_hop(n, near_far).wait_recv()

    def block_copy(b, r, target, send, recv):
        ref = shares.at[b] if r == TABLE else blocks.at[b, half(r)]
        return pltpu.make_async_remote_copy(
            src_ref=ref,
            dst_ref=ref,
            send_sem=send.at[b, r],
            recv_sem=recv.at[b, r],
            device_id=target,
            device_id_type=MESH,
        )

    def edge_in(b, r):
        return block_copy(b, r, inward, gi_send, go_recv)

    def mid_in(b, r):
        return block_copy(b, r, inward, gi_send, gi_recv)

    def mid_out(b, r):
        return block_copy(b, r, outward, go_send, gi_recv)

    def got_in(b, r):
        with jax.named_scope("w_gi"):
            block_copy(b, r, inward, gi_send, gi_recv).wait_recv()

    def got_out(b, r):
        with jax.named_scope("w_go"):
            block_copy(b, r, outward, go_send, go_recv).wait_recv()

    def sum_copy(b, r, j, landing, target, send, recv):
        return pltpu.make_async_remote_copy(
            src_ref=outgoing.at[b, half(r), chunk(j)],
            dst_ref=landing.at[b, half(r), chunk(j)],
            send_sem=send.at[b, r, j],
            recv_sem=recv.at[b, r, j],
            device_id=target,
            device_id_type=MESH,
        )

    def edge_give(b, r, j):
        return sum_copy(b, r, j, from_out, inward, ri_send, ro_recv)

    def mid_give_in(b, r, j):
        return sum_copy(b, r, j, from_in, inward, ri_send, ri_recv)

    def mid_give_out(b, r, j):
        return sum_copy(b, r, j, from_in, outward, ro_send, ri_recv)

    def sum_in(b, r, j):
        with jax.named_scope("w_ri"):
            sum_copy(b, r, j, from_in, inward, ri_send, ri_recv).wait_recv()

    def sum_out(b, r, j):
        with jax.named_scope("w_ro"):
            sum_copy(b, r, j, from_out, outward, ro_send, ro_recv).wait_recv()

    with jax.named_scope("w_barrier"):
        met = 3 + jnp.where(z > 0, 1, 0) + jnp.where(z < last, 1, 0)
        met += jnp.where(jnp.where(x == 1, z < last, z > 0), 1, 0)
        pl.semaphore_wait(barrier, met)

    for n in range(count):
        x_hop(n).start()
        if n in DIRECT:
            direct_hop(n).start()

    loads[0].wait()
    loads[1].wait()

    @pl.when(sp < sp_size - 1)
    def _():
        edge_copy(0).start()
        edge_copy(1).start()

    loads[2].wait()
    proj_copy.start()
    mixed[pad:] = x_ref[...].astype(jnp.float32) * gate_c_ref[...].astype(jnp.float32)
    loads[3].wait()
    loads[4].wait()

    with jax.named_scope("w_edge"):

        @pl.when(sp > 0)
        def _():
            edge_copy(0).wait_recv()
            edge_copy(1).wait_recv()
            mixed[:pad] = edge_x[...].astype(jnp.float32) * edge_c[...].astype(jnp.float32)

        @pl.when(sp == 0)
        def _():
            mixed[:pad] = jnp.zeros((pad, channels), jnp.float32)

    convolved = jnp.zeros((all_rows, channels), jnp.float32)
    for k in range(reach + 1):
        begin = pad - reach + k
        convolved += taps_ref[k : k + 1].astype(jnp.float32) * mixed[begin : begin + all_rows]
    conv[...] = (gate_b_ref[...].astype(jnp.float32) * convolved).astype(jnp.bfloat16)
    conv_copy(1).start()
    conv_copy(0).start()

    def project(n, owner, cols):
        return jnp.dot(
            conv[block_rows(owner)], proj[0, :, cols], preferred_element_type=jnp.float32
        ) + jnp.dot(conv_near[n], proj[1, :, cols], preferred_element_type=jnp.float32)

    with jax.named_scope("w_conv"):
        proj_copy.wait_recv()
        conv_copy(1).wait_recv()

    @pl.loop(0, PIECES)
    def _(j):
        part_out[:, chunk(j)] = project(1, far, chunk(j)).astype(jnp.bfloat16)
        part_copy(j).start()

    loads[5].wait()
    loads[6].wait()
    lanes = lax.broadcasted_iota(jnp.int32, (rows, shares.shape[2]), 1)
    names = lax.broadcasted_iota(jnp.int32, (shares.shape[2], rows), 0)
    table = jnp.zeros((shares.shape[2], rows), jnp.float32)
    for k in range(routes_ref.shape[0]):
        table += jnp.where(names == routes_ref[k : k + 1], weights_ref[k : k + 1], 0.0)
    shares[z] = table.T

    own = z

    @pl.when(level == 0)
    def _():
        edge_in(own, TABLE).start()

    @pl.when(level == 1)
    def _():
        mid_in(own, TABLE).start()
        mid_out(own, TABLE).start()

    conv_copy(0).wait_recv()

    @pl.loop(0, PIECES)
    def _(j):
        projected[:, chunk(j)] = project(0, tp, chunk(j))

    spread(0)
    spread(1)
    for load in loads[7:10]:
        load.wait()

    with jax.named_scope("w_part"):

        @pl.loop(0, PIECES)
        def _(j):
            part_copy(j).wait_recv()
            projected[:, chunk(j)] += part_in[:, chunk(j)].astype(jnp.float32)

    with jax.named_scope("norm"):
        for r in range(HALVES):
            part = half(r)
            block = projected[part]
            scale = lax.rsqrt(jnp.mean(block * block, axis=1, keepdims=True) + epsilon)
            mid = (
                resid_ref[part].astype(jnp.float32)
                + block * scale * mix_ref[...].astype(jnp.float32).reshape(1, width)
            ).astype(jnp.bfloat16)
            resid1[part] = mid
            wide = mid.astype(jnp.float32)
            normal = lax.rsqrt(jnp.mean(wide * wide, axis=1, keepdims=True) + epsilon)
            blocks[own, part] = (
                wide * normal * pre_ref[...].astype(jnp.float32).reshape(1, width)
            ).astype(jnp.bfloat16)

            @pl.when(level == 0)
            def _():
                edge_in(own, r).start()

            @pl.when(level == 1)
            def _():
                mid_in(own, r).start()
                mid_out(own, r).start()

    spread(2)

    def hide(b, begin, size, e):
        part = pl.ds(begin, size)
        expert = z * 2 + x + e * (1 - 2 * x)
        share = jnp.sum(
            jnp.where(lanes[:size] == expert, shares[b, part], 0.0), axis=1, keepdims=True
        )

        @pl.loop(0, hid // 256)
        def _(j):
            cols = pl.ds(pl.multiple_of(j * 256, 256), 256)
            gate = jnp.dot(blocks[b, part], w_gate[e, :, cols], preferred_element_type=jnp.float32)
            up = jnp.dot(blocks[b, part], w_up[e, :, cols], preferred_element_type=jnp.float32)
            kept = pl.ds(pl.multiple_of(e * hid + j * 256, 256), 256)
            hidden[b, part, kept] = (jax.nn.silu(gate) * up * share).astype(jnp.bfloat16)

    def hide_all(b, e):
        hide(b, 0, rows, e)

    def hide_half(b, r):
        hide(b, r * half_rows, half_rows, 0)
        hide(b, r * half_rows, half_rows, 1)

    def down(b, part, j):
        return jnp.dot(
            hidden[b, part], w_down[:, chunk(j)], preferred_element_type=jnp.float32
        )

    def give(b, r, j, arrived, send):
        made = down(b, half(r), j)
        if arrived is not None:
            made += arrived[b, half(r), chunk(j)].astype(jnp.float32)
        outgoing[b, half(r), chunk(j)] = made.astype(jnp.bfloat16)
        send(b, r, j).start()

    def shared_up_to_hidden():
        s_g = jnp.dot(blocks[own], s_gate[...], preferred_element_type=jnp.float32)
        s_u = jnp.dot(blocks[own], s_up[...], preferred_element_type=jnp.float32)
        shared_hidden[...] = (jax.nn.silu(s_g) * s_u).astype(jnp.bfloat16)

    def own_branch():
        @pl.loop(0, PIECES)
        def _(j):
            branch[:, chunk(j)] = down(own, pl.ds(0, rows), j) + jnp.dot(
                shared_hidden[...], s_down[:, chunk(j)], preferred_element_type=jnp.float32
            )

    def yield_out(part, total):
        factor = lax.rsqrt(jnp.mean(total * total, axis=1, keepdims=True) + epsilon)
        out_ref[part] = (
            resid1[part].astype(jnp.float32)
            + total * factor * post_ref[...].astype(jnp.float32).reshape(1, width)
        ).astype(jnp.bfloat16)

    for load in loads[10:14]:
        load.wait()
    hide_all(own, 0)
    shared_up_to_hidden()
    relay(0)
    spread(3)
    for load in loads[14:]:
        load.wait()

    @pl.when(level == 0)
    def _():
        b1, b2, b3 = rel(1), rel(2), rel(3)
        got_in(b1, TABLE)
        got_in(b1, 0)
        hide(b1, 0, half_rows, 0)
        relay(1)
        relay(3)
        got_in(b1, 1)
        hide(b1, half_rows, half_rows, 0)
        spread(4)
        relay(2)
        spread(5)
        got_in(b2, TABLE)
        got_in(b3, TABLE)
        for n in range(4):
            ready(n)
        hide_all(b1, 1)
        hide_all(own, 1)
        relay(4)
        spread(6)
        got_in(b2, 0)
        hide_half(b2, 0)
        ready(4)
        for r in range(HALVES):
            give(b1, r, 0, None, edge_give)
        give(b2, 0, 0, None, edge_give)
        relay(5)
        spread(7)
        ready(5)
        give(b2, 0, 1, None, edge_give)
        for r in range(HALVES):
            give(b1, r, 1, None, edge_give)
        relay(6)
        relay(7)
        got_in(b2, 1)
        hide_half(b2, 1)

        @pl.loop(0, 2)
        def _(j):
            give(b2, 1, j, None, edge_give)

        ready(6)
        ready(7)

        @pl.loop(2, PIECES)
        def _(j):
            for r in range(HALVES):
                give(b2, r, j, None, edge_give)

        own_branch()
        for r in range(HALVES):
            got_in(b3, r)
            hide_half(b3, r)

            @pl.loop(0, PIECES)
            def _(j):
                give(b3, r, j, None, edge_give)

        @pl.loop(2, PIECES)
        def _(j):
            for r in range(HALVES):
                give(b1, r, j, None, edge_give)

        for r in range(HALVES):

            @pl.loop(0, PIECES)
            def _(j):
                sum_in(own, r, j)

            total = branch[half(r)] + from_in[own, half(r)].astype(jnp.float32)
            yield_out(half(r), total)

        for r in range(HALVES + 1):
            edge_in(own, r).wait_send()

        @pl.loop(0, PIECES)
        def _(j):
            for b in (b1, b2, b3):
                for r in range(HALVES):
                    edge_give(b, r, j).wait_send()

    @pl.when(level == 1)
    def _():
        b0, b2, b3 = rel(0), rel(2), rel(3)

        def pass_in(r):
            got_out(b0, r)
            mid_in(b0, r).start()

        def pass_out(b, r):
            got_in(b, r)
            mid_out(b, r).start()

        pass_in(TABLE)
        pass_out(b2, TABLE)
        pass_in(0)
        pass_out(b2, 0)
        pass_out(b3, TABLE)
        relay(1)
        relay(3)
        pass_in(1)
        pass_out(b2, 1)
        hide_all(b0, 0)
        spread(4)
        hide_all(b2, 0)
        relay(2)
        spread(5)
        for n in range(4):
            ready(n)
        hide_all(b2, 1)
        relay(4)
        spread(6)
        hide_all(own, 1)
        pass_out(b3, 0)
        relay(5)
        spread(7)
        hide_all(b0, 1)
        relay(6)
        relay(7)
        pass_out(b3, 1)
        hide_all(b3, 0)
        hide_all(b3, 1)
        for n in range(4, count):
            ready(n)

        def give_in(b, r, j):
            sum_out(b, r, j)
            give(b, r, j, from_out, mid_give_in)

        def give_out(r, j):
            sum_in(b0, r, j)
            give(b0, r, j, from_in, mid_give_out)

        give_in(b2, 0, 0)
        own_branch()
        give_in(b2, 0, 1)

        @pl.loop(0, 2)
        def _(j):
            give_in(b2, 1, j)

        @pl.loop(2, PIECES)
        def _(j):
            for r in range(HALVES):
                give_in(b2, r, j)

        @pl.loop(0, PIECES)
        def _(j):
            give_in(b3, 0, j)

        @pl.loop(0, PIECES)
        def _(j):
            give_out(0, j)
            give_in(b3, 1, j)

        @pl.loop(0, PIECES)
        def _(j):
            give_out(1, j)

        for r in range(HALVES):

            @pl.loop(0, PIECES)
            def _(j):
                sum_in(own, r, j)
                sum_out(own, r, j)

            total = (
                branch[half(r)]
                + from_in[own, half(r)].astype(jnp.float32)
                + from_out[own, half(r)].astype(jnp.float32)
            )
            yield_out(half(r), total)

        for r in range(HALVES + 1):
            for b in (own, b0):
                mid_in(b, r).wait_send()
            for b in (own, b2, b3):
                mid_out(b, r).wait_send()

        @pl.loop(0, PIECES)
        def _(j):
            for r in range(HALVES):
                mid_give_in(b2, r, j).wait_send()
                mid_give_in(b3, r, j).wait_send()
                mid_give_out(b0, r, j).wait_send()

    @pl.when(sp < sp_size - 1)
    def _():
        edge_copy(0).wait_send()
        edge_copy(1).wait_send()

    proj_copy.wait_send()
    conv_copy(0).wait_send()
    conv_copy(1).wait_send()
    for j in range(PIECES):
        part_copy(j).wait_send()
    for n in range(count):
        x_hop(n).wait_send()
        near_hop(n, tp).wait_send()
        far_hop(n, tp).wait_send()
        relay_hop(n, far).wait_send()


def fused_layer(
    x_in, gate_b, gate_c, conv_taps, out_proj, mix_gain, resid, pre_gain, expert_gate, expert_up,
    expert_down, shared_gate, shared_up, shared_down, post_gain, routes, route_weights,
):
    experts = lax.axis_size("sp")
    line = experts // 2
    all_rows, channels = x_in.shape
    rows, width = resid.shape
    hid = expert_gate.shape[2]
    shared_hid = shared_gate.shape[1]
    dma = pltpu.SemaphoreType.DMA
    count = 2 * HALVES + PIECES
    bf, f32 = jnp.bfloat16, jnp.float32
    vmem = pl.BlockSpec(memory_space=pltpu.VMEM)
    hbm = pl.BlockSpec(memory_space=pltpu.HBM)
    lanes = 128 * (-(-experts // 128))
    pad = 16 * (-(-(conv_taps.shape[0] - 1) // 16))
    top = routes.shape[1]
    return pl.pallas_call(
        functools.partial(layer_kernel, line),
        out_shape=jax.ShapeDtypeStruct((rows, width), bf),
        in_specs=[hbm] * 17,
        out_specs=vmem,
        scratch_shapes=[
            pltpu.VMEM((all_rows, channels), bf),
            pltpu.VMEM((all_rows, channels), bf),
            pltpu.VMEM((all_rows, channels), bf),
            pltpu.VMEM(conv_taps.shape, bf),
            pltpu.VMEM((rows, width), bf),
            pltpu.VMEM((width,), bf),
            pltpu.VMEM((width,), bf),
            pltpu.VMEM((width,), bf),
            pltpu.VMEM((top, rows), jnp.int32),
            pltpu.VMEM((top, rows), f32),
            pltpu.VMEM((pad, channels), bf),
            pltpu.VMEM((pad, channels), bf),
            pltpu.VMEM((pad + all_rows, channels), f32),
            pltpu.VMEM((all_rows, channels), bf),
            pltpu.VMEM((2, rows, channels), bf),
            pltpu.VMEM((2, channels, width), bf),
            pltpu.VMEM((rows, width), bf),
            pltpu.VMEM((rows, width), bf),
            pltpu.VMEM((rows, width), f32),
            pltpu.VMEM((rows, width), bf),
            pltpu.VMEM((2, width, hid), bf),
            pltpu.VMEM((2, width, hid), bf),
            pltpu.VMEM((2 * hid, width), bf),
            pltpu.VMEM((width, shared_hid), bf),
            pltpu.VMEM((width, shared_hid), bf),
            pltpu.VMEM((shared_hid, width), bf),
            pltpu.VMEM((line, rows, width), bf),
            pltpu.VMEM((line, rows, lanes), f32),
            pltpu.VMEM((line, rows, 2 * hid), bf),
            pltpu.VMEM((rows, shared_hid), bf),
            pltpu.VMEM((rows, width), f32),
            pltpu.VMEM((line, rows, width), bf),
            pltpu.VMEM((line, rows, width), bf),
            pltpu.VMEM((line, rows, width), bf),
            dma((17,)),
            dma((2,)),
            dma((2,)),
            dma((1,)),
            dma((1,)),
            dma((2,)),
            dma((2,)),
            dma((PIECES,)),
            dma((PIECES,)),
        ]
        + [dma((count,))] * 8
        + [dma((line, HALVES + 1))] * 4
        + [dma((line, HALVES, PIECES))] * 4,
        compiler_params=pltpu.CompilerParams(
            collective_id=0, has_side_effects=True, vmem_limit_bytes=60 * 1024 * 1024
        ),
    )(
        x_in, gate_b, gate_c, conv_taps, resid, mix_gain, pre_gain, post_gain,
        routes.T, route_weights.T, out_proj, expert_gate, expert_up, expert_down,
        shared_gate, shared_up, shared_down,
    )


def passed_along(shard, axis, by):
    size = lax.axis_size(axis)
    pairs = [(i, i + by) for i in range(size) if 0 <= i + by < size]
    return lax.ppermute(shard, axis, pairs)


def body(
    x_in,
    gate_b,
    gate_c,
    conv_taps,
    out_proj,
    mix_gain,
    resid,
    pre_gain,
    expert_gate,
    expert_up,
    expert_down,
    shared_gate,
    shared_up,
    shared_down,
    post_gain,
    routes,
    route_weights,
):
    group = lax.axis_size("sp")
    wide_slots = 3 * resid.shape[0] * routes.shape[1] // group
    if wide_slots > resid.shape[0] and group == 2 * 2 * 2 and lax.axis_size("tp") == 2 * 2:
        return fused_layer(
            x_in, gate_b, gate_c, conv_taps, out_proj, mix_gain, resid, pre_gain, expert_gate,
            expert_up, expert_down, shared_gate, shared_up, shared_down, post_gain, routes,
            route_weights,
        )
    row_count = x_in.shape[0]
    channels = x_in.shape[1]
    reach = conv_taps.shape[0] - 1
    edge_rows = jnp.concatenate([x_in[row_count - reach :], gate_c[row_count - reach :]], 1)
    arrived_edge = passed_along(edge_rows, "sp", 1)
    inputs = jnp.concatenate([arrived_edge[:, :channels], x_in], 0).astype(jnp.float32)
    gate_rows = jnp.concatenate([arrived_edge[:, channels:], gate_c], 0).astype(jnp.float32)
    mixed_in = inputs * gate_rows
    taps = conv_taps.astype(jnp.float32)
    convolved = jnp.zeros((row_count, channels), jnp.float32)
    for index in range(reach + 1):
        convolved = convolved + taps[index][None, :] * mixed_in[index : index + row_count]
    conv_out = (gate_b.astype(jnp.float32) * convolved).astype(jnp.bfloat16)
    width_all = out_proj.shape[1]
    full_rows = lax.all_to_all(conv_out, "tp", split_axis=0, concat_axis=1, tiled=True)
    projected = jnp.dot(
        full_rows,
        lax.all_gather(out_proj, "tp", axis=0, tiled=True),
        preferred_element_type=jnp.float32,
    )
    row_scale = lax.rsqrt(jnp.mean(projected * projected, axis=1, keepdims=True) + epsilon)
    resid1 = (
        resid.astype(jnp.float32) + projected * row_scale * mix_gain.astype(jnp.float32)
    ).astype(jnp.bfloat16)
    wide_resid = resid1.astype(jnp.float32)
    normed = (
        wide_resid
        * lax.rsqrt(jnp.mean(wide_resid * wide_resid, axis=1, keepdims=True) + epsilon)
        * pre_gain.astype(jnp.float32)
    ).astype(jnp.bfloat16)
    experts = lax.axis_size("sp")
    local_rows = resid.shape[0]
    top_count = routes.shape[1]
    capacity = 3 * local_rows * top_count // (2 * experts)
    flat_ids = routes.reshape(-1)
    onehot = (flat_ids[:, None] == jnp.arange(experts, dtype=jnp.int32)[None, :]).astype(jnp.int32)
    before = jnp.cumsum(onehot, axis=0) - onehot
    position = jnp.sum(before * onehot, axis=1)
    slot_index = flat_ids * capacity + position
    outgoing = (
        jnp.zeros((experts * capacity, width_all), jnp.bfloat16)
        .at[slot_index]
        .set(jnp.repeat(normed, top_count, axis=0))
    )
    received = lax.all_to_all(
        outgoing.reshape(experts, capacity, width_all),
        "sp",
        split_axis=0,
        concat_axis=0,
        tiled=True,
    )
    arrived = received.reshape(experts * capacity, width_all)
    gate_h = jnp.dot(arrived, expert_gate[0], preferred_element_type=jnp.float32)
    up_h = jnp.dot(arrived, expert_up[0], preferred_element_type=jnp.float32)
    hidden = (jax.nn.silu(gate_h) * up_h).astype(jnp.bfloat16)
    expert_out = jnp.dot(hidden, expert_down[0], preferred_element_type=jnp.float32).astype(
        jnp.bfloat16
    )
    returned = lax.all_to_all(
        expert_out.reshape(experts, capacity, width_all),
        "sp",
        split_axis=0,
        concat_axis=0,
        tiled=True,
    )
    returned = returned.reshape(experts * capacity, width_all)
    picked = returned[slot_index].astype(jnp.float32).reshape(local_rows, top_count, width_all)
    routed = jnp.einsum("tk,tkd->td", route_weights, picked)
    shared_g = jnp.dot(normed, shared_gate, preferred_element_type=jnp.float32)
    shared_u = jnp.dot(normed, shared_up, preferred_element_type=jnp.float32)
    shared_hidden = (jax.nn.silu(shared_g) * shared_u).astype(jnp.bfloat16)
    shared_out = jnp.dot(shared_hidden, shared_down, preferred_element_type=jnp.float32)
    branch = routed + shared_out
    factor = lax.rsqrt(jnp.mean(branch * branch, axis=1, keepdims=True) + epsilon)
    return (wide_resid + branch * factor * post_gain.astype(jnp.float32)[None, :]).astype(
        jnp.bfloat16
    )


def solution(mesh):
    return jax.shard_map(
        body,
        mesh=mesh,
        in_specs=(
            P("sp", "tp"),
            P("sp", "tp"),
            P("sp", "tp"),
            P(None, "tp"),
            P("tp", None),
            P(),
            P(("sp", "tp"), None),
            P(),
            P("sp", None, None),
            P("sp", None, None),
            P("sp", None, None),
            P(),
            P(),
            P(),
            P(),
            P(("sp", "tp"), None),
            P(("sp", "tp"), None),
        ),
        out_specs=P(("sp", "tp"), None),
        check_vma=False,
    )
```

```python
import functools

import jax
import jax.numpy as jnp
from jax import lax
from jax.experimental import pallas as pl
from jax.experimental.pallas import tpu as pltpu

P = jax.sharding.PartitionSpec
MESH = pl.DeviceIdType.MESH
epsilon = 1e-06
PIECES = 4
HALVES = 2
DIRECT = (3, 7)
TABLE = HALVES


def layer_kernel(
    line,
    x_hbm,
    gate_b_hbm,
    gate_c_hbm,
    taps_hbm,
    resid_hbm,
    mix_hbm,
    pre_hbm,
    post_hbm,
    routes_hbm,
    weights_hbm,
    proj_ref,
    eg_ref,
    eu_ref,
    ed_ref,
    sg_ref,
    su_ref,
    sd_ref,
    out_ref,
    x_ref,
    gate_b_ref,
    gate_c_ref,
    taps_ref,
    resid_ref,
    mix_ref,
    pre_ref,
    post_ref,
    routes_ref,
    weights_ref,
    edge_x,
    edge_c,
    mixed,
    conv,
    conv_near,
    proj,
    part_out,
    part_in,
    projected,
    resid1,
    w_gate,
    w_up,
    w_down,
    s_gate,
    s_up,
    s_down,
    blocks,
    shares,
    hidden,
    shared_hidden,
    branch,
    outgoing,
    from_out,
    from_in,
    out_v,
    load_sem,
    out_sem,
    e_send,
    e_recv,
    p_send,
    p_recv,
    c_send,
    c_recv,
    f_send,
    f_recv,
    wx_send,
    wx_recv,
    wn_send,
    wn_recv,
    wf_send,
    wf_recv,
    wr_send,
    wr_recv,
    gi_send,
    go_send,
    gi_recv,
    go_recv,
    ri_send,
    ro_send,
    ri_recv,
    ro_recv,
):
    sp = lax.axis_index("sp")
    tp = lax.axis_index("tp")
    sp_size = lax.axis_size("sp")
    tp_size = lax.axis_size("tp")
    z = sp // 2
    x = sp % 2
    last = line - 1
    mate = z * 2 + 1 - x
    near = (tp // 2) * 2 + 1 - tp % 2
    far = (tp + 2) % tp_size
    near_far = (near + 2) % tp_size
    upper = z // (line // 2)
    inward_step = 1 - 2 * upper
    level = upper * last + inward_step * z
    inward = ((z + inward_step) * 2 + x, tp)
    outward = ((z - inward_step) * 2 + x, tp)

    def rel(k):
        return upper * last + inward_step * k

    rows, width = resid_ref.shape
    half_rows = rows // HALVES
    hid = w_gate.shape[2]
    shared_hid = s_gate.shape[1]
    part_cols = width // PIECES

    barrier = pltpu.get_barrier_semaphore()

    def greet(device):
        pl.semaphore_signal(barrier, inc=1, device_id=device, device_id_type=MESH)

    greet((mate, tp))
    greet((sp, near))
    greet((sp, far))

    @pl.when(z > 0)
    def _():
        greet((sp - 2, tp))

    @pl.when(z < last)
    def _():
        greet((sp + 2, tp))

    @pl.when((x == 1) & (z < last))
    def _():
        greet((sp + 1, tp))

    @pl.when((x == 0) & (z > 0))
    def _():
        greet((sp - 1, tp))

    pairs = (
        (x_hbm, x_ref),
        (gate_c_hbm, gate_c_ref),
        (proj_ref, proj.at[0]),
        (gate_b_hbm, gate_b_ref),
        (taps_hbm, taps_ref),
        (routes_hbm, routes_ref),
        (weights_hbm, weights_ref),
        (resid_hbm, resid_ref),
        (mix_hbm, mix_ref),
        (pre_hbm, pre_ref),
        (eg_ref.at[0], w_gate.at[0]),
        (eu_ref.at[0], w_up.at[0]),
        (sg_ref, s_gate),
        (su_ref, s_up),
        (ed_ref.at[0], w_down.at[pl.ds(0, hid)]),
        (sd_ref, s_down),
        (post_hbm, post_ref),
    )
    loads = [pltpu.make_async_copy(src, dst, load_sem.at[n]) for n, (src, dst) in enumerate(pairs)]
    for load in loads:
        load.start()

    all_rows, channels = x_ref.shape
    reach = taps_ref.shape[0] - 1
    pad = edge_x.shape[0]

    def edge_copy(n):
        source, landing = ((x_ref, edge_x), (gate_c_ref, edge_c))[n]
        return pltpu.make_async_remote_copy(
            src_ref=source.at[pl.ds(all_rows - pad, pad)],
            dst_ref=landing,
            send_sem=e_send.at[n],
            recv_sem=e_recv.at[n],
            device_id=((sp + 1) % sp_size, tp),
            device_id_type=MESH,
        )

    proj_copy = pltpu.make_async_remote_copy(
        src_ref=proj.at[0],
        dst_ref=proj.at[1],
        send_sem=p_send.at[0],
        recv_sem=p_recv.at[0],
        device_id=(sp, near),
        device_id_type=MESH,
    )

    def block_rows(owner):
        return pl.ds(pl.multiple_of(owner * rows, rows), rows)

    def conv_copy(n):
        return pltpu.make_async_remote_copy(
            src_ref=conv.at[block_rows((near, near_far)[n])],
            dst_ref=conv_near.at[n],
            send_sem=c_send.at[n],
            recv_sem=c_recv.at[n],
            device_id=(sp, near),
            device_id_type=MESH,
        )

    def chunk(j):
        return pl.ds(pl.multiple_of(j * part_cols, part_cols), part_cols)

    def half(r):
        return pl.ds(r * half_rows, half_rows)

    def part_copy(j):
        return pltpu.make_async_remote_copy(
            src_ref=part_out.at[:, chunk(j)],
            dst_ref=part_in.at[:, chunk(j)],
            send_sem=f_send.at[j],
            recv_sem=f_recv.at[j],
            device_id=(sp, far),
            device_id_type=MESH,
        )

    pieces = []
    for ref, held in ((eg_ref, w_gate), (eu_ref, w_up)):
        for h in range(HALVES):
            pieces.append((ref, held, h))
    for j in range(PIECES):
        pieces.append((ed_ref, w_down, j))
    count = len(pieces)

    def cut(n, owner):
        ref, held, h = pieces[n]
        if held is w_down:
            size = hid // tp_size
            begin = pl.multiple_of(owner * size, size)
            return (
                ref.at[0, pl.ds(begin, size), chunk(h)],
                held.at[pl.ds(pl.multiple_of(hid + begin, size), size), chunk(h)],
            )
        size = ref.shape[1] // tp_size // HALVES
        where = pl.ds(pl.multiple_of((owner * HALVES + h) * size, size), size)
        return ref.at[0, where], held.at[1, where]

    def hop(n, owner, target, send, recv, first=False):
        source, landing = cut(n, owner)
        return pltpu.make_async_remote_copy(
            src_ref=source if first else landing,
            dst_ref=landing,
            send_sem=send.at[n],
            recv_sem=recv.at[n],
            device_id=target,
            device_id_type=MESH,
        )

    def x_hop(n):
        return hop(n, tp, (mate, tp), wx_send, wx_recv, True)

    def near_hop(n, owner):
        return hop(n, owner, (sp, near), wn_send, wn_recv)

    def far_hop(n, owner):
        return hop(n, owner, (sp, far), wf_send, wf_recv)

    def direct_hop(n):
        return hop(n, far, (mate, tp), wf_send, wf_recv, True)

    def relay_hop(n, owner):
        return hop(n, owner, (sp, near), wr_send, wr_recv)

    def spread(n):
        with jax.named_scope("w_x"):
            x_hop(n).wait_recv()
        if n not in DIRECT:
            far_hop(n, tp).start()
        near_hop(n, tp).start()

    def relay(n):
        with jax.named_scope("w_far"):
            far_hop(n, far).wait_recv()
        relay_hop(n, far).start()

    def ready(n):
        with jax.named_scope("w_ready"):
            near_hop(n, near).wait_recv()
            relay_hop(n, near_far).wait_recv()

    def block_copy(b, r, target, send, recv):
        ref = shares.at[b] if r == TABLE else blocks.at[b, half(r)]
        return pltpu.make_async_remote_copy(
            src_ref=ref,
            dst_ref=ref,
            send_sem=send.at[b, r],
            recv_sem=recv.at[b, r],
            device_id=target,
            device_id_type=MESH,
        )

    def edge_in(b, r):
        return block_copy(b, r, inward, gi_send, go_recv)

    def mid_in(b, r):
        return block_copy(b, r, inward, gi_send, gi_recv)

    def mid_out(b, r):
        return block_copy(b, r, outward, go_send, gi_recv)

    def got_in(b, r):
        with jax.named_scope("w_gi"):
            block_copy(b, r, inward, gi_send, gi_recv).wait_recv()

    def got_out(b, r):
        with jax.named_scope("w_go"):
            block_copy(b, r, outward, go_send, go_recv).wait_recv()

    def sum_copy(b, r, j, landing, target, send, recv):
        return pltpu.make_async_remote_copy(
            src_ref=outgoing.at[b, half(r), chunk(j)],
            dst_ref=landing.at[b, half(r), chunk(j)],
            send_sem=send.at[b, r, j],
            recv_sem=recv.at[b, r, j],
            device_id=target,
            device_id_type=MESH,
        )

    def edge_give(b, r, j):
        return sum_copy(b, r, j, from_out, inward, ri_send, ro_recv)

    def mid_give_in(b, r, j):
        return sum_copy(b, r, j, from_in, inward, ri_send, ri_recv)

    def mid_give_out(b, r, j):
        return sum_copy(b, r, j, from_in, outward, ro_send, ri_recv)

    def sum_in(b, r, j):
        with jax.named_scope("w_ri"):
            sum_copy(b, r, j, from_in, inward, ri_send, ri_recv).wait_recv()

    def sum_out(b, r, j):
        with jax.named_scope("w_ro"):
            sum_copy(b, r, j, from_out, outward, ro_send, ro_recv).wait_recv()

    with jax.named_scope("w_barrier"):
        met = 3 + jnp.where(z > 0, 1, 0) + jnp.where(z < last, 1, 0)
        met += jnp.where(jnp.where(x == 1, z < last, z > 0), 1, 0)
        pl.semaphore_wait(barrier, met)

    loads[0].wait()
    loads[1].wait()

    @pl.when(sp < sp_size - 1)
    def _():
        edge_copy(0).start()
        edge_copy(1).start()

    for n in range(count):
        x_hop(n).start()
        if n - 1 in DIRECT or n == count - 1:
            direct_hop(min(n, DIRECT[-1]) if n == count - 1 else n - 1).start()

    loads[2].wait()
    proj_copy.start()
    mixed[pad:] = x_ref[...].astype(jnp.float32) * gate_c_ref[...].astype(jnp.float32)
    loads[3].wait()
    loads[4].wait()

    with jax.named_scope("w_edge"):

        @pl.when(sp > 0)
        def _():
            edge_copy(0).wait_recv()
            edge_copy(1).wait_recv()
            mixed[:pad] = edge_x[...].astype(jnp.float32) * edge_c[...].astype(jnp.float32)

        @pl.when(sp == 0)
        def _():
            mixed[:pad] = jnp.zeros((pad, channels), jnp.float32)

    convolved = jnp.zeros((all_rows, channels), jnp.float32)
    for k in range(reach + 1):
        begin = pad - reach + k
        convolved += taps_ref[k : k + 1].astype(jnp.float32) * mixed[begin : begin + all_rows]
    conv[...] = (gate_b_ref[...].astype(jnp.float32) * convolved).astype(jnp.bfloat16)
    conv_copy(1).start()
    conv_copy(0).start()

    def project(n, owner, cols):
        return jnp.dot(
            conv[block_rows(owner)], proj[0, :, cols], preferred_element_type=jnp.float32
        ) + jnp.dot(conv_near[n], proj[1, :, cols], preferred_element_type=jnp.float32)

    with jax.named_scope("w_conv"):
        proj_copy.wait_recv()
        conv_copy(1).wait_recv()

    @pl.loop(0, PIECES)
    def _(j):
        part_out[:, chunk(j)] = project(1, far, chunk(j)).astype(jnp.bfloat16)
        part_copy(j).start()

    loads[5].wait()
    loads[6].wait()
    lanes = lax.broadcasted_iota(jnp.int32, (rows, shares.shape[2]), 1)
    names = lax.broadcasted_iota(jnp.int32, (shares.shape[2], rows), 0)
    table = jnp.zeros((shares.shape[2], rows), jnp.float32)
    for k in range(routes_ref.shape[0]):
        table += jnp.where(names == routes_ref[k : k + 1], weights_ref[k : k + 1], 0.0)
    shares[z] = table.T

    own = z

    @pl.when(level == 0)
    def _():
        edge_in(own, TABLE).start()

    @pl.when(level == 1)
    def _():
        mid_in(own, TABLE).start()
        mid_out(own, TABLE).start()

    conv_copy(0).wait_recv()

    @pl.loop(0, PIECES)
    def _(j):
        projected[:, chunk(j)] = project(0, tp, chunk(j))

    spread(0)
    spread(1)
    for load in loads[7:10]:
        load.wait()

    with jax.named_scope("w_part"):

        @pl.loop(0, PIECES)
        def _(j):
            part_copy(j).wait_recv()
            projected[:, chunk(j)] += part_in[:, chunk(j)].astype(jnp.float32)

    with jax.named_scope("norm"):
        for r in range(HALVES):
            part = half(r)
            block = projected[part]
            scale = lax.rsqrt(jnp.mean(block * block, axis=1, keepdims=True) + epsilon)
            mid = (
                resid_ref[part].astype(jnp.float32)
                + block * scale * mix_ref[...].astype(jnp.float32).reshape(1, width)
            ).astype(jnp.bfloat16)
            resid1[part] = mid
            wide = mid.astype(jnp.float32)
            normal = lax.rsqrt(jnp.mean(wide * wide, axis=1, keepdims=True) + epsilon)
            blocks[own, part] = (
                wide * normal * pre_ref[...].astype(jnp.float32).reshape(1, width)
            ).astype(jnp.bfloat16)

            @pl.when(level == 0)
            def _():
                edge_in(own, r).start()

            @pl.when(level == 1)
            def _():
                mid_in(own, r).start()
                mid_out(own, r).start()

    spread(2)

    def hide(b, begin, size, e):
        part = pl.ds(begin, size)
        expert = z * 2 + x + e * (1 - 2 * x)
        share = jnp.sum(
            jnp.where(lanes[:size] == expert, shares[b, part], 0.0), axis=1, keepdims=True
        )

        @pl.loop(0, hid // 256)
        def _(j):
            cols = pl.ds(pl.multiple_of(j * 256, 256), 256)
            gate = jnp.dot(blocks[b, part], w_gate[e, :, cols], preferred_element_type=jnp.float32)
            up = jnp.dot(blocks[b, part], w_up[e, :, cols], preferred_element_type=jnp.float32)
            kept = pl.ds(pl.multiple_of(e * hid + j * 256, 256), 256)
            hidden[b, part, kept] = (jax.nn.silu(gate) * up * share).astype(jnp.bfloat16)

    def hide_all(b, e):
        hide(b, 0, rows, e)

    def hide_half(b, r):
        hide(b, r * half_rows, half_rows, 0)
        hide(b, r * half_rows, half_rows, 1)

    def down(b, part, j):
        return jnp.dot(
            hidden[b, part], w_down[:, chunk(j)], preferred_element_type=jnp.float32
        )

    def give(b, r, j, arrived, send):
        made = down(b, half(r), j)
        if arrived is not None:
            made += arrived[b, half(r), chunk(j)].astype(jnp.float32)
        outgoing[b, half(r), chunk(j)] = made.astype(jnp.bfloat16)
        send(b, r, j).start()

    def shared_up_to_hidden():
        s_g = jnp.dot(blocks[own], s_gate[...], preferred_element_type=jnp.float32)
        s_u = jnp.dot(blocks[own], s_up[...], preferred_element_type=jnp.float32)
        shared_hidden[...] = (jax.nn.silu(s_g) * s_u).astype(jnp.bfloat16)

    def own_branch():
        @pl.loop(0, PIECES)
        def _(j):
            branch[:, chunk(j)] = down(own, pl.ds(0, rows), j) + jnp.dot(
                shared_hidden[...], s_down[:, chunk(j)], preferred_element_type=jnp.float32
            )

    def out_copy(r):
        return pltpu.make_async_copy(out_v.at[half(r)], out_ref.at[half(r)], out_sem.at[r])

    def yield_out(r, total):
        factor = lax.rsqrt(jnp.mean(total * total, axis=1, keepdims=True) + epsilon)
        out_v[half(r)] = (
            resid1[half(r)].astype(jnp.float32)
            + total * factor * post_ref[...].astype(jnp.float32).reshape(1, width)
        ).astype(jnp.bfloat16)
        out_copy(r).start()

    def settle():
        @pl.when(sp < sp_size - 1)
        def _():
            edge_copy(0).wait_send()
            edge_copy(1).wait_send()

        proj_copy.wait_send()
        conv_copy(0).wait_send()
        conv_copy(1).wait_send()
        for j in range(PIECES):
            part_copy(j).wait_send()
        for n in range(count):
            x_hop(n).wait_send()
            near_hop(n, tp).wait_send()
            far_hop(n, tp).wait_send()
            relay_hop(n, far).wait_send()

    for load in loads[10:14]:
        load.wait()
    hide_all(own, 0)
    shared_up_to_hidden()
    relay(0)
    spread(3)
    spread(4)
    for load in loads[14:]:
        load.wait()

    @pl.when(level == 0)
    def _():
        b1, b2, b3 = rel(1), rel(2), rel(3)
        got_in(b1, TABLE)
        got_in(b1, 0)
        hide(b1, 0, half_rows, 0)
        relay(1)
        got_in(b1, 1)
        hide(b1, half_rows, half_rows, 0)
        relay(3)
        relay(2)
        spread(5)
        for n in range(4):
            ready(n)
        hide_all(b1, 1)
        relay(4)
        spread(6)
        ready(4)
        for r in range(HALVES):
            give(b1, r, 0, None, edge_give)
        got_in(b2, TABLE)
        got_in(b2, 0)
        hide_half(b2, 0)
        give(b2, 0, 0, None, edge_give)
        relay(5)
        spread(7)
        ready(5)
        for r in range(HALVES):
            give(b1, r, 1, None, edge_give)
        give(b2, 0, 1, None, edge_give)
        relay(6)
        relay(7)
        got_in(b2, 1)
        hide_half(b2, 1)

        @pl.loop(0, 2)
        def _(j):
            give(b2, 1, j, None, edge_give)

        ready(6)
        ready(7)

        @pl.loop(2, PIECES)
        def _(j):
            give(b2, 0, j, None, edge_give)

        hide_all(own, 1)
        got_in(b3, TABLE)
        for r in range(HALVES):
            got_in(b3, r)
            hide_half(b3, r)

            @pl.loop(0, PIECES)
            def _(j):
                give(b3, r, j, None, edge_give)

        @pl.loop(2, PIECES)
        def _(j):
            give(b2, 1, j, None, edge_give)

        @pl.loop(2, PIECES)
        def _(j):
            for r in range(HALVES):
                give(b1, r, j, None, edge_give)

        own_branch()
        settle()
        for r in range(HALVES + 1):
            edge_in(own, r).wait_send()

        @pl.loop(0, PIECES)
        def _(j):
            for b in (b2, b3):
                for r in range(HALVES):
                    edge_give(b, r, j).wait_send()

        for r in range(HALVES):

            @pl.loop(0, PIECES)
            def _(j):
                sum_in(own, r, j)

            total = branch[half(r)] + from_in[own, half(r)].astype(jnp.float32)
            yield_out(r, total)

        @pl.loop(0, PIECES)
        def _(j):
            for r in range(HALVES):
                edge_give(b1, r, j).wait_send()

    @pl.when(level == 1)
    def _():
        b0, b2, b3 = rel(0), rel(2), rel(3)

        def pass_in(r):
            got_out(b0, r)
            mid_in(b0, r).start()

        def pass_out(b, r):
            got_in(b, r)
            mid_out(b, r).start()

        pass_in(TABLE)
        pass_out(b2, TABLE)
        pass_in(0)
        pass_out(b2, 0)
        pass_out(b3, TABLE)
        relay(1)
        pass_in(1)
        pass_out(b2, 1)
        relay(3)
        hide_all(b0, 0)
        relay(2)
        spread(5)
        hide_all(b2, 0)
        for n in range(4):
            ready(n)
        relay(4)
        spread(6)
        hide_all(b2, 1)
        pass_out(b3, 0)
        relay(5)
        spread(7)
        hide_all(own, 1)
        relay(6)
        relay(7)
        pass_out(b3, 1)
        hide_all(b3, 0)
        hide_all(b3, 1)
        hide_all(b0, 1)
        for n in range(4, count):
            ready(n)

        def give_in(b, r, j):
            sum_out(b, r, j)
            give(b, r, j, from_out, mid_give_in)

        def give_out(r, j):
            sum_in(b0, r, j)
            give(b0, r, j, from_in, mid_give_out)

        give_in(b2, 0, 0)
        give_in(b2, 0, 1)
        own_branch()

        @pl.loop(0, 2)
        def _(j):
            give_in(b2, 1, j)

        @pl.loop(2, PIECES)
        def _(j):
            give_in(b2, 0, j)

        @pl.loop(0, PIECES)
        def _(j):
            give_in(b3, 0, j)

        settle()

        @pl.loop(0, PIECES)
        def _(j):
            give_out(0, j)
            give_in(b3, 1, j)

        give_out(1, 0)
        give_out(1, 1)

        @pl.loop(2, PIECES)
        def _(j):
            give_in(b2, 1, j)
            give_out(1, j)

        for r in range(HALVES + 1):
            for b in (own, b0):
                mid_in(b, r).wait_send()
            for b in (own, b2, b3):
                mid_out(b, r).wait_send()

        @pl.loop(0, PIECES)
        def _(j):
            mid_give_in(b2, 0, j).wait_send()
            mid_give_in(b3, 0, j).wait_send()
            mid_give_in(b3, 1, j).wait_send()

        for r in range(HALVES):

            @pl.loop(0, PIECES)
            def _(j):
                sum_in(own, r, j)
                sum_out(own, r, j)

            total = (
                branch[half(r)]
                + from_in[own, half(r)].astype(jnp.float32)
                + from_out[own, half(r)].astype(jnp.float32)
            )
            yield_out(r, total)

        @pl.loop(0, PIECES)
        def _(j):
            mid_give_in(b2, 1, j).wait_send()
            for r in range(HALVES):
                mid_give_out(b0, r, j).wait_send()

    for r in range(HALVES):
        out_copy(r).wait()


def fused_layer(
    x_in, gate_b, gate_c, conv_taps, out_proj, mix_gain, resid, pre_gain, expert_gate, expert_up,
    expert_down, shared_gate, shared_up, shared_down, post_gain, routes, route_weights,
):
    experts = lax.axis_size("sp")
    line = experts // 2
    all_rows, channels = x_in.shape
    rows, width = resid.shape
    hid = expert_gate.shape[2]
    shared_hid = shared_gate.shape[1]
    dma = pltpu.SemaphoreType.DMA
    count = 2 * HALVES + PIECES
    bf, f32 = jnp.bfloat16, jnp.float32
    hbm = pl.BlockSpec(memory_space=pltpu.HBM)
    lanes = 128 * (-(-experts // 128))
    pad = 16 * (-(-(conv_taps.shape[0] - 1) // 16))
    top = routes.shape[1]
    return pl.pallas_call(
        functools.partial(layer_kernel, line),
        out_shape=jax.ShapeDtypeStruct((rows, width), bf),
        in_specs=[hbm] * 17,
        out_specs=hbm,
        scratch_shapes=[
            pltpu.VMEM((all_rows, channels), bf),
            pltpu.VMEM((all_rows, channels), bf),
            pltpu.VMEM((all_rows, channels), bf),
            pltpu.VMEM(conv_taps.shape, bf),
            pltpu.VMEM((rows, width), bf),
            pltpu.VMEM((width,), bf),
            pltpu.VMEM((width,), bf),
            pltpu.VMEM((width,), bf),
            pltpu.VMEM((top, rows), jnp.int32),
            pltpu.VMEM((top, rows), f32),
            pltpu.VMEM((pad, channels), bf),
            pltpu.VMEM((pad, channels), bf),
            pltpu.VMEM((pad + all_rows, channels), f32),
            pltpu.VMEM((all_rows, channels), bf),
            pltpu.VMEM((2, rows, channels), bf),
            pltpu.VMEM((2, channels, width), bf),
            pltpu.VMEM((rows, width), bf),
            pltpu.VMEM((rows, width), bf),
            pltpu.VMEM((rows, width), f32),
            pltpu.VMEM((rows, width), bf),
            pltpu.VMEM((2, width, hid), bf),
            pltpu.VMEM((2, width, hid), bf),
            pltpu.VMEM((2 * hid, width), bf),
            pltpu.VMEM((width, shared_hid), bf),
            pltpu.VMEM((width, shared_hid), bf),
            pltpu.VMEM((shared_hid, width), bf),
            pltpu.VMEM((line, rows, width), bf),
            pltpu.VMEM((line, rows, lanes), f32),
            pltpu.VMEM((line, rows, 2 * hid), bf),
            pltpu.VMEM((rows, shared_hid), bf),
            pltpu.VMEM((rows, width), f32),
            pltpu.VMEM((line, rows, width), bf),
            pltpu.VMEM((line, rows, width), bf),
            pltpu.VMEM((line, rows, width), bf),
            pltpu.VMEM((rows, width), bf),
            dma((17,)),
            dma((HALVES,)),
            dma((2,)),
            dma((2,)),
            dma((1,)),
            dma((1,)),
            dma((2,)),
            dma((2,)),
            dma((PIECES,)),
            dma((PIECES,)),
        ]
        + [dma((count,))] * 8
        + [dma((line, HALVES + 1))] * 4
        + [dma((line, HALVES, PIECES))] * 4,
        compiler_params=pltpu.CompilerParams(
            collective_id=0, has_side_effects=True, vmem_limit_bytes=60 * 1024 * 1024
        ),
    )(
        x_in, gate_b, gate_c, conv_taps, resid, mix_gain, pre_gain, post_gain,
        routes.T, route_weights.T, out_proj, expert_gate, expert_up, expert_down,
        shared_gate, shared_up, shared_down,
    )


def passed_along(shard, axis, by):
    size = lax.axis_size(axis)
    pairs = [(i, i + by) for i in range(size) if 0 <= i + by < size]
    return lax.ppermute(shard, axis, pairs)


def body(
    x_in,
    gate_b,
    gate_c,
    conv_taps,
    out_proj,
    mix_gain,
    resid,
    pre_gain,
    expert_gate,
    expert_up,
    expert_down,
    shared_gate,
    shared_up,
    shared_down,
    post_gain,
    routes,
    route_weights,
):
    group = lax.axis_size("sp")
    wide_slots = 3 * resid.shape[0] * routes.shape[1] // group
    if wide_slots > resid.shape[0] and group == 2 * 2 * 2 and lax.axis_size("tp") == 2 * 2:
        return fused_layer(
            x_in, gate_b, gate_c, conv_taps, out_proj, mix_gain, resid, pre_gain, expert_gate,
            expert_up, expert_down, shared_gate, shared_up, shared_down, post_gain, routes,
            route_weights,
        )
    row_count = x_in.shape[0]
    channels = x_in.shape[1]
    reach = conv_taps.shape[0] - 1
    edge_rows = jnp.concatenate([x_in[row_count - reach :], gate_c[row_count - reach :]], 1)
    arrived_edge = passed_along(edge_rows, "sp", 1)
    inputs = jnp.concatenate([arrived_edge[:, :channels], x_in], 0).astype(jnp.float32)
    gate_rows = jnp.concatenate([arrived_edge[:, channels:], gate_c], 0).astype(jnp.float32)
    mixed_in = inputs * gate_rows
    taps = conv_taps.astype(jnp.float32)
    convolved = jnp.zeros((row_count, channels), jnp.float32)
    for index in range(reach + 1):
        convolved = convolved + taps[index][None, :] * mixed_in[index : index + row_count]
    conv_out = (gate_b.astype(jnp.float32) * convolved).astype(jnp.bfloat16)
    width_all = out_proj.shape[1]
    full_rows = lax.all_to_all(conv_out, "tp", split_axis=0, concat_axis=1, tiled=True)
    projected = jnp.dot(
        full_rows,
        lax.all_gather(out_proj, "tp", axis=0, tiled=True),
        preferred_element_type=jnp.float32,
    )
    row_scale = lax.rsqrt(jnp.mean(projected * projected, axis=1, keepdims=True) + epsilon)
    resid1 = (
        resid.astype(jnp.float32) + projected * row_scale * mix_gain.astype(jnp.float32)
    ).astype(jnp.bfloat16)
    wide_resid = resid1.astype(jnp.float32)
    normed = (
        wide_resid
        * lax.rsqrt(jnp.mean(wide_resid * wide_resid, axis=1, keepdims=True) + epsilon)
        * pre_gain.astype(jnp.float32)
    ).astype(jnp.bfloat16)
    experts = lax.axis_size("sp")
    local_rows = resid.shape[0]
    top_count = routes.shape[1]
    capacity = 3 * local_rows * top_count // (2 * experts)
    flat_ids = routes.reshape(-1)
    onehot = (flat_ids[:, None] == jnp.arange(experts, dtype=jnp.int32)[None, :]).astype(jnp.int32)
    before = jnp.cumsum(onehot, axis=0) - onehot
    position = jnp.sum(before * onehot, axis=1)
    slot_index = flat_ids * capacity + position
    outgoing = (
        jnp.zeros((experts * capacity, width_all), jnp.bfloat16)
        .at[slot_index]
        .set(jnp.repeat(normed, top_count, axis=0))
    )
    received = lax.all_to_all(
        outgoing.reshape(experts, capacity, width_all),
        "sp",
        split_axis=0,
        concat_axis=0,
        tiled=True,
    )
    arrived = received.reshape(experts * capacity, width_all)
    gate_h = jnp.dot(arrived, expert_gate[0], preferred_element_type=jnp.float32)
    up_h = jnp.dot(arrived, expert_up[0], preferred_element_type=jnp.float32)
    hidden = (jax.nn.silu(gate_h) * up_h).astype(jnp.bfloat16)
    expert_out = jnp.dot(hidden, expert_down[0], preferred_element_type=jnp.float32).astype(
        jnp.bfloat16
    )
    returned = lax.all_to_all(
        expert_out.reshape(experts, capacity, width_all),
        "sp",
        split_axis=0,
        concat_axis=0,
        tiled=True,
    )
    returned = returned.reshape(experts * capacity, width_all)
    picked = returned[slot_index].astype(jnp.float32).reshape(local_rows, top_count, width_all)
    routed = jnp.einsum("tk,tkd->td", route_weights, picked)
    shared_g = jnp.dot(normed, shared_gate, preferred_element_type=jnp.float32)
    shared_u = jnp.dot(normed, shared_up, preferred_element_type=jnp.float32)
    shared_hidden = (jax.nn.silu(shared_g) * shared_u).astype(jnp.bfloat16)
    shared_out = jnp.dot(shared_hidden, shared_down, preferred_element_type=jnp.float32)
    branch = routed + shared_out
    factor = lax.rsqrt(jnp.mean(branch * branch, axis=1, keepdims=True) + epsilon)
    return (wide_resid + branch * factor * post_gain.astype(jnp.float32)[None, :]).astype(
        jnp.bfloat16
    )


def solution(mesh):
    return jax.shard_map(
        body,
        mesh=mesh,
        in_specs=(
            P("sp", "tp"),
            P("sp", "tp"),
            P("sp", "tp"),
            P(None, "tp"),
            P("tp", None),
            P(),
            P(("sp", "tp"), None),
            P(),
            P("sp", None, None),
            P("sp", None, None),
            P("sp", None, None),
            P(),
            P(),
            P(),
            P(),
            P(("sp", "tp"), None),
            P(("sp", "tp"), None),
        ),
        out_specs=P(("sp", "tp"), None),
        check_vma=False,
    )
```

```python
import functools

import jax
import jax.numpy as jnp
from jax import lax
from jax.experimental import pallas as pl
from jax.experimental.pallas import tpu as pltpu

P = jax.sharding.PartitionSpec
MESH = pl.DeviceIdType.MESH
epsilon = 1e-06
PIECES = 4
HALVES = 2
DIRECT = (3, 7)
ORDER = (0, 1, 2, 3, 4, -3, 5, 6, 7, -7)
TABLE = HALVES


def layer_kernel(
    line,
    x_hbm,
    gate_b_hbm,
    gate_c_hbm,
    taps_hbm,
    resid_hbm,
    mix_hbm,
    pre_hbm,
    post_hbm,
    routes_hbm,
    weights_hbm,
    proj_ref,
    eg_ref,
    eu_ref,
    ed_ref,
    sg_ref,
    su_ref,
    sd_ref,
    out_ref,
    x_ref,
    gate_b_ref,
    gate_c_ref,
    taps_ref,
    resid_ref,
    mix_ref,
    pre_ref,
    post_ref,
    routes_ref,
    weights_ref,
    edge_x,
    edge_c,
    mixed,
    conv,
    conv_near,
    proj,
    part_out,
    part_in,
    projected,
    resid1,
    w_gate,
    w_up,
    w_down,
    s_gate,
    s_up,
    s_down,
    blocks,
    shares,
    hidden,
    shared_hidden,
    branch,
    outgoing,
    from_out,
    from_in,
    out_v,
    load_sem,
    out_sem,
    edge_send,
    misc_send,
    spread_send,
    relay_send,
    in_send,
    out_send,
    e_recv,
    p_recv,
    c_recv,
    f_recv,
    wx_recv,
    wn_recv,
    wf_recv,
    wr_recv,
    gi_recv,
    go_recv,
    ri_recv,
    ro_recv,
):
    sp = lax.axis_index("sp")
    tp = lax.axis_index("tp")
    sp_size = lax.axis_size("sp")
    tp_size = lax.axis_size("tp")
    z = sp // 2
    x = sp % 2
    last = line - 1
    mate = z * 2 + 1 - x
    near = (tp // 2) * 2 + 1 - tp % 2
    far = (tp + 2) % tp_size
    near_far = (near + 2) % tp_size
    upper = z // (line // 2)
    inward_step = 1 - 2 * upper
    level = upper * last + inward_step * z
    inward = ((z + inward_step) * 2 + x, tp)
    outward = ((z - inward_step) * 2 + x, tp)

    def rel(k):
        return upper * last + inward_step * k

    rows, width = resid_ref.shape
    half_rows = rows // HALVES
    hid = w_gate.shape[2]
    shared_hid = s_gate.shape[1]
    part_cols = width // PIECES

    barrier = pltpu.get_barrier_semaphore()

    def greet(device):
        pl.semaphore_signal(barrier, inc=1, device_id=device, device_id_type=MESH)

    greet((mate, tp))
    greet((sp, near))
    greet((sp, far))

    @pl.when(z > 0)
    def _():
        greet((sp - 2, tp))

    @pl.when(z < last)
    def _():
        greet((sp + 2, tp))

    @pl.when((x == 1) & (z < last))
    def _():
        greet((sp + 1, tp))

    @pl.when((x == 0) & (z > 0))
    def _():
        greet((sp - 1, tp))

    pairs = (
        (x_hbm, x_ref),
        (gate_c_hbm, gate_c_ref),
        (proj_ref, proj.at[0]),
        (gate_b_hbm, gate_b_ref),
        (taps_hbm, taps_ref),
        (routes_hbm, routes_ref),
        (weights_hbm, weights_ref),
        (resid_hbm, resid_ref),
        (mix_hbm, mix_ref),
        (pre_hbm, pre_ref),
        (eg_ref.at[0], w_gate.at[0]),
        (eu_ref.at[0], w_up.at[0]),
        (sg_ref, s_gate),
        (su_ref, s_up),
        (ed_ref.at[0], w_down.at[pl.ds(0, hid)]),
        (sd_ref, s_down),
        (post_hbm, post_ref),
    )
    loads = [pltpu.make_async_copy(src, dst, load_sem.at[n]) for n, (src, dst) in enumerate(pairs)]
    for load in loads:
        load.start()

    all_rows, channels = x_ref.shape
    reach = taps_ref.shape[0] - 1
    pad = edge_x.shape[0]

    def edge_copy(n):
        source, landing = ((x_hbm, edge_x), (gate_c_hbm, edge_c))[n]
        return pltpu.make_async_remote_copy(
            src_ref=source.at[pl.ds(all_rows - pad, pad)],
            dst_ref=landing,
            send_sem=edge_send.at[0],
            recv_sem=e_recv.at[n],
            device_id=((sp + 1) % sp_size, tp),
            device_id_type=MESH,
        )

    def block_rows(owner):
        return pl.ds(pl.multiple_of(owner * rows, rows), rows)

    def conv_copy(n, k):
        begin, size = ((pad, rows - pad), (0, pad))[k]
        return pltpu.make_async_remote_copy(
            src_ref=conv.at[pl.ds(pl.multiple_of((near, near_far)[n] * rows + begin, pad), size)],
            dst_ref=conv_near.at[n, pl.ds(begin, size)],
            send_sem=misc_send.at[0],
            recv_sem=c_recv.at[n, k],
            device_id=(sp, near),
            device_id_type=MESH,
        )

    def chunk(j):
        return pl.ds(pl.multiple_of(j * part_cols, part_cols), part_cols)

    def half(r):
        return pl.ds(r * half_rows, half_rows)

    def proj_copy(j):
        return pltpu.make_async_remote_copy(
            src_ref=proj.at[0, :, chunk(j)],
            dst_ref=proj.at[1, :, chunk(j)],
            send_sem=misc_send.at[0],
            recv_sem=p_recv.at[j],
            device_id=(sp, near),
            device_id_type=MESH,
        )

    def part_copy(j):
        where = (pl.ds(pad, rows - pad), chunk(j))
        return pltpu.make_async_remote_copy(
            src_ref=part_out.at[where],
            dst_ref=part_in.at[where],
            send_sem=misc_send.at[0],
            recv_sem=f_recv.at[j],
            device_id=(sp, far),
            device_id_type=MESH,
        )

    part_head = pltpu.make_async_remote_copy(
        src_ref=part_out.at[pl.ds(0, pad)],
        dst_ref=part_in.at[pl.ds(0, pad)],
        send_sem=misc_send.at[0],
        recv_sem=f_recv.at[PIECES],
        device_id=(sp, far),
        device_id_type=MESH,
    )

    pieces = []
    for ref, held in ((eg_ref, w_gate), (eu_ref, w_up)):
        for h in range(HALVES):
            pieces.append((ref, held, h))
    for j in range(PIECES):
        pieces.append((ed_ref, w_down, j))
    count = len(pieces)

    def cut(n, owner):
        ref, held, h = pieces[n]
        if held is w_down:
            size = hid // tp_size
            begin = pl.multiple_of(owner * size, size)
            return (
                ref.at[0, pl.ds(begin, size), chunk(h)],
                held.at[pl.ds(pl.multiple_of(hid + begin, size), size), chunk(h)],
            )
        size = ref.shape[1] // tp_size // HALVES
        where = pl.ds(pl.multiple_of((owner * HALVES + h) * size, size), size)
        return ref.at[0, where], held.at[1, where]

    def hop(n, owner, target, send, recv, first=False):
        source, landing = cut(n, owner)
        return pltpu.make_async_remote_copy(
            src_ref=source if first else landing,
            dst_ref=landing,
            send_sem=send.at[0],
            recv_sem=recv,
            device_id=target,
            device_id_type=MESH,
        )

    def late(n):
        return max(0, n - 2 * HALVES + 1)

    def x_hop(n):
        return hop(n, tp, (mate, tp), spread_send, wx_recv.at[n], True)

    def near_hop(n, owner):
        return hop(n, owner, (sp, near), spread_send, wn_recv.at[late(n)])

    def far_hop(n, owner):
        return hop(n, owner, (sp, far), relay_send, wf_recv.at[n])

    def direct_hop(n):
        return hop(n, far, (mate, tp), relay_send, wf_recv.at[n], True)

    def relay_hop(n, owner):
        return hop(n, owner, (sp, near), relay_send, wr_recv.at[late(n)])

    def drain(send, recv, size):
        where = w_down.at[pl.ds(0, size)]
        return pltpu.make_async_remote_copy(
            src_ref=where,
            dst_ref=where,
            send_sem=send.at[0],
            recv_sem=recv.at[0],
            device_id=(sp, near),
            device_id_type=MESH,
        )

    def spread(n):
        with jax.named_scope("w_x"):
            x_hop(n).wait_recv()
        if n not in DIRECT:
            far_hop(n, tp).start()
        near_hop(n, tp).start()

    def relay(n):
        with jax.named_scope("w_far"):
            far_hop(n, far).wait_recv()
        relay_hop(n, far).start()

    def ready(n):
        with jax.named_scope("w_ready"):
            near_hop(n, near).wait_recv()
            relay_hop(n, near_far).wait_recv()

    def ready_both():
        size = 2 * hid // tp_size
        with jax.named_scope("w_ready"):
            drain(spread_send, wn_recv, size).wait_recv()
            drain(relay_send, wr_recv, size).wait_recv()

    def block_copy(b, r, target, send, recv):
        ref = shares.at[b] if r == TABLE else blocks.at[b, half(r)]
        return pltpu.make_async_remote_copy(
            src_ref=ref,
            dst_ref=ref,
            send_sem=send.at[0],
            recv_sem=recv,
            device_id=target,
            device_id_type=MESH,
        )

    def edge_in(r):
        return block_copy(rel(0), r, inward, in_send, go_recv.at[r])

    def mid_in(k, r):
        return block_copy(rel(k), r, inward, in_send, gi_recv.at[last - k - 1, r])

    def mid_out(k, r):
        return block_copy(rel(k), r, outward, out_send, gi_recv.at[k - 1, r])

    def got_in(k, r):
        with jax.named_scope("w_gi"):
            block_copy(rel(k), r, inward, in_send, gi_recv.at[k - 1, r]).wait_recv()

    def got_out(r):
        with jax.named_scope("w_go"):
            block_copy(rel(0), r, outward, out_send, go_recv.at[r]).wait_recv()

    def sum_copy(k, r, j, landing, target, send, recv):
        return pltpu.make_async_remote_copy(
            src_ref=outgoing.at[rel(k), half(r), chunk(j)],
            dst_ref=landing.at[rel(k), half(r), chunk(j)],
            send_sem=send.at[0],
            recv_sem=recv.at[j],
            device_id=target,
            device_id_type=MESH,
        )

    def edge_give(k, r, j):
        return sum_copy(k, r, j, from_out, inward, in_send, ro_recv.at[k - 1, r])

    def mid_give_in(k, r, j):
        return sum_copy(k, r, j, from_in, inward, in_send, ri_recv.at[last - k, r])

    def mid_give_out(k, r, j):
        return sum_copy(k, r, j, from_in, outward, out_send, ri_recv.at[k, r])

    def sum_in(k, r, j):
        with jax.named_scope("w_ri"):
            sum_copy(k, r, j, from_in, inward, in_send, ri_recv.at[k, r]).wait_recv()

    def sum_out(k, r, j):
        with jax.named_scope("w_ro"):
            sum_copy(k, r, j, from_out, outward, out_send, ro_recv.at[k - 1, r]).wait_recv()

    with jax.named_scope("w_barrier"):
        met = 3 + jnp.where(z > 0, 1, 0) + jnp.where(z < last, 1, 0)
        met += jnp.where(jnp.where(x == 1, z < last, z > 0), 1, 0)
        pl.semaphore_wait(barrier, met)

    @pl.when(sp < sp_size - 1)
    def _():
        edge_copy(0).start()
        edge_copy(1).start()

    for n in ORDER:
        if n < 0:
            direct_hop(-n).start()
        else:
            x_hop(n).start()

    loads[2].wait()
    for j in range(PIECES):
        proj_copy(j).start()

    for n in (0, 1, 3, 4):
        loads[n].wait()
    mixed[:pad] = jnp.zeros((pad, channels), jnp.float32)
    mixed[pad:] = x_ref[...].astype(jnp.float32) * gate_c_ref[...].astype(jnp.float32)

    def convolve(size):
        convolved = jnp.zeros((size, channels), jnp.float32)
        for k in range(reach + 1):
            begin = pad - reach + k
            convolved += taps_ref[k : k + 1].astype(jnp.float32) * mixed[begin : begin + size]
        conv[:size] = (gate_b_ref[:size].astype(jnp.float32) * convolved).astype(jnp.bfloat16)

    convolve(all_rows)
    conv_copy(1, 0).start()
    conv_copy(0, 0).start()
    loads[5].wait()
    loads[6].wait()
    lanes = lax.broadcasted_iota(jnp.int32, (rows, shares.shape[2]), 1)
    names = lax.broadcasted_iota(jnp.int32, (shares.shape[2], rows), 0)
    table = jnp.zeros((shares.shape[2], rows), jnp.float32)
    for k in range(routes_ref.shape[0]):
        table += jnp.where(names == routes_ref[k : k + 1], weights_ref[k : k + 1], 0.0)
    own = z
    shares[own] = table.T

    def send_own(r):
        @pl.when(level == 0)
        def _():
            edge_in(r).start()

        @pl.when(level == 1)
        def _():
            mid_in(1, r).start()
            mid_out(1, r).start()

    send_own(TABLE)

    def project(n, owner, cols, begin, size):
        mine = pl.ds(pl.multiple_of(owner * rows + begin, pad), size)
        return jnp.dot(
            conv[mine], proj[0, :, cols], preferred_element_type=jnp.float32
        ) + jnp.dot(
            conv_near[n, begin : begin + size], proj[1, :, cols], preferred_element_type=jnp.float32
        )

    with jax.named_scope("w_conv"):
        conv_copy(1, 0).wait_recv()

    @pl.loop(0, PIECES)
    def _(j):
        proj_copy(j).wait_recv()
        part_out[pad:, chunk(j)] = project(1, far, chunk(j), pad, rows - pad).astype(jnp.bfloat16)
        part_copy(j).start()

    with jax.named_scope("w_edge"):

        @pl.when(sp > 0)
        def _():
            edge_copy(0).wait_recv()
            edge_copy(1).wait_recv()
            mixed[:pad] = edge_x[...].astype(jnp.float32) * edge_c[...].astype(jnp.float32)

    convolve(pad)
    conv_copy(1, 1).start()
    conv_copy(0, 1).start()
    with jax.named_scope("w_head"):
        conv_copy(1, 1).wait_recv()

    @pl.loop(0, PIECES)
    def _(j):
        part_out[:pad, chunk(j)] = project(1, far, chunk(j), 0, pad).astype(jnp.bfloat16)

    part_head.start()
    conv_copy(0, 0).wait_recv()
    conv_copy(0, 1).wait_recv()

    @pl.loop(0, PIECES)
    def _(j):
        projected[:, chunk(j)] = project(0, tp, chunk(j), 0, rows)

    spread(0)
    spread(1)
    for load in loads[7:10]:
        load.wait()

    with jax.named_scope("w_part"):

        @pl.loop(0, PIECES)
        def _(j):
            part_copy(j).wait_recv()
            projected[pad:, chunk(j)] += part_in[pad:, chunk(j)].astype(jnp.float32)

        part_head.wait_recv()
        projected[:pad] += part_in[:pad].astype(jnp.float32)

    with jax.named_scope("norm"):
        for r in range(HALVES):
            part = half(r)
            block = projected[part]
            scale = lax.rsqrt(jnp.mean(block * block, axis=1, keepdims=True) + epsilon)
            mid = (
                resid_ref[part].astype(jnp.float32)
                + block * scale * mix_ref[...].astype(jnp.float32).reshape(1, width)
            ).astype(jnp.bfloat16)
            resid1[part] = mid
            wide = mid.astype(jnp.float32)
            normal = lax.rsqrt(jnp.mean(wide * wide, axis=1, keepdims=True) + epsilon)
            blocks[own, part] = (
                wide * normal * pre_ref[...].astype(jnp.float32).reshape(1, width)
            ).astype(jnp.bfloat16)

            send_own(r)

    spread(2)

    def hide(b, begin, size, e):
        part = pl.ds(begin, size)
        expert = z * 2 + x + e * (1 - 2 * x)
        share = jnp.sum(
            jnp.where(lanes[:size] == expert, shares[b, part], 0.0), axis=1, keepdims=True
        )

        @pl.loop(0, hid // 256)
        def _(j):
            cols = pl.ds(pl.multiple_of(j * 256, 256), 256)
            gate = jnp.dot(blocks[b, part], w_gate[e, :, cols], preferred_element_type=jnp.float32)
            up = jnp.dot(blocks[b, part], w_up[e, :, cols], preferred_element_type=jnp.float32)
            kept = pl.ds(pl.multiple_of(e * hid + j * 256, 256), 256)
            hidden[b, part, kept] = (jax.nn.silu(gate) * up * share).astype(jnp.bfloat16)

    def hide_all(b, e):
        hide(b, 0, rows, e)

    def hide_half(b, r):
        hide(b, r * half_rows, half_rows, 0)
        hide(b, r * half_rows, half_rows, 1)

    def down(b, part, j):
        return jnp.dot(
            hidden[b, part], w_down[:, chunk(j)], preferred_element_type=jnp.float32
        )

    def give(k, r, j, arrived, send):
        made = down(rel(k), half(r), j)
        if arrived is not None:
            made += arrived[rel(k), half(r), chunk(j)].astype(jnp.float32)
        outgoing[rel(k), half(r), chunk(j)] = made.astype(jnp.bfloat16)
        send(k, r, j).start()

    def shared_up_to_hidden():
        s_g = jnp.dot(blocks[own], s_gate[...], preferred_element_type=jnp.float32)
        s_u = jnp.dot(blocks[own], s_up[...], preferred_element_type=jnp.float32)
        shared_hidden[...] = (jax.nn.silu(s_g) * s_u).astype(jnp.bfloat16)

    def own_branch():
        @pl.loop(0, PIECES)
        def _(j):
            branch[:, chunk(j)] = down(own, pl.ds(0, rows), j) + jnp.dot(
                shared_hidden[...], s_down[:, chunk(j)], preferred_element_type=jnp.float32
            )

    def out_copy(r):
        return pltpu.make_async_copy(out_v.at[half(r)], out_ref.at[half(r)], out_sem.at[r])

    def yield_out(r, total):
        factor = lax.rsqrt(jnp.mean(total * total, axis=1, keepdims=True) + epsilon)
        out_v[half(r)] = (
            resid1[half(r)].astype(jnp.float32)
            + total * factor * post_ref[...].astype(jnp.float32).reshape(1, width)
        ).astype(jnp.bfloat16)
        out_copy(r).start()

    def settle():
        @pl.when(sp < sp_size - 1)
        def _():
            drain(edge_send, e_recv, 2 * pad * channels // width).wait_send()

        drain(misc_send, e_recv, channels + 2 * rows * channels // width + rows).wait_send()
        drain(spread_send, e_recv, 2 * 3 * hid // tp_size).wait_send()
        drain(relay_send, e_recv, 2 * 3 * hid // tp_size).wait_send()

    sent_block = rows + 2 * rows * shares.shape[2] // width
    sent_sums = rows

    for load in loads[10:14]:
        load.wait()
    hide_all(own, 0)
    shared_up_to_hidden()
    relay(0)
    spread(3)
    for load in loads[14:]:
        load.wait()

    @pl.when(level == 0)
    def _():
        got_in(1, TABLE)
        got_in(1, 0)
        hide(rel(1), 0, half_rows, 0)
        spread(4)
        relay(1)
        got_in(1, 1)
        hide(rel(1), half_rows, half_rows, 0)
        relay(2)
        relay(3)
        ready_both()
        hide_all(rel(1), 1)
        relay(4)
        spread(5)
        ready(4)
        for r in range(HALVES):
            give(1, r, 0, None, edge_give)
        spread(6)
        got_in(2, TABLE)
        got_in(2, 0)
        hide_half(rel(2), 0)
        give(2, 0, 0, None, edge_give)
        relay(5)
        spread(7)
        ready(5)
        for r in range(HALVES):
            give(1, r, 1, None, edge_give)
        give(2, 0, 1, None, edge_give)
        relay(6)
        relay(7)
        got_in(2, 1)
        hide_half(rel(2), 1)

        @pl.loop(0, 2)
        def _(j):
            give(2, 1, j, None, edge_give)

        ready(6)
        ready(7)

        @pl.loop(2, PIECES)
        def _(j):
            give(2, 0, j, None, edge_give)

        hide_all(own, 1)
        got_in(3, TABLE)
        for r in range(HALVES):
            got_in(3, r)
            hide_half(rel(3), r)

            @pl.loop(0, PIECES)
            def _(j):
                give(3, r, j, None, edge_give)

        @pl.loop(2, PIECES)
        def _(j):
            give(2, 1, j, None, edge_give)

        @pl.loop(2, PIECES)
        def _(j):
            for r in range(HALVES):
                give(1, r, j, None, edge_give)

        own_branch()
        settle()
        for r in range(HALVES):

            @pl.loop(0, PIECES)
            def _(j):
                sum_in(0, r, j)

            total = branch[half(r)] + from_in[own, half(r)].astype(jnp.float32)
            yield_out(r, total)

        drain(in_send, e_recv, sent_block + 3 * sent_sums).wait_send()

    @pl.when(level == 1)
    def _():
        def pass_in(r):
            got_out(r)
            mid_in(0, r).start()

        def pass_out(k, r):
            got_in(k, r)
            mid_out(k, r).start()

        pass_in(TABLE)
        pass_out(2, TABLE)
        pass_in(0)
        pass_out(2, 0)
        pass_out(3, TABLE)
        spread(4)
        relay(1)
        pass_in(1)
        pass_out(2, 1)
        hide_all(rel(0), 0)
        relay(2)
        relay(3)
        hide_all(rel(2), 0)
        relay(4)
        spread(5)
        ready_both()
        pass_out(3, 0)
        hide_all(rel(2), 1)
        spread(6)
        relay(5)
        spread(7)
        hide_all(own, 1)
        pass_out(3, 1)
        relay(6)
        relay(7)
        hide_all(rel(3), 0)
        hide_all(rel(3), 1)
        hide_all(rel(0), 1)
        for n in range(4, count):
            ready(n)

        def give_in(k, r, j):
            sum_out(k, r, j)
            give(k, r, j, from_out, mid_give_in)

        def give_out(r, j):
            sum_in(0, r, j)
            give(0, r, j, from_in, mid_give_out)

        @pl.loop(0, 2)
        def _(j):
            give_in(2, 0, j)

        own_branch()

        @pl.loop(0, 2)
        def _(j):
            give_in(2, 1, j)

        @pl.loop(2, PIECES)
        def _(j):
            give_in(2, 0, j)

        @pl.loop(0, PIECES)
        def _(j):
            give_in(3, 0, j)

        settle()

        @pl.loop(0, PIECES)
        def _(j):
            give_out(0, j)
            give_in(3, 1, j)

        @pl.loop(0, 2)
        def _(j):
            give_out(1, j)

        @pl.loop(2, PIECES)
        def _(j):
            give_in(2, 1, j)
            give_out(1, j)

        for r in range(HALVES):

            @pl.loop(0, PIECES)
            def _(j):
                sum_in(1, r, j)
                sum_out(1, r, j)

            total = (
                branch[half(r)]
                + from_in[own, half(r)].astype(jnp.float32)
                + from_out[own, half(r)].astype(jnp.float32)
            )
            yield_out(r, total)

        drain(in_send, e_recv, 2 * sent_block + 2 * sent_sums).wait_send()
        drain(out_send, e_recv, 3 * sent_block + sent_sums).wait_send()

    for r in range(HALVES):
        out_copy(r).wait()


def fused_layer(
    x_in, gate_b, gate_c, conv_taps, out_proj, mix_gain, resid, pre_gain, expert_gate, expert_up,
    expert_down, shared_gate, shared_up, shared_down, post_gain, routes, route_weights,
):
    experts = lax.axis_size("sp")
    line = experts // 2
    all_rows, channels = x_in.shape
    rows, width = resid.shape
    hid = expert_gate.shape[2]
    shared_hid = shared_gate.shape[1]
    dma = pltpu.SemaphoreType.DMA
    count = 2 * HALVES + PIECES
    bf, f32 = jnp.bfloat16, jnp.float32
    hbm = pl.BlockSpec(memory_space=pltpu.HBM)
    lanes = 128 * (-(-experts // 128))
    pad = 16 * (-(-(conv_taps.shape[0] - 1) // 16))
    top = routes.shape[1]
    return pl.pallas_call(
        functools.partial(layer_kernel, line),
        out_shape=jax.ShapeDtypeStruct((rows, width), bf),
        in_specs=[hbm] * 17,
        out_specs=hbm,
        scratch_shapes=[
            pltpu.VMEM((all_rows, channels), bf),
            pltpu.VMEM((all_rows, channels), bf),
            pltpu.VMEM((all_rows, channels), bf),
            pltpu.VMEM(conv_taps.shape, bf),
            pltpu.VMEM((rows, width), bf),
            pltpu.VMEM((width,), bf),
            pltpu.VMEM((width,), bf),
            pltpu.VMEM((width,), bf),
            pltpu.VMEM((top, rows), jnp.int32),
            pltpu.VMEM((top, rows), f32),
            pltpu.VMEM((pad, channels), bf),
            pltpu.VMEM((pad, channels), bf),
            pltpu.VMEM((pad + all_rows, channels), f32),
            pltpu.VMEM((all_rows, channels), bf),
            pltpu.VMEM((2, rows, channels), bf),
            pltpu.VMEM((2, channels, width), bf),
            pltpu.VMEM((rows, width), bf),
            pltpu.VMEM((rows, width), bf),
            pltpu.VMEM((rows, width), f32),
            pltpu.VMEM((rows, width), bf),
            pltpu.VMEM((2, width, hid), bf),
            pltpu.VMEM((2, width, hid), bf),
            pltpu.VMEM((2 * hid, width), bf),
            pltpu.VMEM((width, shared_hid), bf),
            pltpu.VMEM((width, shared_hid), bf),
            pltpu.VMEM((shared_hid, width), bf),
            pltpu.VMEM((line, rows, width), bf),
            pltpu.VMEM((line, rows, lanes), f32),
            pltpu.VMEM((line, rows, 2 * hid), bf),
            pltpu.VMEM((rows, shared_hid), bf),
            pltpu.VMEM((rows, width), f32),
            pltpu.VMEM((line, rows, width), bf),
            pltpu.VMEM((line, rows, width), bf),
            pltpu.VMEM((line, rows, width), bf),
            pltpu.VMEM((rows, width), bf),
            dma((17,)),
            dma((HALVES,)),
        ]
        + [dma((1,))] * 6
        + [
            dma((2,)),
            dma((PIECES,)),
            dma((2, 2)),
            dma((PIECES + 1,)),
            dma((count,)),
            dma((1 + PIECES,)),
            dma((count,)),
            dma((1 + PIECES,)),
            dma((line - 1, HALVES + 1)),
            dma((HALVES + 1,)),
            dma((2, HALVES, PIECES)),
            dma((line - 1, HALVES, PIECES)),
        ],
        compiler_params=pltpu.CompilerParams(
            collective_id=0, has_side_effects=True, vmem_limit_bytes=60 * 1024 * 1024
        ),
    )(
        x_in, gate_b, gate_c, conv_taps, resid, mix_gain, pre_gain, post_gain,
        routes.T, route_weights.T, out_proj, expert_gate, expert_up, expert_down,
        shared_gate, shared_up, shared_down,
    )


def passed_along(shard, axis, by):
    size = lax.axis_size(axis)
    pairs = [(i, i + by) for i in range(size) if 0 <= i + by < size]
    return lax.ppermute(shard, axis, pairs)


def body(
    x_in,
    gate_b,
    gate_c,
    conv_taps,
    out_proj,
    mix_gain,
    resid,
    pre_gain,
    expert_gate,
    expert_up,
    expert_down,
    shared_gate,
    shared_up,
    shared_down,
    post_gain,
    routes,
    route_weights,
):
    group = lax.axis_size("sp")
    wide_slots = 3 * resid.shape[0] * routes.shape[1] // group
    if wide_slots > resid.shape[0] and group == 2 * 2 * 2 and lax.axis_size("tp") == 2 * 2:
        return fused_layer(
            x_in, gate_b, gate_c, conv_taps, out_proj, mix_gain, resid, pre_gain, expert_gate,
            expert_up, expert_down, shared_gate, shared_up, shared_down, post_gain, routes,
            route_weights,
        )
    row_count = x_in.shape[0]
    channels = x_in.shape[1]
    reach = conv_taps.shape[0] - 1
    edge_rows = jnp.concatenate([x_in[row_count - reach :], gate_c[row_count - reach :]], 1)
    arrived_edge = passed_along(edge_rows, "sp", 1)
    inputs = jnp.concatenate([arrived_edge[:, :channels], x_in], 0).astype(jnp.float32)
    gate_rows = jnp.concatenate([arrived_edge[:, channels:], gate_c], 0).astype(jnp.float32)
    mixed_in = inputs * gate_rows
    taps = conv_taps.astype(jnp.float32)
    convolved = jnp.zeros((row_count, channels), jnp.float32)
    for index in range(reach + 1):
        convolved = convolved + taps[index][None, :] * mixed_in[index : index + row_count]
    conv_out = (gate_b.astype(jnp.float32) * convolved).astype(jnp.bfloat16)
    width_all = out_proj.shape[1]
    full_rows = lax.all_to_all(conv_out, "tp", split_axis=0, concat_axis=1, tiled=True)
    projected = jnp.dot(
        full_rows,
        lax.all_gather(out_proj, "tp", axis=0, tiled=True),
        preferred_element_type=jnp.float32,
    )
    row_scale = lax.rsqrt(jnp.mean(projected * projected, axis=1, keepdims=True) + epsilon)
    resid1 = (
        resid.astype(jnp.float32) + projected * row_scale * mix_gain.astype(jnp.float32)
    ).astype(jnp.bfloat16)
    wide_resid = resid1.astype(jnp.float32)
    normed = (
        wide_resid
        * lax.rsqrt(jnp.mean(wide_resid * wide_resid, axis=1, keepdims=True) + epsilon)
        * pre_gain.astype(jnp.float32)
    ).astype(jnp.bfloat16)
    experts = lax.axis_size("sp")
    local_rows = resid.shape[0]
    top_count = routes.shape[1]
    capacity = 3 * local_rows * top_count // (2 * experts)
    flat_ids = routes.reshape(-1)
    onehot = (flat_ids[:, None] == jnp.arange(experts, dtype=jnp.int32)[None, :]).astype(jnp.int32)
    before = jnp.cumsum(onehot, axis=0) - onehot
    position = jnp.sum(before * onehot, axis=1)
    slot_index = flat_ids * capacity + position
    outgoing = (
        jnp.zeros((experts * capacity, width_all), jnp.bfloat16)
        .at[slot_index]
        .set(jnp.repeat(normed, top_count, axis=0))
    )
    received = lax.all_to_all(
        outgoing.reshape(experts, capacity, width_all),
        "sp",
        split_axis=0,
        concat_axis=0,
        tiled=True,
    )
    arrived = received.reshape(experts * capacity, width_all)
    gate_h = jnp.dot(arrived, expert_gate[0], preferred_element_type=jnp.float32)
    up_h = jnp.dot(arrived, expert_up[0], preferred_element_type=jnp.float32)
    hidden = (jax.nn.silu(gate_h) * up_h).astype(jnp.bfloat16)
    expert_out = jnp.dot(hidden, expert_down[0], preferred_element_type=jnp.float32).astype(
        jnp.bfloat16
    )
    returned = lax.all_to_all(
        expert_out.reshape(experts, capacity, width_all),
        "sp",
        split_axis=0,
        concat_axis=0,
        tiled=True,
    )
    returned = returned.reshape(experts * capacity, width_all)
    picked = returned[slot_index].astype(jnp.float32).reshape(local_rows, top_count, width_all)
    routed = jnp.einsum("tk,tkd->td", route_weights, picked)
    shared_g = jnp.dot(normed, shared_gate, preferred_element_type=jnp.float32)
    shared_u = jnp.dot(normed, shared_up, preferred_element_type=jnp.float32)
    shared_hidden = (jax.nn.silu(shared_g) * shared_u).astype(jnp.bfloat16)
    shared_out = jnp.dot(shared_hidden, shared_down, preferred_element_type=jnp.float32)
    branch = routed + shared_out
    factor = lax.rsqrt(jnp.mean(branch * branch, axis=1, keepdims=True) + epsilon)
    return (wide_resid + branch * factor * post_gain.astype(jnp.float32)[None, :]).astype(
        jnp.bfloat16
    )


def solution(mesh):
    return jax.shard_map(
        body,
        mesh=mesh,
        in_specs=(
            P("sp", "tp"),
            P("sp", "tp"),
            P("sp", "tp"),
            P(None, "tp"),
            P("tp", None),
            P(),
            P(("sp", "tp"), None),
            P(),
            P("sp", None, None),
            P("sp", None, None),
            P("sp", None, None),
            P(),
            P(),
            P(),
            P(),
            P(("sp", "tp"), None),
            P(("sp", "tp"), None),
        ),
        out_specs=P(("sp", "tp"), None),
        check_vma=False,
    )
```

```python
import functools

import jax
import jax.numpy as jnp
from jax import lax
from jax.experimental import pallas as pl
from jax.experimental.pallas import tpu as pltpu

P = jax.sharding.PartitionSpec
MESH = pl.DeviceIdType.MESH
epsilon = 1e-06
PIECES = 4
HALVES = 2
DIRECT = (4, 5, 8)
ORDER = (0, 1, 2, 3, 4, -4, 6, 5, -5, 7, 8, -8)
CUTS = ((0, 0, 2), (0, 2, 2), (1, 0, 2), (1, 2, 1), (1, 3, 1))
TABLE = HALVES


def layer_kernel(
    line,
    x_hbm,
    gate_b_hbm,
    gate_c_hbm,
    taps_hbm,
    resid_hbm,
    mix_hbm,
    pre_hbm,
    post_hbm,
    routes_hbm,
    weights_hbm,
    proj_ref,
    eg_ref,
    eu_ref,
    ed_ref,
    sg_ref,
    su_ref,
    sd_ref,
    out_ref,
    x_ref,
    gate_b_ref,
    gate_c_ref,
    taps_ref,
    resid_ref,
    mix_ref,
    pre_ref,
    post_ref,
    routes_ref,
    weights_ref,
    edge_x,
    edge_c,
    mixed,
    conv,
    conv_near,
    proj,
    part_out,
    part_in,
    projected,
    resid1,
    w_gate,
    w_up,
    w_down,
    s_gate,
    s_up,
    s_down,
    blocks,
    shares,
    hidden,
    shared_hidden,
    branch,
    outgoing,
    from_out,
    from_in,
    out_v,
    load_sem,
    out_sem,
    edge_send,
    misc_send,
    spread_send,
    relay_send,
    in_send,
    out_send,
    e_recv,
    p_recv,
    c_recv,
    f_recv,
    wx_recv,
    wn_recv,
    wf_recv,
    wr_recv,
    gi_recv,
    go_recv,
    ri_recv,
    ro_recv,
):
    sp = lax.axis_index("sp")
    tp = lax.axis_index("tp")
    sp_size = lax.axis_size("sp")
    tp_size = lax.axis_size("tp")
    z = sp // 2
    x = sp % 2
    last = line - 1
    mate = z * 2 + 1 - x
    near = (tp // 2) * 2 + 1 - tp % 2
    far = (tp + 2) % tp_size
    near_far = (near + 2) % tp_size
    upper = z // (line // 2)
    inward_step = 1 - 2 * upper
    level = upper * last + inward_step * z
    inward = ((z + inward_step) * 2 + x, tp)
    outward = ((z - inward_step) * 2 + x, tp)

    def rel(k):
        return upper * last + inward_step * k

    rows, width = resid_ref.shape
    half_rows = rows // HALVES
    hid = w_gate.shape[2]
    shared_hid = s_gate.shape[1]
    part_cols = width // PIECES

    barrier = pltpu.get_barrier_semaphore()

    def greet(device):
        pl.semaphore_signal(barrier, inc=1, device_id=device, device_id_type=MESH)

    greet((mate, tp))
    greet((sp, near))
    greet((sp, far))

    @pl.when(z > 0)
    def _():
        greet((sp - 2, tp))

    @pl.when(z < last)
    def _():
        greet((sp + 2, tp))

    @pl.when((x == 1) & (z < last))
    def _():
        greet((sp + 1, tp))

    @pl.when((x == 0) & (z > 0))
    def _():
        greet((sp - 1, tp))

    pairs = (
        (x_hbm, x_ref),
        (gate_c_hbm, gate_c_ref),
        (proj_ref, proj.at[0]),
        (gate_b_hbm, gate_b_ref),
        (taps_hbm, taps_ref),
        (routes_hbm, routes_ref),
        (weights_hbm, weights_ref),
        (resid_hbm, resid_ref),
        (mix_hbm, mix_ref),
        (pre_hbm, pre_ref),
        (eg_ref.at[0], w_gate.at[0]),
        (eu_ref.at[0], w_up.at[0]),
        (sg_ref, s_gate),
        (su_ref, s_up),
        (ed_ref.at[0], w_down.at[pl.ds(0, hid)]),
        (sd_ref, s_down),
        (post_hbm, post_ref),
    )
    loads = [pltpu.make_async_copy(src, dst, load_sem.at[n]) for n, (src, dst) in enumerate(pairs)]
    for load in loads:
        load.start()

    all_rows, channels = x_ref.shape
    reach = taps_ref.shape[0] - 1
    pad = edge_x.shape[0]

    def edge_copy(n):
        source, landing = ((x_hbm, edge_x), (gate_c_hbm, edge_c))[n]
        return pltpu.make_async_remote_copy(
            src_ref=source.at[pl.ds(all_rows - pad, pad)],
            dst_ref=landing,
            send_sem=edge_send.at[0],
            recv_sem=e_recv.at[n],
            device_id=((sp + 1) % sp_size, tp),
            device_id_type=MESH,
        )

    def block_rows(owner):
        return pl.ds(pl.multiple_of(owner * rows, rows), rows)

    def conv_copy(n, k):
        begin, size = ((pad, rows - pad), (0, pad))[k]
        return pltpu.make_async_remote_copy(
            src_ref=conv.at[pl.ds(pl.multiple_of((near, near_far)[n] * rows + begin, pad), size)],
            dst_ref=conv_near.at[n, pl.ds(begin, size)],
            send_sem=misc_send.at[0],
            recv_sem=c_recv.at[n, k],
            device_id=(sp, near),
            device_id_type=MESH,
        )

    def chunk(j):
        return pl.ds(pl.multiple_of(j * part_cols, part_cols), part_cols)

    def half(r):
        return pl.ds(r * half_rows, half_rows)

    def proj_copy(j):
        return pltpu.make_async_remote_copy(
            src_ref=proj.at[0, :, chunk(j)],
            dst_ref=proj.at[1, :, chunk(j)],
            send_sem=misc_send.at[0],
            recv_sem=p_recv.at[j],
            device_id=(sp, near),
            device_id_type=MESH,
        )

    def part_copy(j):
        where = (pl.ds(pad, rows - pad), chunk(j))
        return pltpu.make_async_remote_copy(
            src_ref=part_out.at[where],
            dst_ref=part_in.at[where],
            send_sem=misc_send.at[0],
            recv_sem=f_recv.at[j],
            device_id=(sp, far),
            device_id_type=MESH,
        )

    part_head = pltpu.make_async_remote_copy(
        src_ref=part_out.at[pl.ds(0, pad)],
        dst_ref=part_in.at[pl.ds(0, pad)],
        send_sem=misc_send.at[0],
        recv_sem=f_recv.at[PIECES],
        device_id=(sp, far),
        device_id_type=MESH,
    )

    pieces = [((eg_ref, w_gate), (eu_ref, w_up))[k] + (first, size) for k, first, size in CUTS]
    for j in range(PIECES):
        pieces.append((ed_ref, w_down, j, 1))
    count = len(pieces)

    def cut(n, owner):
        ref, held, first, steps = pieces[n]
        if held is w_down:
            size = hid // tp_size
            begin = pl.multiple_of(owner * size, size)
            return (
                ref.at[0, pl.ds(begin, size), chunk(first)],
                held.at[pl.ds(pl.multiple_of(hid + begin, size), size), chunk(first)],
            )
        size = ref.shape[1] // tp_size // 4
        where = pl.ds(pl.multiple_of((owner * 4 + first) * size, size), size * steps)
        return ref.at[0, where], held.at[1, where]

    def hop(n, owner, target, send, recv, first=False):
        source, landing = cut(n, owner)
        return pltpu.make_async_remote_copy(
            src_ref=source if first else landing,
            dst_ref=landing,
            send_sem=send.at[0],
            recv_sem=recv,
            device_id=target,
            device_id_type=MESH,
        )

    def late(n):
        return min(n // 2, 1) + max(0, n - len(CUTS) + 1)

    def x_hop(n):
        return hop(n, tp, (mate, tp), spread_send, wx_recv.at[n], True)

    def near_hop(n, owner):
        return hop(n, owner, (sp, near), spread_send, wn_recv.at[late(n)])

    def far_hop(n, owner):
        return hop(n, owner, (sp, far), relay_send, wf_recv.at[n])

    def direct_hop(n):
        return hop(n, far, (mate, tp), relay_send, wf_recv.at[n], True)

    def relay_hop(n, owner):
        return hop(n, owner, (sp, near), relay_send, wr_recv.at[late(n)])

    def drain(send, recv, size):
        where = w_down.at[pl.ds(0, size)]
        return pltpu.make_async_remote_copy(
            src_ref=where,
            dst_ref=where,
            send_sem=send.at[0],
            recv_sem=recv.at[0],
            device_id=(sp, near),
            device_id_type=MESH,
        )

    def spread(n):
        with jax.named_scope("w_x"):
            x_hop(n).wait_recv()
        if n not in DIRECT:
            far_hop(n, tp).start()
        near_hop(n, tp).start()

    def relay(n):
        with jax.named_scope("w_far"):
            far_hop(n, far).wait_recv()
        relay_hop(n, far).start()

    def ready(n):
        with jax.named_scope("w_ready"):
            near_hop(n, near).wait_recv()
            relay_hop(n, near_far).wait_recv()

    def ready_part(k):
        with jax.named_scope("w_ready"):
            drain(spread_send, wn_recv.at[pl.ds(k, 1)], hid // tp_size).wait_recv()
            drain(relay_send, wr_recv.at[pl.ds(k, 1)], hid // tp_size).wait_recv()

    def block_copy(b, r, target, send, recv):
        ref = shares.at[b] if r == TABLE else blocks.at[b, half(r)]
        return pltpu.make_async_remote_copy(
            src_ref=ref,
            dst_ref=ref,
            send_sem=send.at[0],
            recv_sem=recv,
            device_id=target,
            device_id_type=MESH,
        )

    def edge_in(r):
        return block_copy(rel(0), r, inward, in_send, go_recv.at[r])

    def mid_in(k, r):
        return block_copy(rel(k), r, inward, in_send, gi_recv.at[last - k - 1, r])

    def mid_out(k, r):
        return block_copy(rel(k), r, outward, out_send, gi_recv.at[k - 1, r])

    def got_in(k, r):
        with jax.named_scope("w_gi"):
            block_copy(rel(k), r, inward, in_send, gi_recv.at[k - 1, r]).wait_recv()

    def got_out(r):
        with jax.named_scope("w_go"):
            block_copy(rel(0), r, outward, out_send, go_recv.at[r]).wait_recv()

    def sum_copy(k, r, j, landing, target, send, recv):
        return pltpu.make_async_remote_copy(
            src_ref=outgoing.at[rel(k), half(r), chunk(j)],
            dst_ref=landing.at[rel(k), half(r), chunk(j)],
            send_sem=send.at[0],
            recv_sem=recv.at[j],
            device_id=target,
            device_id_type=MESH,
        )

    def edge_give(k, r, j):
        return sum_copy(k, r, j, from_out, inward, in_send, ro_recv.at[k - 1, r])

    def mid_give_in(k, r, j):
        return sum_copy(k, r, j, from_in, inward, in_send, ri_recv.at[last - k, r])

    def mid_give_out(k, r, j):
        return sum_copy(k, r, j, from_in, outward, out_send, ri_recv.at[k, r])

    def sum_in(k, r, j):
        with jax.named_scope("w_ri"):
            sum_copy(k, r, j, from_in, inward, in_send, ri_recv.at[k, r]).wait_recv()

    def sum_out(k, r, j):
        with jax.named_scope("w_ro"):
            sum_copy(k, r, j, from_out, outward, out_send, ro_recv.at[k - 1, r]).wait_recv()

    with jax.named_scope("w_barrier"):
        met = 3 + jnp.where(z > 0, 1, 0) + jnp.where(z < last, 1, 0)
        met += jnp.where(jnp.where(x == 1, z < last, z > 0), 1, 0)
        pl.semaphore_wait(barrier, met)

    @pl.when(sp < sp_size - 1)
    def _():
        edge_copy(0).start()
        edge_copy(1).start()

    for n in ORDER:
        if n < 0:
            direct_hop(-n).start()
        else:
            x_hop(n).start()

    loads[2].wait()
    for j in range(PIECES):
        proj_copy(j).start()

    for n in (0, 1, 3, 4):
        loads[n].wait()
    mixed[:pad] = jnp.zeros((pad, channels), jnp.float32)
    mixed[pad:] = x_ref[...].astype(jnp.float32) * gate_c_ref[...].astype(jnp.float32)

    def convolve(size):
        convolved = jnp.zeros((size, channels), jnp.float32)
        for k in range(reach + 1):
            begin = pad - reach + k
            convolved += taps_ref[k : k + 1].astype(jnp.float32) * mixed[begin : begin + size]
        conv[:size] = (gate_b_ref[:size].astype(jnp.float32) * convolved).astype(jnp.bfloat16)

    convolve(all_rows)
    conv_copy(1, 0).start()
    conv_copy(0, 0).start()
    loads[5].wait()
    loads[6].wait()
    lanes = lax.broadcasted_iota(jnp.int32, (rows, shares.shape[2]), 1)
    names = lax.broadcasted_iota(jnp.int32, (shares.shape[2], rows), 0)
    table = jnp.zeros((shares.shape[2], rows), jnp.float32)
    for k in range(routes_ref.shape[0]):
        table += jnp.where(names == routes_ref[k : k + 1], weights_ref[k : k + 1], 0.0)
    own = z
    shares[own] = table.T

    def send_own(r):
        @pl.when(level == 0)
        def _():
            edge_in(r).start()

        @pl.when(level == 1)
        def _():
            if r != HALVES - 1:
                mid_in(1, r).start()
            mid_out(1, r).start()

    send_own(TABLE)

    def project(n, owner, cols, begin, size):
        mine = pl.ds(pl.multiple_of(owner * rows + begin, pad), size)
        return jnp.dot(
            conv[mine], proj[0, :, cols], preferred_element_type=jnp.float32
        ) + jnp.dot(
            conv_near[n, begin : begin + size], proj[1, :, cols], preferred_element_type=jnp.float32
        )

    with jax.named_scope("w_conv"):
        conv_copy(1, 0).wait_recv()

    @pl.loop(0, PIECES)
    def _(j):
        proj_copy(j).wait_recv()
        part_out[pad:, chunk(j)] = project(1, far, chunk(j), pad, rows - pad).astype(jnp.bfloat16)
        part_copy(j).start()

    with jax.named_scope("w_edge"):

        @pl.when(sp > 0)
        def _():
            edge_copy(0).wait_recv()
            edge_copy(1).wait_recv()
            mixed[:pad] = edge_x[...].astype(jnp.float32) * edge_c[...].astype(jnp.float32)

    convolve(pad)
    conv_copy(1, 1).start()
    conv_copy(0, 1).start()
    with jax.named_scope("w_head"):
        conv_copy(1, 1).wait_recv()

    @pl.loop(0, PIECES)
    def _(j):
        part_out[:pad, chunk(j)] = project(1, far, chunk(j), 0, pad).astype(jnp.bfloat16)

    part_head.start()
    conv_copy(0, 0).wait_recv()
    conv_copy(0, 1).wait_recv()

    @pl.loop(0, PIECES)
    def _(j):
        projected[:, chunk(j)] = project(0, tp, chunk(j), 0, rows)

    spread(0)
    spread(1)
    for load in loads[7:10]:
        load.wait()

    with jax.named_scope("w_part"):

        @pl.loop(0, PIECES)
        def _(j):
            part_copy(j).wait_recv()
            projected[pad:, chunk(j)] += part_in[pad:, chunk(j)].astype(jnp.float32)

        part_head.wait_recv()
        projected[:pad] += part_in[:pad].astype(jnp.float32)

    with jax.named_scope("norm"):
        for r in range(HALVES):
            part = half(r)
            block = projected[part]
            scale = lax.rsqrt(jnp.mean(block * block, axis=1, keepdims=True) + epsilon)
            mid = (
                resid_ref[part].astype(jnp.float32)
                + block * scale * mix_ref[...].astype(jnp.float32).reshape(1, width)
            ).astype(jnp.bfloat16)
            resid1[part] = mid
            wide = mid.astype(jnp.float32)
            normal = lax.rsqrt(jnp.mean(wide * wide, axis=1, keepdims=True) + epsilon)
            blocks[own, part] = (
                wide * normal * pre_ref[...].astype(jnp.float32).reshape(1, width)
            ).astype(jnp.bfloat16)

            send_own(r)

    spread(2)

    def hide(b, begin, size, e):
        part = pl.ds(begin, size)
        expert = z * 2 + x + e * (1 - 2 * x)
        share = jnp.sum(
            jnp.where(lanes[:size] == expert, shares[b, part], 0.0), axis=1, keepdims=True
        )

        def step(j):
            cols = pl.ds(pl.multiple_of(j * 256, 256), 256)
            gate = jnp.dot(blocks[b, part], w_gate[e, :, cols], preferred_element_type=jnp.float32)
            up = jnp.dot(blocks[b, part], w_up[e, :, cols], preferred_element_type=jnp.float32)
            kept = pl.ds(pl.multiple_of(e * hid + j * 256, 256), 256)
            hidden[b, part, kept] = (jax.nn.silu(gate) * up * share).astype(jnp.bfloat16)

        if size < rows:
            for j in range(hid // 256):
                step(j)
        else:
            pl.loop(0, hid // 256)(step)

    def share_of(b, e):
        expert = z * 2 + x + e * (1 - 2 * x)
        return jnp.sum(jnp.where(lanes == expert, shares[b], 0.0), axis=1, keepdims=True)

    def gate_ahead(b):
        share = share_of(b, 1)

        @pl.loop(0, hid // 256)
        def _(j):
            cols = pl.ds(pl.multiple_of(j * 256, 256), 256)
            gate = jnp.dot(blocks[b], w_gate[1, :, cols], preferred_element_type=jnp.float32)
            projected[:, cols] = jax.nn.silu(gate) * share

    def up_after(b):
        for j in range(hid // 256):
            cols = pl.ds(j * 256, 256)
            up = jnp.dot(blocks[b], w_up[1, :, cols], preferred_element_type=jnp.float32)
            kept = pl.ds(hid + j * 256, 256)
            hidden[b, :, kept] = (projected[:, cols] * up).astype(jnp.bfloat16)

    def hide_all(b, e):
        hide(b, 0, rows, e)

    def hide_half(b, r):
        hide(b, r * half_rows, half_rows, 0)
        hide(b, r * half_rows, half_rows, 1)

    def down(b, part, j):
        return jnp.dot(
            hidden[b, part], w_down[:, chunk(j)], preferred_element_type=jnp.float32
        )

    def give(k, r, j, arrived, send):
        made = down(rel(k), half(r), j)
        if arrived is not None:
            made += arrived[rel(k), half(r), chunk(j)].astype(jnp.float32)
        outgoing[rel(k), half(r), chunk(j)] = made.astype(jnp.bfloat16)
        send(k, r, j).start()

    def shared_up_to_hidden():
        s_g = jnp.dot(blocks[own], s_gate[...], preferred_element_type=jnp.float32)
        s_u = jnp.dot(blocks[own], s_up[...], preferred_element_type=jnp.float32)
        shared_hidden[...] = (jax.nn.silu(s_g) * s_u).astype(jnp.bfloat16)

    def own_branch():
        @pl.loop(0, PIECES)
        def _(j):
            branch[:, chunk(j)] = down(own, pl.ds(0, rows), j) + jnp.dot(
                shared_hidden[...], s_down[:, chunk(j)], preferred_element_type=jnp.float32
            )

    def out_copy(r):
        return pltpu.make_async_copy(out_v.at[half(r)], out_ref.at[half(r)], out_sem.at[r])

    def yield_out(r, total):
        factor = lax.rsqrt(jnp.mean(total * total, axis=1, keepdims=True) + epsilon)
        out_v[half(r)] = (
            resid1[half(r)].astype(jnp.float32)
            + total * factor * post_ref[...].astype(jnp.float32).reshape(1, width)
        ).astype(jnp.bfloat16)
        out_copy(r).start()

    def settle():
        @pl.when(sp < sp_size - 1)
        def _():
            drain(edge_send, e_recv, 2 * pad * channels // width).wait_send()

        drain(misc_send, e_recv, channels + 2 * rows * channels // width + rows).wait_send()
        drain(spread_send, e_recv, 2 * 3 * hid // tp_size).wait_send()
        drain(relay_send, e_recv, 2 * 3 * hid // tp_size).wait_send()

    sent_block = rows + 2 * rows * shares.shape[2] // width
    sent_sums = rows

    for load in loads[10:14]:
        load.wait()
    hide_all(own, 0)
    shared_up_to_hidden()
    relay(0)
    spread(3)
    for load in loads[14:]:
        load.wait()

    @pl.when(level == 0)
    def _():
        got_in(1, TABLE)
        got_in(1, 0)
        hide(rel(1), 0, half_rows, 0)
        spread(4)
        relay(1)
        relay(4)
        spread(6)
        got_in(1, 1)
        hide(rel(1), half_rows, half_rows, 0)
        relay(2)
        ready_part(0)
        gate_ahead(rel(1))
        spread(5)
        relay(3)
        relay(5)
        ready_part(1)
        up_after(rel(1))
        ready(5)
        for r in range(HALVES):
            give(1, r, 0, None, edge_give)
        relay(6)
        spread(7)
        ready(6)
        for r in range(HALVES):
            give(1, r, 1, None, edge_give)
        got_in(2, TABLE)
        got_in(2, 0)
        hide_half(rel(2), 0)

        @pl.loop(0, 2)
        def _(j):
            give(2, 0, j, None, edge_give)

        spread(8)
        got_in(3, TABLE)
        got_in(3, 0)
        hide_half(rel(3), 0)

        @pl.loop(0, 2)
        def _(j):
            give(3, 0, j, None, edge_give)

        relay(7)
        relay(8)
        ready(7)
        ready(8)

        @pl.loop(2, PIECES)
        def _(j):
            give(3, 0, j, None, edge_give)

        got_in(3, 1)
        hide_half(rel(3), 1)

        @pl.loop(0, PIECES)
        def _(j):
            give(3, 1, j, None, edge_give)

        @pl.loop(2, PIECES)
        def _(j):
            give(2, 0, j, None, edge_give)

        hide_all(own, 1)
        got_in(2, 1)
        hide_half(rel(2), 1)

        @pl.loop(0, PIECES)
        def _(j):
            give(2, 1, j, None, edge_give)

        @pl.loop(2, PIECES)
        def _(j):
            for r in range(HALVES):
                give(1, r, j, None, edge_give)

        own_branch()
        settle()
        for r in range(HALVES):

            @pl.loop(0, PIECES)
            def _(j):
                sum_in(0, r, j)

            total = branch[half(r)] + from_in[own, half(r)].astype(jnp.float32)
            yield_out(r, total)

        drain(in_send, e_recv, sent_block + 3 * sent_sums).wait_send()

    @pl.when(level == 1)
    def _():
        def pass_in(r):
            got_out(r)
            mid_in(0, r).start()

        def pass_out(k, r):
            got_in(k, r)
            mid_out(k, r).start()

        pass_in(TABLE)
        pass_out(2, TABLE)
        pass_in(0)
        pass_out(2, 0)
        pass_out(3, TABLE)
        spread(4)
        relay(1)
        relay(4)
        spread(6)
        pass_in(1)
        mid_in(1, HALVES - 1).start()
        pass_out(3, 0)
        hide_all(rel(0), 0)
        relay(2)
        spread(5)
        relay(3)
        relay(5)
        ready_part(0)
        ready_part(1)
        hide_half(rel(2), 0)
        relay(6)
        spread(7)
        pass_out(3, 1)
        hide_all(own, 1)
        spread(8)
        hide_all(rel(3), 0)
        relay(7)
        relay(8)
        hide_all(rel(3), 1)
        pass_out(2, 1)
        hide_half(rel(2), 1)
        hide_all(rel(0), 1)
        for n in range(len(CUTS), count):
            ready(n)

        def give_in(k, r, j):
            sum_out(k, r, j)
            give(k, r, j, from_out, mid_give_in)

        def give_out(r, j):
            sum_in(0, r, j)
            give(0, r, j, from_in, mid_give_out)

        @pl.loop(0, 2)
        def _(j):
            give_in(2, 0, j)

        own_branch()

        @pl.loop(0, PIECES)
        def _(j):
            give_in(3, 0, j)

        settle()

        @pl.loop(0, PIECES)
        def _(j):
            give_out(0, j)
            give_in(3, 1, j)

        @pl.loop(0, 2)
        def _(j):
            give_out(1, j)

        @pl.loop(2, PIECES)
        def _(j):
            give_in(2, 0, j)
            give_out(1, j)

        @pl.loop(0, PIECES)
        def _(j):
            give_in(2, 1, j)

        for r in range(HALVES):

            @pl.loop(0, PIECES)
            def _(j):
                sum_in(1, r, j)
                sum_out(1, r, j)

            total = (
                branch[half(r)]
                + from_in[own, half(r)].astype(jnp.float32)
                + from_out[own, half(r)].astype(jnp.float32)
            )
            yield_out(r, total)

        drain(in_send, e_recv, 2 * sent_block + 2 * sent_sums).wait_send()
        drain(out_send, e_recv, 3 * sent_block + sent_sums).wait_send()

    for r in range(HALVES):
        out_copy(r).wait()


def fused_layer(
    x_in, gate_b, gate_c, conv_taps, out_proj, mix_gain, resid, pre_gain, expert_gate, expert_up,
    expert_down, shared_gate, shared_up, shared_down, post_gain, routes, route_weights,
):
    experts = lax.axis_size("sp")
    line = experts // 2
    all_rows, channels = x_in.shape
    rows, width = resid.shape
    hid = expert_gate.shape[2]
    shared_hid = shared_gate.shape[1]
    dma = pltpu.SemaphoreType.DMA
    count = len(CUTS) + PIECES
    bf, f32 = jnp.bfloat16, jnp.float32
    hbm = pl.BlockSpec(memory_space=pltpu.HBM)
    lanes = 128 * (-(-experts // 128))
    pad = 16 * (-(-(conv_taps.shape[0] - 1) // 16))
    top = routes.shape[1]
    return pl.pallas_call(
        functools.partial(layer_kernel, line),
        out_shape=jax.ShapeDtypeStruct((rows, width), bf),
        in_specs=[hbm] * 17,
        out_specs=hbm,
        scratch_shapes=[
            pltpu.VMEM((all_rows, channels), bf),
            pltpu.VMEM((all_rows, channels), bf),
            pltpu.VMEM((all_rows, channels), bf),
            pltpu.VMEM(conv_taps.shape, bf),
            pltpu.VMEM((rows, width), bf),
            pltpu.VMEM((width,), bf),
            pltpu.VMEM((width,), bf),
            pltpu.VMEM((width,), bf),
            pltpu.VMEM((top, rows), jnp.int32),
            pltpu.VMEM((top, rows), f32),
            pltpu.VMEM((pad, channels), bf),
            pltpu.VMEM((pad, channels), bf),
            pltpu.VMEM((pad + all_rows, channels), f32),
            pltpu.VMEM((all_rows, channels), bf),
            pltpu.VMEM((2, rows, channels), bf),
            pltpu.VMEM((2, channels, width), bf),
            pltpu.VMEM((rows, width), bf),
            pltpu.VMEM((rows, width), bf),
            pltpu.VMEM((rows, width), f32),
            pltpu.VMEM((rows, width), bf),
            pltpu.VMEM((2, width, hid), bf),
            pltpu.VMEM((2, width, hid), bf),
            pltpu.VMEM((2 * hid, width), bf),
            pltpu.VMEM((width, shared_hid), bf),
            pltpu.VMEM((width, shared_hid), bf),
            pltpu.VMEM((shared_hid, width), bf),
            pltpu.VMEM((line, rows, width), bf),
            pltpu.VMEM((line, rows, lanes), f32),
            pltpu.VMEM((line, rows, 2 * hid), bf),
            pltpu.VMEM((rows, shared_hid), bf),
            pltpu.VMEM((rows, width), f32),
            pltpu.VMEM((line, rows, width), bf),
            pltpu.VMEM((line, rows, width), bf),
            pltpu.VMEM((line, rows, width), bf),
            pltpu.VMEM((rows, width), bf),
            dma((17,)),
            dma((HALVES,)),
        ]
        + [dma((1,))] * 6
        + [
            dma((2,)),
            dma((PIECES,)),
            dma((2, 2)),
            dma((PIECES + 1,)),
            dma((count,)),
            dma((2 + PIECES,)),
            dma((count,)),
            dma((2 + PIECES,)),
            dma((line - 1, HALVES + 1)),
            dma((HALVES + 1,)),
            dma((2, HALVES, PIECES)),
            dma((line - 1, HALVES, PIECES)),
        ],
        compiler_params=pltpu.CompilerParams(
            collective_id=0, has_side_effects=True, vmem_limit_bytes=60 * 1024 * 1024
        ),
    )(
        x_in, gate_b, gate_c, conv_taps, resid, mix_gain, pre_gain, post_gain,
        routes.T, route_weights.T, out_proj, expert_gate, expert_up, expert_down,
        shared_gate, shared_up, shared_down,
    )


def passed_along(shard, axis, by):
    size = lax.axis_size(axis)
    pairs = [(i, i + by) for i in range(size) if 0 <= i + by < size]
    return lax.ppermute(shard, axis, pairs)


def body(
    x_in,
    gate_b,
    gate_c,
    conv_taps,
    out_proj,
    mix_gain,
    resid,
    pre_gain,
    expert_gate,
    expert_up,
    expert_down,
    shared_gate,
    shared_up,
    shared_down,
    post_gain,
    routes,
    route_weights,
):
    group = lax.axis_size("sp")
    wide_slots = 3 * resid.shape[0] * routes.shape[1] // group
    if wide_slots > resid.shape[0] and group == 2 * 2 * 2 and lax.axis_size("tp") == 2 * 2:
        return fused_layer(
            x_in, gate_b, gate_c, conv_taps, out_proj, mix_gain, resid, pre_gain, expert_gate,
            expert_up, expert_down, shared_gate, shared_up, shared_down, post_gain, routes,
            route_weights,
        )
    row_count = x_in.shape[0]
    channels = x_in.shape[1]
    reach = conv_taps.shape[0] - 1
    edge_rows = jnp.concatenate([x_in[row_count - reach :], gate_c[row_count - reach :]], 1)
    arrived_edge = passed_along(edge_rows, "sp", 1)
    inputs = jnp.concatenate([arrived_edge[:, :channels], x_in], 0).astype(jnp.float32)
    gate_rows = jnp.concatenate([arrived_edge[:, channels:], gate_c], 0).astype(jnp.float32)
    mixed_in = inputs * gate_rows
    taps = conv_taps.astype(jnp.float32)
    convolved = jnp.zeros((row_count, channels), jnp.float32)
    for index in range(reach + 1):
        convolved = convolved + taps[index][None, :] * mixed_in[index : index + row_count]
    conv_out = (gate_b.astype(jnp.float32) * convolved).astype(jnp.bfloat16)
    width_all = out_proj.shape[1]
    full_rows = lax.all_to_all(conv_out, "tp", split_axis=0, concat_axis=1, tiled=True)
    projected = jnp.dot(
        full_rows,
        lax.all_gather(out_proj, "tp", axis=0, tiled=True),
        preferred_element_type=jnp.float32,
    )
    row_scale = lax.rsqrt(jnp.mean(projected * projected, axis=1, keepdims=True) + epsilon)
    resid1 = (
        resid.astype(jnp.float32) + projected * row_scale * mix_gain.astype(jnp.float32)
    ).astype(jnp.bfloat16)
    wide_resid = resid1.astype(jnp.float32)
    normed = (
        wide_resid
        * lax.rsqrt(jnp.mean(wide_resid * wide_resid, axis=1, keepdims=True) + epsilon)
        * pre_gain.astype(jnp.float32)
    ).astype(jnp.bfloat16)
    experts = lax.axis_size("sp")
    local_rows = resid.shape[0]
    top_count = routes.shape[1]
    capacity = 3 * local_rows * top_count // (2 * experts)
    flat_ids = routes.reshape(-1)
    onehot = (flat_ids[:, None] == jnp.arange(experts, dtype=jnp.int32)[None, :]).astype(jnp.int32)
    before = jnp.cumsum(onehot, axis=0) - onehot
    position = jnp.sum(before * onehot, axis=1)
    slot_index = flat_ids * capacity + position
    outgoing = (
        jnp.zeros((experts * capacity, width_all), jnp.bfloat16)
        .at[slot_index]
        .set(jnp.repeat(normed, top_count, axis=0))
    )
    received = lax.all_to_all(
        outgoing.reshape(experts, capacity, width_all),
        "sp",
        split_axis=0,
        concat_axis=0,
        tiled=True,
    )
    arrived = received.reshape(experts * capacity, width_all)
    gate_h = jnp.dot(arrived, expert_gate[0], preferred_element_type=jnp.float32)
    up_h = jnp.dot(arrived, expert_up[0], preferred_element_type=jnp.float32)
    hidden = (jax.nn.silu(gate_h) * up_h).astype(jnp.bfloat16)
    expert_out = jnp.dot(hidden, expert_down[0], preferred_element_type=jnp.float32).astype(
        jnp.bfloat16
    )
    returned = lax.all_to_all(
        expert_out.reshape(experts, capacity, width_all),
        "sp",
        split_axis=0,
        concat_axis=0,
        tiled=True,
    )
    returned = returned.reshape(experts * capacity, width_all)
    picked = returned[slot_index].astype(jnp.float32).reshape(local_rows, top_count, width_all)
    routed = jnp.einsum("tk,tkd->td", route_weights, picked)
    shared_g = jnp.dot(normed, shared_gate, preferred_element_type=jnp.float32)
    shared_u = jnp.dot(normed, shared_up, preferred_element_type=jnp.float32)
    shared_hidden = (jax.nn.silu(shared_g) * shared_u).astype(jnp.bfloat16)
    shared_out = jnp.dot(shared_hidden, shared_down, preferred_element_type=jnp.float32)
    branch = routed + shared_out
    factor = lax.rsqrt(jnp.mean(branch * branch, axis=1, keepdims=True) + epsilon)
    return (wide_resid + branch * factor * post_gain.astype(jnp.float32)[None, :]).astype(
        jnp.bfloat16
    )


def solution(mesh):
    return jax.shard_map(
        body,
        mesh=mesh,
        in_specs=(
            P("sp", "tp"),
            P("sp", "tp"),
            P("sp", "tp"),
            P(None, "tp"),
            P("tp", None),
            P(),
            P(("sp", "tp"), None),
            P(),
            P("sp", None, None),
            P("sp", None, None),
            P("sp", None, None),
            P(),
            P(),
            P(),
            P(),
            P(("sp", "tp"), None),
            P(("sp", "tp"), None),
        ),
        out_specs=P(("sp", "tp"), None),
        check_vma=False,
    )
```

```python
import functools

import jax
import jax.numpy as jnp
from jax import lax
from jax.experimental import pallas as pl
from jax.experimental.pallas import tpu as pltpu

P = jax.sharding.PartitionSpec
MESH = pl.DeviceIdType.MESH
epsilon = 1e-06
PIECES = 4
HALVES = 2
DIRECT = (4, 5, 8)
ORDER = (0, 1, 2, 3, 4, -4, 6, 5, -5, 7, 8, -8)
CUTS = ((0, 0, 2), (0, 2, 2), (1, 0, 2), (1, 2, 1), (1, 3, 1))
TABLE = HALVES


def layer_kernel(
    line,
    x_hbm,
    gate_b_hbm,
    gate_c_hbm,
    taps_hbm,
    resid_hbm,
    mix_hbm,
    pre_hbm,
    post_hbm,
    routes_hbm,
    weights_hbm,
    proj_ref,
    eg_ref,
    eu_ref,
    ed_ref,
    sg_ref,
    su_ref,
    sd_ref,
    out_ref,
    x_ref,
    gate_b_ref,
    gate_c_ref,
    taps_ref,
    resid_ref,
    mix_ref,
    pre_ref,
    post_ref,
    routes_ref,
    weights_ref,
    edge_x,
    edge_c,
    mixed,
    conv,
    conv_near,
    proj,
    part_out,
    part_in,
    projected,
    resid1,
    w_gate,
    w_up,
    w_down,
    s_gate,
    s_up,
    s_down,
    blocks,
    shares,
    hidden,
    shared_hidden,
    branch,
    outgoing,
    from_out,
    from_in,
    load_sem,
    edge_send,
    misc_send,
    spread_send,
    relay_send,
    in_send,
    out_send,
    e_recv,
    p_recv,
    c_recv,
    f_recv,
    wx_recv,
    wn_recv,
    wf_recv,
    wr_recv,
    gi_recv,
    go_recv,
    ri_recv,
    ro_recv,
):
    sp = lax.axis_index("sp")
    tp = lax.axis_index("tp")
    sp_size = lax.axis_size("sp")
    tp_size = lax.axis_size("tp")
    z = sp // 2
    x = sp % 2
    last = line - 1
    mate = z * 2 + 1 - x
    near = (tp // 2) * 2 + 1 - tp % 2
    far = (tp + 2) % tp_size
    near_far = (near + 2) % tp_size
    upper = z // (line // 2)
    inward_step = 1 - 2 * upper
    level = upper * last + inward_step * z
    inward = ((z + inward_step) * 2 + x, tp)
    outward = ((z - inward_step) * 2 + x, tp)

    def rel(k):
        return upper * last + inward_step * k

    rows, width = resid_ref.shape
    half_rows = rows // HALVES
    hid = w_gate.shape[2]
    shared_hid = s_gate.shape[1]
    part_cols = width // PIECES

    barrier = pltpu.get_barrier_semaphore()

    def greet(device):
        pl.semaphore_signal(barrier, inc=1, device_id=device, device_id_type=MESH)

    greet((mate, tp))
    greet((sp, near))
    greet((sp, far))

    @pl.when(z > 0)
    def _():
        greet((sp - 2, tp))

    @pl.when(z < last)
    def _():
        greet((sp + 2, tp))

    @pl.when((x == 1) & (z < last))
    def _():
        greet((sp + 1, tp))

    @pl.when((x == 0) & (z > 0))
    def _():
        greet((sp - 1, tp))

    pairs = (
        (x_hbm, x_ref),
        (gate_c_hbm, gate_c_ref),
        (proj_ref, proj.at[0]),
        (gate_b_hbm, gate_b_ref),
        (taps_hbm, taps_ref),
        (routes_hbm, routes_ref),
        (weights_hbm, weights_ref),
        (resid_hbm, resid_ref),
        (mix_hbm, mix_ref),
        (pre_hbm, pre_ref),
        (eg_ref.at[0], w_gate.at[0]),
        (eu_ref.at[0], w_up.at[0]),
        (sg_ref, s_gate),
        (su_ref, s_up),
        (ed_ref.at[0], w_down.at[pl.ds(0, hid)]),
        (sd_ref, s_down),
        (post_hbm, post_ref),
    )
    loads = [pltpu.make_async_copy(src, dst, load_sem.at[n]) for n, (src, dst) in enumerate(pairs)]
    for load in loads:
        load.start()

    all_rows, channels = x_ref.shape
    reach = taps_ref.shape[0] - 1
    pad = edge_x.shape[0]

    def edge_copy(n):
        source, landing = ((x_hbm, edge_x), (gate_c_hbm, edge_c))[n]
        return pltpu.make_async_remote_copy(
            src_ref=source.at[pl.ds(all_rows - pad, pad)],
            dst_ref=landing,
            send_sem=edge_send.at[0],
            recv_sem=e_recv.at[n],
            device_id=((sp + 1) % sp_size, tp),
            device_id_type=MESH,
        )

    def block_rows(owner):
        return pl.ds(pl.multiple_of(owner * rows, rows), rows)

    def conv_copy(n, k):
        begin, size = ((pad, rows - pad), (0, pad))[k]
        return pltpu.make_async_remote_copy(
            src_ref=conv.at[pl.ds(pl.multiple_of((near, near_far)[n] * rows + begin, pad), size)],
            dst_ref=conv_near.at[n, pl.ds(begin, size)],
            send_sem=misc_send.at[0],
            recv_sem=c_recv.at[n, k],
            device_id=(sp, near),
            device_id_type=MESH,
        )

    def chunk(j):
        return pl.ds(pl.multiple_of(j * part_cols, part_cols), part_cols)

    def half(r):
        return pl.ds(r * half_rows, half_rows)

    def proj_copy(j):
        return pltpu.make_async_remote_copy(
            src_ref=proj.at[0, :, chunk(j)],
            dst_ref=proj.at[1, :, chunk(j)],
            send_sem=misc_send.at[0],
            recv_sem=p_recv.at[j],
            device_id=(sp, near),
            device_id_type=MESH,
        )

    def part_copy(j):
        where = (pl.ds(pad, rows - pad), chunk(j))
        return pltpu.make_async_remote_copy(
            src_ref=part_out.at[where],
            dst_ref=part_in.at[where],
            send_sem=misc_send.at[0],
            recv_sem=f_recv.at[j],
            device_id=(sp, far),
            device_id_type=MESH,
        )

    part_head = pltpu.make_async_remote_copy(
        src_ref=part_out.at[pl.ds(0, pad)],
        dst_ref=part_in.at[pl.ds(0, pad)],
        send_sem=misc_send.at[0],
        recv_sem=f_recv.at[PIECES],
        device_id=(sp, far),
        device_id_type=MESH,
    )

    pieces = [((eg_ref, w_gate), (eu_ref, w_up))[k] + (first, size) for k, first, size in CUTS]
    for j in range(PIECES):
        pieces.append((ed_ref, w_down, j, 1))
    count = len(pieces)

    def cut(n, owner):
        ref, held, first, steps = pieces[n]
        if held is w_down:
            size = hid // tp_size
            begin = pl.multiple_of(owner * size, size)
            return (
                ref.at[0, pl.ds(begin, size), chunk(first)],
                held.at[pl.ds(pl.multiple_of(hid + begin, size), size), chunk(first)],
            )
        size = ref.shape[1] // tp_size // 4
        where = pl.ds(pl.multiple_of((owner * 4 + first) * size, size), size * steps)
        return ref.at[0, where], held.at[1, where]

    def hop(n, owner, target, send, recv, first=False):
        source, landing = cut(n, owner)
        return pltpu.make_async_remote_copy(
            src_ref=source if first else landing,
            dst_ref=landing,
            send_sem=send.at[0],
            recv_sem=recv,
            device_id=target,
            device_id_type=MESH,
        )

    def late(n):
        return min(n // 2, 1) + max(0, n - len(CUTS) + 1)

    def x_hop(n):
        return hop(n, tp, (mate, tp), spread_send, wx_recv.at[n], True)

    def near_hop(n, owner):
        return hop(n, owner, (sp, near), spread_send, wn_recv.at[late(n)])

    def far_hop(n, owner):
        return hop(n, owner, (sp, far), relay_send, wf_recv.at[n])

    def direct_hop(n):
        return hop(n, far, (mate, tp), relay_send, wf_recv.at[n], True)

    def relay_hop(n, owner):
        return hop(n, owner, (sp, near), relay_send, wr_recv.at[late(n)])

    def drain(send, recv, size):
        where = w_down.at[pl.ds(0, size)]
        return pltpu.make_async_remote_copy(
            src_ref=where,
            dst_ref=where,
            send_sem=send.at[0],
            recv_sem=recv.at[0],
            device_id=(sp, near),
            device_id_type=MESH,
        )

    def spread(n):
        with jax.named_scope("w_x"):
            x_hop(n).wait_recv()
        if n not in DIRECT:
            far_hop(n, tp).start()
        near_hop(n, tp).start()

    def relay(n):
        with jax.named_scope("w_far"):
            far_hop(n, far).wait_recv()
        relay_hop(n, far).start()

    def ready(n):
        with jax.named_scope("w_ready"):
            near_hop(n, near).wait_recv()
            relay_hop(n, near_far).wait_recv()

    def ready_part(k):
        with jax.named_scope("w_ready"):
            drain(spread_send, wn_recv.at[pl.ds(k, 1)], hid // tp_size).wait_recv()
            drain(relay_send, wr_recv.at[pl.ds(k, 1)], hid // tp_size).wait_recv()

    def block_copy(b, r, target, send, recv):
        ref = shares.at[b] if r == TABLE else blocks.at[b, half(r)]
        return pltpu.make_async_remote_copy(
            src_ref=ref,
            dst_ref=ref,
            send_sem=send.at[0],
            recv_sem=recv,
            device_id=target,
            device_id_type=MESH,
        )

    def edge_in(r):
        return block_copy(rel(0), r, inward, in_send, go_recv.at[r])

    def mid_in(k, r):
        return block_copy(rel(k), r, inward, in_send, gi_recv.at[last - k - 1, r])

    def mid_out(k, r):
        return block_copy(rel(k), r, outward, out_send, gi_recv.at[k - 1, r])

    def got_in(k, r):
        with jax.named_scope("w_gi"):
            block_copy(rel(k), r, inward, in_send, gi_recv.at[k - 1, r]).wait_recv()

    def got_out(r):
        with jax.named_scope("w_go"):
            block_copy(rel(0), r, outward, out_send, go_recv.at[r]).wait_recv()

    def sum_copy(k, r, j, landing, target, send, recv):
        return pltpu.make_async_remote_copy(
            src_ref=outgoing.at[rel(k), half(r), chunk(j)],
            dst_ref=landing.at[rel(k), half(r), chunk(j)],
            send_sem=send.at[0],
            recv_sem=recv.at[j],
            device_id=target,
            device_id_type=MESH,
        )

    def edge_give(k, r, j):
        return sum_copy(k, r, j, from_out, inward, in_send, ro_recv.at[k - 1, r])

    def mid_give_in(k, r, j):
        return sum_copy(k, r, j, from_in, inward, in_send, ri_recv.at[last - k, r])

    def mid_give_out(k, r, j):
        return sum_copy(k, r, j, from_in, outward, out_send, ri_recv.at[k, r])

    def sum_in(k, r, j):
        with jax.named_scope("w_ri"):
            sum_copy(k, r, j, from_in, inward, in_send, ri_recv.at[k, r]).wait_recv()

    def sum_out(k, r, j):
        with jax.named_scope("w_ro"):
            sum_copy(k, r, j, from_out, outward, out_send, ro_recv.at[k - 1, r]).wait_recv()

    with jax.named_scope("w_barrier"):
        met = 3 + jnp.where(z > 0, 1, 0) + jnp.where(z < last, 1, 0)
        met += jnp.where(jnp.where(x == 1, z < last, z > 0), 1, 0)
        pl.semaphore_wait(barrier, met)

    @pl.when(sp < sp_size - 1)
    def _():
        edge_copy(0).start()
        edge_copy(1).start()

    for n in ORDER:
        if n < 0:
            direct_hop(-n).start()
        else:
            x_hop(n).start()

    for n in (0, 1, 3, 4):
        loads[n].wait()
    mixed[:pad] = jnp.zeros((pad, channels), jnp.float32)
    mixed[pad:] = x_ref[...].astype(jnp.float32) * gate_c_ref[...].astype(jnp.float32)

    def convolve(size):
        convolved = jnp.zeros((size, channels), jnp.float32)
        for k in range(reach + 1):
            begin = pad - reach + k
            convolved += taps_ref[k : k + 1].astype(jnp.float32) * mixed[begin : begin + size]
        conv[:size] = (gate_b_ref[:size].astype(jnp.float32) * convolved).astype(jnp.bfloat16)

    convolve(all_rows)
    conv_copy(1, 0).start()
    loads[2].wait()
    for j in range(PIECES):
        proj_copy(j).start()
    conv_copy(0, 0).start()
    loads[5].wait()
    loads[6].wait()
    lanes = lax.broadcasted_iota(jnp.int32, (rows, shares.shape[2]), 1)
    names = lax.broadcasted_iota(jnp.int32, (shares.shape[2], rows), 0)
    table = jnp.zeros((shares.shape[2], rows), jnp.float32)
    for k in range(routes_ref.shape[0]):
        table += jnp.where(names == routes_ref[k : k + 1], weights_ref[k : k + 1], 0.0)
    own = z
    shares[own] = table.T

    def send_own(r):
        @pl.when(level == 0)
        def _():
            edge_in(r).start()

        @pl.when(level == 1)
        def _():
            if r != HALVES - 1:
                mid_in(1, r).start()
            mid_out(1, r).start()

    send_own(TABLE)

    def project(n, owner, cols, begin, size):
        mine = pl.ds(pl.multiple_of(owner * rows + begin, pad), size)
        return jnp.dot(
            conv[mine], proj[0, :, cols], preferred_element_type=jnp.float32
        ) + jnp.dot(
            conv_near[n, begin : begin + size], proj[1, :, cols], preferred_element_type=jnp.float32
        )

    with jax.named_scope("w_conv"):
        conv_copy(1, 0).wait_recv()

    @pl.loop(0, PIECES)
    def _(j):
        proj_copy(j).wait_recv()
        part_out[pad:, chunk(j)] = project(1, far, chunk(j), pad, rows - pad).astype(jnp.bfloat16)
        part_copy(j).start()

    with jax.named_scope("w_edge"):

        @pl.when(sp > 0)
        def _():
            edge_copy(0).wait_recv()
            edge_copy(1).wait_recv()
            mixed[:pad] = edge_x[...].astype(jnp.float32) * edge_c[...].astype(jnp.float32)

    convolve(pad)
    conv_copy(1, 1).start()
    conv_copy(0, 1).start()
    with jax.named_scope("w_head"):
        conv_copy(1, 1).wait_recv()

    @pl.loop(0, PIECES)
    def _(j):
        part_out[:pad, chunk(j)] = project(1, far, chunk(j), 0, pad).astype(jnp.bfloat16)

    part_head.start()
    conv_copy(0, 0).wait_recv()
    conv_copy(0, 1).wait_recv()

    @pl.loop(0, PIECES)
    def _(j):
        projected[:, chunk(j)] = project(0, tp, chunk(j), 0, rows)

    spread(0)
    spread(1)
    for load in loads[7:10]:
        load.wait()

    with jax.named_scope("w_part"):

        @pl.loop(0, PIECES)
        def _(j):
            part_copy(j).wait_recv()
            projected[pad:, chunk(j)] += part_in[pad:, chunk(j)].astype(jnp.float32)

        part_head.wait_recv()
        projected[:pad] += part_in[:pad].astype(jnp.float32)

    with jax.named_scope("norm"):
        for r in range(HALVES):
            part = half(r)
            block = projected[part]
            scale = lax.rsqrt(jnp.mean(block * block, axis=1, keepdims=True) + epsilon)
            mid = (
                resid_ref[part].astype(jnp.float32)
                + block * scale * mix_ref[...].astype(jnp.float32).reshape(1, width)
            ).astype(jnp.bfloat16)
            resid1[part] = mid
            wide = mid.astype(jnp.float32)
            normal = lax.rsqrt(jnp.mean(wide * wide, axis=1, keepdims=True) + epsilon)
            blocks[own, part] = (
                wide * normal * pre_ref[...].astype(jnp.float32).reshape(1, width)
            ).astype(jnp.bfloat16)

            send_own(r)

    spread(2)

    def hide(b, begin, size, e):
        part = pl.ds(begin, size)
        expert = z * 2 + x + e * (1 - 2 * x)
        share = jnp.sum(
            jnp.where(lanes[:size] == expert, shares[b, part], 0.0), axis=1, keepdims=True
        )

        def step(j):
            cols = pl.ds(pl.multiple_of(j * 256, 256), 256)
            gate = jnp.dot(blocks[b, part], w_gate[e, :, cols], preferred_element_type=jnp.float32)
            up = jnp.dot(blocks[b, part], w_up[e, :, cols], preferred_element_type=jnp.float32)
            kept = pl.ds(pl.multiple_of(e * hid + j * 256, 256), 256)
            hidden[b, part, kept] = (jax.nn.silu(gate) * up * share).astype(jnp.bfloat16)

        if size < rows:
            for j in range(hid // 256):
                step(j)
        else:
            pl.loop(0, hid // 256)(step)

    def share_of(b, e):
        expert = z * 2 + x + e * (1 - 2 * x)
        return jnp.sum(jnp.where(lanes == expert, shares[b], 0.0), axis=1, keepdims=True)

    def gate_ahead(b):
        share = share_of(b, 1)

        @pl.loop(0, hid // 256)
        def _(j):
            cols = pl.ds(pl.multiple_of(j * 256, 256), 256)
            gate = jnp.dot(blocks[b], w_gate[1, :, cols], preferred_element_type=jnp.float32)
            projected[:, cols] = jax.nn.silu(gate) * share

    def up_after(b):
        for j in range(hid // 256):
            cols = pl.ds(j * 256, 256)
            up = jnp.dot(blocks[b], w_up[1, :, cols], preferred_element_type=jnp.float32)
            kept = pl.ds(hid + j * 256, 256)
            hidden[b, :, kept] = (projected[:, cols] * up).astype(jnp.bfloat16)

    def hide_all(b, e):
        hide(b, 0, rows, e)

    def hide_half(b, r):
        hide(b, r * half_rows, half_rows, 0)
        hide(b, r * half_rows, half_rows, 1)

    def down(b, part, j):
        return jnp.dot(
            hidden[b, part], w_down[:, chunk(j)], preferred_element_type=jnp.float32
        )

    def give(k, r, j, arrived, send):
        made = down(rel(k), half(r), j)
        if arrived is not None:
            made += arrived[rel(k), half(r), chunk(j)].astype(jnp.float32)
        outgoing[rel(k), half(r), chunk(j)] = made.astype(jnp.bfloat16)
        send(k, r, j).start()

    def shared_up_to_hidden():
        s_g = jnp.dot(blocks[own], s_gate[...], preferred_element_type=jnp.float32)
        s_u = jnp.dot(blocks[own], s_up[...], preferred_element_type=jnp.float32)
        shared_hidden[...] = (jax.nn.silu(s_g) * s_u).astype(jnp.bfloat16)

    def own_branch():
        @pl.loop(0, PIECES)
        def _(j):
            branch[:, chunk(j)] = down(own, pl.ds(0, rows), j) + jnp.dot(
                shared_hidden[...], s_down[:, chunk(j)], preferred_element_type=jnp.float32
            )

    def yield_out(r, total):
        factor = lax.rsqrt(jnp.mean(total * total, axis=1, keepdims=True) + epsilon)
        out_ref[half(r)] = (
            resid1[half(r)].astype(jnp.float32)
            + total * factor * post_ref[...].astype(jnp.float32).reshape(1, width)
        ).astype(jnp.bfloat16)

    def settle():
        @pl.when(sp < sp_size - 1)
        def _():
            drain(edge_send, e_recv, 2 * pad * channels // width).wait_send()

        drain(misc_send, e_recv, channels + 2 * rows * channels // width + rows).wait_send()
        drain(spread_send, e_recv, 2 * 3 * hid // tp_size).wait_send()
        drain(relay_send, e_recv, 2 * 3 * hid // tp_size).wait_send()

    sent_block = rows + 2 * rows * shares.shape[2] // width
    sent_sums = rows

    for load in loads[10:14]:
        load.wait()
    hide_all(own, 0)
    shared_up_to_hidden()
    relay(0)
    spread(3)
    for load in loads[14:]:
        load.wait()

    @pl.when(level == 0)
    def _():
        got_in(1, TABLE)
        got_in(1, 0)
        hide(rel(1), 0, half_rows, 0)
        spread(4)
        relay(1)
        relay(4)
        spread(6)
        got_in(1, 1)
        hide(rel(1), half_rows, half_rows, 0)
        relay(2)
        ready_part(0)
        gate_ahead(rel(1))
        spread(5)
        relay(3)
        relay(5)
        ready_part(1)
        up_after(rel(1))
        ready(5)
        for r in range(HALVES):
            give(1, r, 0, None, edge_give)
        relay(6)
        spread(7)
        ready(6)
        for r in range(HALVES):
            give(1, r, 1, None, edge_give)
        got_in(2, TABLE)
        got_in(2, 0)
        hide_half(rel(2), 0)

        @pl.loop(0, 2)
        def _(j):
            give(2, 0, j, None, edge_give)

        spread(8)
        got_in(3, TABLE)
        got_in(3, 0)
        hide_half(rel(3), 0)

        @pl.loop(0, 2)
        def _(j):
            give(3, 0, j, None, edge_give)

        relay(7)
        relay(8)
        ready(7)
        ready(8)

        @pl.loop(2, PIECES)
        def _(j):
            give(3, 0, j, None, edge_give)

        got_in(3, 1)
        hide_half(rel(3), 1)

        @pl.loop(0, PIECES)
        def _(j):
            give(3, 1, j, None, edge_give)

        @pl.loop(2, PIECES)
        def _(j):
            give(2, 0, j, None, edge_give)

        hide_all(own, 1)
        got_in(2, 1)
        hide_half(rel(2), 1)

        @pl.loop(0, PIECES)
        def _(j):
            give(2, 1, j, None, edge_give)

        @pl.loop(2, PIECES)
        def _(j):
            for r in range(HALVES):
                give(1, r, j, None, edge_give)

        own_branch()
        settle()
        for r in range(HALVES):

            @pl.loop(0, PIECES)
            def _(j):
                sum_in(0, r, j)

            total = branch[half(r)] + from_in[own, half(r)].astype(jnp.float32)
            yield_out(r, total)

        drain(in_send, e_recv, sent_block + 3 * sent_sums).wait_send()

    @pl.when(level == 1)
    def _():
        def pass_in(r):
            got_out(r)
            mid_in(0, r).start()

        def pass_out(k, r):
            got_in(k, r)
            mid_out(k, r).start()

        pass_in(TABLE)
        pass_out(2, TABLE)
        pass_in(0)
        pass_out(2, 0)
        pass_out(3, TABLE)
        spread(4)
        relay(1)
        relay(4)
        spread(6)
        pass_in(1)
        mid_in(1, HALVES - 1).start()
        pass_out(3, 0)
        hide_all(rel(0), 0)
        relay(2)
        spread(5)
        relay(3)
        relay(5)
        ready_part(0)
        ready_part(1)
        hide_half(rel(2), 0)
        relay(6)
        spread(7)
        pass_out(3, 1)
        hide_all(own, 1)
        spread(8)
        hide_all(rel(3), 0)
        relay(7)
        relay(8)
        hide_all(rel(3), 1)
        pass_out(2, 1)
        hide_half(rel(2), 1)
        hide_all(rel(0), 1)
        for n in range(len(CUTS), count):
            ready(n)

        def give_in(k, r, j):
            sum_out(k, r, j)
            give(k, r, j, from_out, mid_give_in)

        def give_out(r, j):
            sum_in(0, r, j)
            give(0, r, j, from_in, mid_give_out)

        @pl.loop(0, 2)
        def _(j):
            give_in(2, 0, j)

        own_branch()

        @pl.loop(0, PIECES)
        def _(j):
            give_in(3, 0, j)

        settle()

        @pl.loop(0, PIECES)
        def _(j):
            give_out(0, j)
            give_in(3, 1, j)

        @pl.loop(0, 2)
        def _(j):
            give_out(1, j)

        @pl.loop(2, PIECES)
        def _(j):
            give_in(2, 0, j)
            give_out(1, j)

        @pl.loop(0, PIECES)
        def _(j):
            give_in(2, 1, j)

        for r in range(HALVES):

            @pl.loop(0, PIECES)
            def _(j):
                sum_in(1, r, j)
                sum_out(1, r, j)

            total = (
                branch[half(r)]
                + from_in[own, half(r)].astype(jnp.float32)
                + from_out[own, half(r)].astype(jnp.float32)
            )
            yield_out(r, total)

        drain(in_send, e_recv, 2 * sent_block + 2 * sent_sums).wait_send()
        drain(out_send, e_recv, 3 * sent_block + sent_sums).wait_send()


def fused_layer(
    x_in, gate_b, gate_c, conv_taps, out_proj, mix_gain, resid, pre_gain, expert_gate, expert_up,
    expert_down, shared_gate, shared_up, shared_down, post_gain, routes, route_weights,
):
    experts = lax.axis_size("sp")
    line = experts // 2
    all_rows, channels = x_in.shape
    rows, width = resid.shape
    hid = expert_gate.shape[2]
    shared_hid = shared_gate.shape[1]
    dma = pltpu.SemaphoreType.DMA
    count = len(CUTS) + PIECES
    bf, f32 = jnp.bfloat16, jnp.float32
    hbm = pl.BlockSpec(memory_space=pltpu.HBM)
    lanes = 128 * (-(-experts // 128))
    pad = 16 * (-(-(conv_taps.shape[0] - 1) // 16))
    top = routes.shape[1]
    return pl.pallas_call(
        functools.partial(layer_kernel, line),
        out_shape=jax.ShapeDtypeStruct((rows, width), bf),
        in_specs=[hbm] * 17,
        out_specs=pl.BlockSpec(memory_space=pltpu.VMEM),
        scratch_shapes=[
            pltpu.VMEM((all_rows, channels), bf),
            pltpu.VMEM((all_rows, channels), bf),
            pltpu.VMEM((all_rows, channels), bf),
            pltpu.VMEM(conv_taps.shape, bf),
            pltpu.VMEM((rows, width), bf),
            pltpu.VMEM((width,), bf),
            pltpu.VMEM((width,), bf),
            pltpu.VMEM((width,), bf),
            pltpu.VMEM((top, rows), jnp.int32),
            pltpu.VMEM((top, rows), f32),
            pltpu.VMEM((pad, channels), bf),
            pltpu.VMEM((pad, channels), bf),
            pltpu.VMEM((pad + all_rows, channels), f32),
            pltpu.VMEM((all_rows, channels), bf),
            pltpu.VMEM((2, rows, channels), bf),
            pltpu.VMEM((2, channels, width), bf),
            pltpu.VMEM((rows, width), bf),
            pltpu.VMEM((rows, width), bf),
            pltpu.VMEM((rows, width), f32),
            pltpu.VMEM((rows, width), bf),
            pltpu.VMEM((2, width, hid), bf),
            pltpu.VMEM((2, width, hid), bf),
            pltpu.VMEM((2 * hid, width), bf),
            pltpu.VMEM((width, shared_hid), bf),
            pltpu.VMEM((width, shared_hid), bf),
            pltpu.VMEM((shared_hid, width), bf),
            pltpu.VMEM((line, rows, width), bf),
            pltpu.VMEM((line, rows, lanes), f32),
            pltpu.VMEM((line, rows, 2 * hid), bf),
            pltpu.VMEM((rows, shared_hid), bf),
            pltpu.VMEM((rows, width), f32),
            pltpu.VMEM((line, rows, width), bf),
            pltpu.VMEM((line, rows, width), bf),
            pltpu.VMEM((line, rows, width), bf),
            dma((17,)),
        ]
        + [dma((1,))] * 6
        + [
            dma((2,)),
            dma((PIECES,)),
            dma((2, 2)),
            dma((PIECES + 1,)),
            dma((count,)),
            dma((2 + PIECES,)),
            dma((count,)),
            dma((2 + PIECES,)),
            dma((line - 1, HALVES + 1)),
            dma((HALVES + 1,)),
            dma((2, HALVES, PIECES)),
            dma((line - 1, HALVES, PIECES)),
        ],
        compiler_params=pltpu.CompilerParams(
            collective_id=0, has_side_effects=True, vmem_limit_bytes=46 * 1024 * 1024
        ),
    )(
        *(
            pltpu.with_memory_space_constraint(ref, pltpu.HBM)
            for ref in (
                x_in, gate_b, gate_c, conv_taps, resid, mix_gain, pre_gain, post_gain,
                routes.T, route_weights.T, out_proj, expert_gate, expert_up, expert_down,
                shared_gate, shared_up, shared_down,
            )
        )
    )


def passed_along(shard, axis, by):
    size = lax.axis_size(axis)
    pairs = [(i, i + by) for i in range(size) if 0 <= i + by < size]
    return lax.ppermute(shard, axis, pairs)


def body(
    x_in,
    gate_b,
    gate_c,
    conv_taps,
    out_proj,
    mix_gain,
    resid,
    pre_gain,
    expert_gate,
    expert_up,
    expert_down,
    shared_gate,
    shared_up,
    shared_down,
    post_gain,
    routes,
    route_weights,
):
    group = lax.axis_size("sp")
    wide_slots = 3 * resid.shape[0] * routes.shape[1] // group
    if wide_slots > resid.shape[0] and group == 2 * 2 * 2 and lax.axis_size("tp") == 2 * 2:
        return fused_layer(
            x_in, gate_b, gate_c, conv_taps, out_proj, mix_gain, resid, pre_gain, expert_gate,
            expert_up, expert_down, shared_gate, shared_up, shared_down, post_gain, routes,
            route_weights,
        )
    row_count = x_in.shape[0]
    channels = x_in.shape[1]
    reach = conv_taps.shape[0] - 1
    edge_rows = jnp.concatenate([x_in[row_count - reach :], gate_c[row_count - reach :]], 1)
    arrived_edge = passed_along(edge_rows, "sp", 1)
    inputs = jnp.concatenate([arrived_edge[:, :channels], x_in], 0).astype(jnp.float32)
    gate_rows = jnp.concatenate([arrived_edge[:, channels:], gate_c], 0).astype(jnp.float32)
    mixed_in = inputs * gate_rows
    taps = conv_taps.astype(jnp.float32)
    convolved = jnp.zeros((row_count, channels), jnp.float32)
    for index in range(reach + 1):
        convolved = convolved + taps[index][None, :] * mixed_in[index : index + row_count]
    conv_out = (gate_b.astype(jnp.float32) * convolved).astype(jnp.bfloat16)
    width_all = out_proj.shape[1]
    full_rows = lax.all_to_all(conv_out, "tp", split_axis=0, concat_axis=1, tiled=True)
    projected = jnp.dot(
        full_rows,
        lax.all_gather(out_proj, "tp", axis=0, tiled=True),
        preferred_element_type=jnp.float32,
    )
    row_scale = lax.rsqrt(jnp.mean(projected * projected, axis=1, keepdims=True) + epsilon)
    resid1 = (
        resid.astype(jnp.float32) + projected * row_scale * mix_gain.astype(jnp.float32)
    ).astype(jnp.bfloat16)
    wide_resid = resid1.astype(jnp.float32)
    normed = (
        wide_resid
        * lax.rsqrt(jnp.mean(wide_resid * wide_resid, axis=1, keepdims=True) + epsilon)
        * pre_gain.astype(jnp.float32)
    ).astype(jnp.bfloat16)
    experts = lax.axis_size("sp")
    local_rows = resid.shape[0]
    top_count = routes.shape[1]
    capacity = 3 * local_rows * top_count // (2 * experts)
    flat_ids = routes.reshape(-1)
    onehot = (flat_ids[:, None] == jnp.arange(experts, dtype=jnp.int32)[None, :]).astype(jnp.int32)
    before = jnp.cumsum(onehot, axis=0) - onehot
    position = jnp.sum(before * onehot, axis=1)
    slot_index = flat_ids * capacity + position
    outgoing = (
        jnp.zeros((experts * capacity, width_all), jnp.bfloat16)
        .at[slot_index]
        .set(jnp.repeat(normed, top_count, axis=0))
    )
    received = lax.all_to_all(
        outgoing.reshape(experts, capacity, width_all),
        "sp",
        split_axis=0,
        concat_axis=0,
        tiled=True,
    )
    arrived = received.reshape(experts * capacity, width_all)
    gate_h = jnp.dot(arrived, expert_gate[0], preferred_element_type=jnp.float32)
    up_h = jnp.dot(arrived, expert_up[0], preferred_element_type=jnp.float32)
    hidden = (jax.nn.silu(gate_h) * up_h).astype(jnp.bfloat16)
    expert_out = jnp.dot(hidden, expert_down[0], preferred_element_type=jnp.float32).astype(
        jnp.bfloat16
    )
    returned = lax.all_to_all(
        expert_out.reshape(experts, capacity, width_all),
        "sp",
        split_axis=0,
        concat_axis=0,
        tiled=True,
    )
    returned = returned.reshape(experts * capacity, width_all)
    picked = returned[slot_index].astype(jnp.float32).reshape(local_rows, top_count, width_all)
    routed = jnp.einsum("tk,tkd->td", route_weights, picked)
    shared_g = jnp.dot(normed, shared_gate, preferred_element_type=jnp.float32)
    shared_u = jnp.dot(normed, shared_up, preferred_element_type=jnp.float32)
    shared_hidden = (jax.nn.silu(shared_g) * shared_u).astype(jnp.bfloat16)
    shared_out = jnp.dot(shared_hidden, shared_down, preferred_element_type=jnp.float32)
    branch = routed + shared_out
    factor = lax.rsqrt(jnp.mean(branch * branch, axis=1, keepdims=True) + epsilon)
    return (wide_resid + branch * factor * post_gain.astype(jnp.float32)[None, :]).astype(
        jnp.bfloat16
    )


def solution(mesh):
    return jax.shard_map(
        body,
        mesh=mesh,
        in_specs=(
            P("sp", "tp"),
            P("sp", "tp"),
            P("sp", "tp"),
            P(None, "tp"),
            P("tp", None),
            P(),
            P(("sp", "tp"), None),
            P(),
            P("sp", None, None),
            P("sp", None, None),
            P("sp", None, None),
            P(),
            P(),
            P(),
            P(),
            P(("sp", "tp"), None),
            P(("sp", "tp"), None),
        ),
        out_specs=P(("sp", "tp"), None),
        check_vma=False,
    )
```

```python
import functools

import jax
import jax.numpy as jnp
from jax import lax
from jax.experimental import pallas as pl
from jax.experimental.pallas import tpu as pltpu

P = jax.sharding.PartitionSpec
MESH = pl.DeviceIdType.MESH
epsilon = 1e-06
PIECES = 4
HALVES = 2
DIRECT = (4, 5, 8)
ORDER = (0, 1, 2, 3, 4, -4, 6, 5, -5, 7, 8, -8)
CUTS = ((0, 0, 8), (0, 8, 8), (1, 0, 8), (1, 8, 5), (1, 13, 3))
SLICES = 16
TABLE = HALVES


def layer_kernel(
    line,
    x_hbm,
    gate_b_hbm,
    gate_c_hbm,
    taps_hbm,
    resid_hbm,
    mix_hbm,
    pre_hbm,
    post_hbm,
    routes_hbm,
    weights_hbm,
    proj_ref,
    eg_ref,
    eu_ref,
    ed_ref,
    sg_ref,
    su_ref,
    sd_ref,
    out_ref,
    x_ref,
    gate_b_ref,
    gate_c_ref,
    taps_ref,
    resid_ref,
    mix_ref,
    pre_ref,
    post_ref,
    routes_ref,
    weights_ref,
    edge_x,
    edge_c,
    mixed,
    conv,
    conv_near,
    proj,
    part_out,
    part_in,
    projected,
    resid1,
    w_gate,
    w_up,
    w_down,
    s_gate,
    s_up,
    s_down,
    blocks,
    shares,
    hidden,
    shared_hidden,
    branch,
    outgoing,
    from_out,
    from_in,
    load_sem,
    edge_send,
    misc_send,
    spread_send,
    relay_send,
    in_send,
    out_send,
    e_recv,
    p_recv,
    c_recv,
    f_recv,
    wx_recv,
    wn_recv,
    wf_recv,
    wr_recv,
    gi_recv,
    go_recv,
    ri_recv,
    ro_recv,
):
    sp = lax.axis_index("sp")
    tp = lax.axis_index("tp")
    sp_size = lax.axis_size("sp")
    tp_size = lax.axis_size("tp")
    z = sp // 2
    x = sp % 2
    last = line - 1
    mate = z * 2 + 1 - x
    near = (tp // 2) * 2 + 1 - tp % 2
    far = (tp + 2) % tp_size
    near_far = (near + 2) % tp_size
    upper = z // (line // 2)
    inward_step = 1 - 2 * upper
    level = upper * last + inward_step * z
    inward = ((z + inward_step) * 2 + x, tp)
    outward = ((z - inward_step) * 2 + x, tp)

    def rel(k):
        return upper * last + inward_step * k

    rows, width = resid_ref.shape
    half_rows = rows // HALVES
    hid = w_gate.shape[2]
    shared_hid = s_gate.shape[1]
    part_cols = width // PIECES

    barrier = pltpu.get_barrier_semaphore()

    def greet(device):
        pl.semaphore_signal(barrier, inc=1, device_id=device, device_id_type=MESH)

    greet((mate, tp))
    greet((sp, near))
    greet((sp, far))

    @pl.when(z > 0)
    def _():
        greet((sp - 2, tp))

    @pl.when(z < last)
    def _():
        greet((sp + 2, tp))

    @pl.when((x == 1) & (z < last))
    def _():
        greet((sp + 1, tp))

    @pl.when((x == 0) & (z > 0))
    def _():
        greet((sp - 1, tp))

    pairs = (
        (x_hbm, x_ref),
        (gate_c_hbm, gate_c_ref),
        (proj_ref, proj.at[0]),
        (gate_b_hbm, gate_b_ref),
        (taps_hbm, taps_ref),
        (routes_hbm, routes_ref),
        (weights_hbm, weights_ref),
        (resid_hbm, resid_ref),
        (mix_hbm, mix_ref),
        (pre_hbm, pre_ref),
        (eg_ref.at[0], w_gate.at[0]),
        (eu_ref.at[0], w_up.at[0]),
        (sg_ref, s_gate),
        (su_ref, s_up),
        (ed_ref.at[0], w_down.at[pl.ds(0, hid)]),
        (sd_ref, s_down),
        (post_hbm, post_ref),
    )
    loads = [pltpu.make_async_copy(src, dst, load_sem.at[n]) for n, (src, dst) in enumerate(pairs)]
    for load in loads:
        load.start()

    all_rows, channels = x_ref.shape
    reach = taps_ref.shape[0] - 1
    pad = edge_x.shape[0]

    def edge_copy(n):
        source, landing = ((x_hbm, edge_x), (gate_c_hbm, edge_c))[n]
        return pltpu.make_async_remote_copy(
            src_ref=source.at[pl.ds(all_rows - pad, pad)],
            dst_ref=landing,
            send_sem=edge_send.at[0],
            recv_sem=e_recv.at[n],
            device_id=((sp + 1) % sp_size, tp),
            device_id_type=MESH,
        )

    def block_rows(owner):
        return pl.ds(pl.multiple_of(owner * rows, rows), rows)

    def conv_copy(n, k):
        begin, size = ((pad, rows - pad), (0, pad))[k]
        return pltpu.make_async_remote_copy(
            src_ref=conv.at[pl.ds(pl.multiple_of((near, near_far)[n] * rows + begin, pad), size)],
            dst_ref=conv_near.at[n, pl.ds(begin, size)],
            send_sem=misc_send.at[0],
            recv_sem=c_recv.at[n, k],
            device_id=(sp, near),
            device_id_type=MESH,
        )

    def chunk(j):
        return pl.ds(pl.multiple_of(j * part_cols, part_cols), part_cols)

    def half(r):
        return pl.ds(r * half_rows, half_rows)

    def proj_copy(j):
        return pltpu.make_async_remote_copy(
            src_ref=proj.at[0, :, chunk(j)],
            dst_ref=proj.at[1, :, chunk(j)],
            send_sem=misc_send.at[0],
            recv_sem=p_recv.at[j],
            device_id=(sp, near),
            device_id_type=MESH,
        )

    def part_copy(j):
        where = (pl.ds(pad, rows - pad), chunk(j))
        return pltpu.make_async_remote_copy(
            src_ref=part_out.at[where],
            dst_ref=part_in.at[where],
            send_sem=misc_send.at[0],
            recv_sem=f_recv.at[j],
            device_id=(sp, far),
            device_id_type=MESH,
        )

    part_head = pltpu.make_async_remote_copy(
        src_ref=part_out.at[pl.ds(0, pad)],
        dst_ref=part_in.at[pl.ds(0, pad)],
        send_sem=misc_send.at[0],
        recv_sem=f_recv.at[PIECES],
        device_id=(sp, far),
        device_id_type=MESH,
    )

    pieces = [((eg_ref, w_gate), (eu_ref, w_up))[k] + (first, size) for k, first, size in CUTS]
    for j in range(PIECES):
        pieces.append((ed_ref, w_down, j, 1))
    count = len(pieces)

    def cut(n, owner):
        ref, held, first, steps = pieces[n]
        if held is w_down:
            size = hid // tp_size
            begin = pl.multiple_of(owner * size, size)
            return (
                ref.at[0, pl.ds(begin, size), chunk(first)],
                held.at[pl.ds(pl.multiple_of(hid + begin, size), size), chunk(first)],
            )
        size = ref.shape[1] // tp_size // SLICES
        where = pl.ds(pl.multiple_of((owner * SLICES + first) * size, size), size * steps)
        return ref.at[0, where], held.at[1, where]

    def hop(n, owner, target, send, recv, first=False):
        source, landing = cut(n, owner)
        return pltpu.make_async_remote_copy(
            src_ref=source if first else landing,
            dst_ref=landing,
            send_sem=send.at[0],
            recv_sem=recv,
            device_id=target,
            device_id_type=MESH,
        )

    def late(n):
        return min(n // 2, 1) + max(0, n - len(CUTS) + 1)

    def x_hop(n):
        return hop(n, tp, (mate, tp), spread_send, wx_recv.at[n], True)

    def near_hop(n, owner):
        return hop(n, owner, (sp, near), spread_send, wn_recv.at[late(n)])

    def far_hop(n, owner):
        return hop(n, owner, (sp, far), relay_send, wf_recv.at[n])

    def direct_hop(n):
        return hop(n, far, (mate, tp), relay_send, wf_recv.at[n], True)

    def relay_hop(n, owner):
        return hop(n, owner, (sp, near), relay_send, wr_recv.at[late(n)])

    def drain(send, recv, size):
        where = w_down.at[pl.ds(0, size)]
        return pltpu.make_async_remote_copy(
            src_ref=where,
            dst_ref=where,
            send_sem=send.at[0],
            recv_sem=recv.at[0],
            device_id=(sp, near),
            device_id_type=MESH,
        )

    def spread(n):
        with jax.named_scope("w_x"):
            x_hop(n).wait_recv()
        if n not in DIRECT:
            far_hop(n, tp).start()
        near_hop(n, tp).start()

    def relay(n):
        with jax.named_scope("w_far"):
            far_hop(n, far).wait_recv()
        relay_hop(n, far).start()

    def ready(n):
        with jax.named_scope("w_ready"):
            near_hop(n, near).wait_recv()
            relay_hop(n, near_far).wait_recv()

    def ready_part(k):
        with jax.named_scope("w_ready"):
            drain(spread_send, wn_recv.at[pl.ds(k, 1)], hid // tp_size).wait_recv()
            drain(relay_send, wr_recv.at[pl.ds(k, 1)], hid // tp_size).wait_recv()

    def block_copy(b, r, target, send, recv):
        ref = shares.at[b] if r == TABLE else blocks.at[b, half(r)]
        return pltpu.make_async_remote_copy(
            src_ref=ref,
            dst_ref=ref,
            send_sem=send.at[0],
            recv_sem=recv,
            device_id=target,
            device_id_type=MESH,
        )

    def edge_in(r):
        return block_copy(rel(0), r, inward, in_send, go_recv.at[r])

    def mid_in(k, r):
        return block_copy(rel(k), r, inward, in_send, gi_recv.at[last - k - 1, r])

    def mid_out(k, r):
        return block_copy(rel(k), r, outward, out_send, gi_recv.at[k - 1, r])

    def got_in(k, r):
        with jax.named_scope("w_gi"):
            block_copy(rel(k), r, inward, in_send, gi_recv.at[k - 1, r]).wait_recv()

    def got_out(r):
        with jax.named_scope("w_go"):
            block_copy(rel(0), r, outward, out_send, go_recv.at[r]).wait_recv()

    def sum_copy(k, r, j, landing, target, send, recv):
        return pltpu.make_async_remote_copy(
            src_ref=outgoing.at[rel(k), half(r), chunk(j)],
            dst_ref=landing.at[rel(k), half(r), chunk(j)],
            send_sem=send.at[0],
            recv_sem=recv.at[j],
            device_id=target,
            device_id_type=MESH,
        )

    def edge_give(k, r, j):
        return sum_copy(k, r, j, from_out, inward, in_send, ro_recv.at[k - 1, r])

    def mid_give_in(k, r, j):
        return sum_copy(k, r, j, from_in, inward, in_send, ri_recv.at[last - k, r])

    def mid_give_out(k, r, j):
        return sum_copy(k, r, j, from_in, outward, out_send, ri_recv.at[k, r])

    def sum_in(k, r, j):
        with jax.named_scope("w_ri"):
            sum_copy(k, r, j, from_in, inward, in_send, ri_recv.at[k, r]).wait_recv()

    def sum_out(k, r, j):
        with jax.named_scope("w_ro"):
            sum_copy(k, r, j, from_out, outward, out_send, ro_recv.at[k - 1, r]).wait_recv()

    with jax.named_scope("w_barrier"):
        met = 3 + jnp.where(z > 0, 1, 0) + jnp.where(z < last, 1, 0)
        met += jnp.where(jnp.where(x == 1, z < last, z > 0), 1, 0)
        pl.semaphore_wait(barrier, met)

    @pl.when(sp < sp_size - 1)
    def _():
        edge_copy(0).start()
        edge_copy(1).start()

    for n in ORDER:
        if n < 0:
            direct_hop(-n).start()
        else:
            x_hop(n).start()

    for n in (0, 1, 3, 4):
        loads[n].wait()
    mixed[:pad] = jnp.zeros((pad, channels), jnp.float32)
    mixed[pad:] = x_ref[...].astype(jnp.float32) * gate_c_ref[...].astype(jnp.float32)

    def convolve(size):
        convolved = jnp.zeros((size, channels), jnp.float32)
        for k in range(reach + 1):
            begin = pad - reach + k
            convolved += taps_ref[k : k + 1].astype(jnp.float32) * mixed[begin : begin + size]
        conv[:size] = (gate_b_ref[:size].astype(jnp.float32) * convolved).astype(jnp.bfloat16)

    convolve(all_rows)
    conv_copy(1, 0).start()
    loads[2].wait()
    for j in range(PIECES):
        proj_copy(j).start()
    conv_copy(0, 0).start()
    loads[5].wait()
    loads[6].wait()
    lanes = lax.broadcasted_iota(jnp.int32, (rows, shares.shape[2]), 1)
    names = lax.broadcasted_iota(jnp.int32, (shares.shape[2], rows), 0)
    table = jnp.zeros((shares.shape[2], rows), jnp.float32)
    for k in range(routes_ref.shape[0]):
        table += jnp.where(names == routes_ref[k : k + 1], weights_ref[k : k + 1], 0.0)
    own = z
    shares[own] = table.T

    def send_own(r):
        @pl.when(level == 0)
        def _():
            edge_in(r).start()

        @pl.when(level == 1)
        def _():
            if r != HALVES - 1:
                mid_in(1, r).start()
            mid_out(1, r).start()

    send_own(TABLE)

    def project(n, owner, cols, begin, size):
        mine = pl.ds(pl.multiple_of(owner * rows + begin, pad), size)
        return jnp.dot(
            conv[mine], proj[0, :, cols], preferred_element_type=jnp.float32
        ) + jnp.dot(
            conv_near[n, begin : begin + size], proj[1, :, cols], preferred_element_type=jnp.float32
        )

    with jax.named_scope("w_conv"):
        conv_copy(1, 0).wait_recv()

    @pl.loop(0, PIECES)
    def _(j):
        proj_copy(j).wait_recv()
        part_out[pad:, chunk(j)] = project(1, far, chunk(j), pad, rows - pad).astype(jnp.bfloat16)
        part_copy(j).start()

    with jax.named_scope("w_edge"):

        @pl.when(sp > 0)
        def _():
            edge_copy(0).wait_recv()
            edge_copy(1).wait_recv()
            mixed[:pad] = edge_x[...].astype(jnp.float32) * edge_c[...].astype(jnp.float32)

    convolve(pad)
    conv_copy(1, 1).start()
    conv_copy(0, 1).start()
    with jax.named_scope("w_head"):
        conv_copy(1, 1).wait_recv()

    @pl.loop(0, PIECES)
    def _(j):
        part_out[:pad, chunk(j)] = project(1, far, chunk(j), 0, pad).astype(jnp.bfloat16)

    part_head.start()
    conv_copy(0, 0).wait_recv()
    conv_copy(0, 1).wait_recv()

    @pl.loop(0, PIECES)
    def _(j):
        projected[:, chunk(j)] = project(0, tp, chunk(j), 0, rows)

    spread(0)
    spread(1)
    for load in loads[7:10]:
        load.wait()

    with jax.named_scope("w_part"):

        @pl.loop(0, PIECES)
        def _(j):
            part_copy(j).wait_recv()
            projected[pad:, chunk(j)] += part_in[pad:, chunk(j)].astype(jnp.float32)

        part_head.wait_recv()
        projected[:pad] += part_in[:pad].astype(jnp.float32)

    with jax.named_scope("norm"):
        for r in range(HALVES):
            part = half(r)
            block = projected[part]
            scale = lax.rsqrt(jnp.mean(block * block, axis=1, keepdims=True) + epsilon)
            mid = (
                resid_ref[part].astype(jnp.float32)
                + block * scale * mix_ref[...].astype(jnp.float32).reshape(1, width)
            ).astype(jnp.bfloat16)
            resid1[part] = mid
            wide = mid.astype(jnp.float32)
            normal = lax.rsqrt(jnp.mean(wide * wide, axis=1, keepdims=True) + epsilon)
            blocks[own, part] = (
                wide * normal * pre_ref[...].astype(jnp.float32).reshape(1, width)
            ).astype(jnp.bfloat16)

            send_own(r)

    spread(2)

    def hide(b, begin, size, e):
        part = pl.ds(begin, size)
        expert = z * 2 + x + e * (1 - 2 * x)
        share = jnp.sum(
            jnp.where(lanes[:size] == expert, shares[b, part], 0.0), axis=1, keepdims=True
        )

        def step(j):
            cols = pl.ds(pl.multiple_of(j * 256, 256), 256)
            gate = jnp.dot(blocks[b, part], w_gate[e, :, cols], preferred_element_type=jnp.float32)
            up = jnp.dot(blocks[b, part], w_up[e, :, cols], preferred_element_type=jnp.float32)
            kept = pl.ds(pl.multiple_of(e * hid + j * 256, 256), 256)
            hidden[b, part, kept] = (jax.nn.silu(gate) * up * share).astype(jnp.bfloat16)

        if size < rows:
            for j in range(hid // 256):
                step(j)
        else:
            pl.loop(0, hid // 256)(step)

    def share_of(b, e):
        expert = z * 2 + x + e * (1 - 2 * x)
        return jnp.sum(jnp.where(lanes == expert, shares[b], 0.0), axis=1, keepdims=True)

    def gate_ahead(b):
        share = share_of(b, 1)

        @pl.loop(0, hid // 256)
        def _(j):
            cols = pl.ds(pl.multiple_of(j * 256, 256), 256)
            gate = jnp.dot(blocks[b], w_gate[1, :, cols], preferred_element_type=jnp.float32)
            projected[:, cols] = jax.nn.silu(gate) * share

    def up_after(b):
        for j in range(hid // 256):
            cols = pl.ds(j * 256, 256)
            up = jnp.dot(blocks[b], w_up[1, :, cols], preferred_element_type=jnp.float32)
            kept = pl.ds(hid + j * 256, 256)
            hidden[b, :, kept] = (projected[:, cols] * up).astype(jnp.bfloat16)

    def hide_all(b, e):
        hide(b, 0, rows, e)

    def hide_half(b, r):
        hide(b, r * half_rows, half_rows, 0)
        hide(b, r * half_rows, half_rows, 1)

    def down(b, part, j):
        return jnp.dot(
            hidden[b, part], w_down[:, chunk(j)], preferred_element_type=jnp.float32
        )

    def give(k, r, j, arrived, send):
        made = down(rel(k), half(r), j)
        if arrived is not None:
            made += arrived[rel(k), half(r), chunk(j)].astype(jnp.float32)
        outgoing[rel(k), half(r), chunk(j)] = made.astype(jnp.bfloat16)
        send(k, r, j).start()

    def shared_up_to_hidden():
        s_g = jnp.dot(blocks[own], s_gate[...], preferred_element_type=jnp.float32)
        s_u = jnp.dot(blocks[own], s_up[...], preferred_element_type=jnp.float32)
        shared_hidden[...] = (jax.nn.silu(s_g) * s_u).astype(jnp.bfloat16)

    def own_branch():
        @pl.loop(0, PIECES)
        def _(j):
            branch[:, chunk(j)] = down(own, pl.ds(0, rows), j) + jnp.dot(
                shared_hidden[...], s_down[:, chunk(j)], preferred_element_type=jnp.float32
            )

    def yield_out(r, total):
        factor = lax.rsqrt(jnp.mean(total * total, axis=1, keepdims=True) + epsilon)
        out_ref[half(r)] = (
            resid1[half(r)].astype(jnp.float32)
            + total * factor * post_ref[...].astype(jnp.float32).reshape(1, width)
        ).astype(jnp.bfloat16)

    def settle():
        @pl.when(sp < sp_size - 1)
        def _():
            drain(edge_send, e_recv, 2 * pad * channels // width).wait_send()

        drain(misc_send, e_recv, channels + 2 * rows * channels // width + rows).wait_send()
        drain(spread_send, e_recv, 2 * 3 * hid // tp_size).wait_send()
        drain(relay_send, e_recv, 2 * 3 * hid // tp_size).wait_send()

    sent_block = rows + 2 * rows * shares.shape[2] // width
    sent_sums = rows

    for load in loads[10:14]:
        load.wait()
    hide_all(own, 0)
    shared_up_to_hidden()
    relay(0)
    spread(3)
    for load in loads[14:]:
        load.wait()

    @pl.when(level == 0)
    def _():
        got_in(1, TABLE)
        got_in(1, 0)
        hide(rel(1), 0, half_rows, 0)
        spread(4)
        relay(1)
        relay(4)
        spread(6)
        got_in(1, 1)
        hide(rel(1), half_rows, half_rows, 0)
        relay(2)
        ready_part(0)
        gate_ahead(rel(1))
        spread(5)
        relay(3)
        relay(5)
        ready_part(1)
        up_after(rel(1))
        ready(5)
        for r in range(HALVES):
            give(1, r, 0, None, edge_give)
        relay(6)
        spread(7)
        ready(6)
        for r in range(HALVES):
            give(1, r, 1, None, edge_give)
        got_in(2, TABLE)
        got_in(2, 0)
        hide_half(rel(2), 0)

        @pl.loop(0, 2)
        def _(j):
            give(2, 0, j, None, edge_give)

        spread(8)
        relay(7)
        relay(8)
        got_in(3, TABLE)
        got_in(3, 0)
        hide_half(rel(3), 0)

        @pl.loop(0, 2)
        def _(j):
            give(3, 0, j, None, edge_give)

        ready(7)
        ready(8)

        @pl.loop(2, PIECES)
        def _(j):
            give(3, 0, j, None, edge_give)

        got_in(3, 1)
        hide_half(rel(3), 1)

        @pl.loop(0, PIECES)
        def _(j):
            give(3, 1, j, None, edge_give)

        @pl.loop(2, PIECES)
        def _(j):
            give(2, 0, j, None, edge_give)

        hide_all(own, 1)
        got_in(2, 1)
        hide_half(rel(2), 1)

        @pl.loop(0, PIECES)
        def _(j):
            give(2, 1, j, None, edge_give)

        @pl.loop(2, PIECES)
        def _(j):
            for r in range(HALVES):
                give(1, r, j, None, edge_give)

        own_branch()
        settle()
        for r in range(HALVES):

            @pl.loop(0, PIECES)
            def _(j):
                sum_in(0, r, j)

            total = branch[half(r)] + from_in[own, half(r)].astype(jnp.float32)
            yield_out(r, total)

        drain(in_send, e_recv, sent_block + 3 * sent_sums).wait_send()

    @pl.when(level == 1)
    def _():
        def pass_in(r):
            got_out(r)
            mid_in(0, r).start()

        def pass_out(k, r):
            got_in(k, r)
            mid_out(k, r).start()

        pass_in(TABLE)
        pass_out(2, TABLE)
        pass_in(0)
        pass_out(2, 0)
        pass_out(3, TABLE)
        spread(4)
        relay(1)
        relay(4)
        spread(6)
        pass_in(1)
        mid_in(1, HALVES - 1).start()
        pass_out(3, 0)
        hide_all(rel(0), 0)
        relay(2)
        spread(5)
        relay(3)
        relay(5)
        ready_part(0)
        ready_part(1)
        hide_half(rel(2), 0)
        relay(6)
        spread(7)
        pass_out(3, 1)
        hide_all(own, 1)
        spread(8)
        hide_all(rel(3), 0)
        relay(7)
        relay(8)
        hide_all(rel(3), 1)
        pass_out(2, 1)
        hide_half(rel(2), 1)
        hide_all(rel(0), 1)
        for n in range(len(CUTS), count):
            ready(n)

        def give_in(k, r, j):
            sum_out(k, r, j)
            give(k, r, j, from_out, mid_give_in)

        def give_out(r, j):
            sum_in(0, r, j)
            give(0, r, j, from_in, mid_give_out)

        @pl.loop(0, 2)
        def _(j):
            give_in(2, 0, j)

        own_branch()

        @pl.loop(0, PIECES)
        def _(j):
            give_in(3, 0, j)

        settle()

        @pl.loop(0, PIECES)
        def _(j):
            give_out(0, j)
            give_in(3, 1, j)

        @pl.loop(0, 2)
        def _(j):
            give_out(1, j)

        @pl.loop(2, PIECES)
        def _(j):
            give_in(2, 0, j)
            give_out(1, j)

        @pl.loop(0, PIECES)
        def _(j):
            give_in(2, 1, j)

        for r in range(HALVES):

            @pl.loop(0, PIECES)
            def _(j):
                sum_in(1, r, j)
                sum_out(1, r, j)

            total = (
                branch[half(r)]
                + from_in[own, half(r)].astype(jnp.float32)
                + from_out[own, half(r)].astype(jnp.float32)
            )
            yield_out(r, total)

        drain(in_send, e_recv, 2 * sent_block + 2 * sent_sums).wait_send()
        drain(out_send, e_recv, 3 * sent_block + sent_sums).wait_send()


def fused_layer(
    x_in, gate_b, gate_c, conv_taps, out_proj, mix_gain, resid, pre_gain, expert_gate, expert_up,
    expert_down, shared_gate, shared_up, shared_down, post_gain, routes, route_weights,
):
    experts = lax.axis_size("sp")
    line = experts // 2
    all_rows, channels = x_in.shape
    rows, width = resid.shape
    hid = expert_gate.shape[2]
    shared_hid = shared_gate.shape[1]
    dma = pltpu.SemaphoreType.DMA
    count = len(CUTS) + PIECES
    bf, f32 = jnp.bfloat16, jnp.float32
    hbm = pl.BlockSpec(memory_space=pltpu.HBM)
    lanes = 128 * (-(-experts // 128))
    pad = 16 * (-(-(conv_taps.shape[0] - 1) // 16))
    top = routes.shape[1]
    return pl.pallas_call(
        functools.partial(layer_kernel, line),
        out_shape=jax.ShapeDtypeStruct((rows, width), bf),
        in_specs=[hbm] * 17,
        out_specs=pl.BlockSpec(memory_space=pltpu.VMEM),
        scratch_shapes=[
            pltpu.VMEM((all_rows, channels), bf),
            pltpu.VMEM((all_rows, channels), bf),
            pltpu.VMEM((all_rows, channels), bf),
            pltpu.VMEM(conv_taps.shape, bf),
            pltpu.VMEM((rows, width), bf),
            pltpu.VMEM((width,), bf),
            pltpu.VMEM((width,), bf),
            pltpu.VMEM((width,), bf),
            pltpu.VMEM((top, rows), jnp.int32),
            pltpu.VMEM((top, rows), f32),
            pltpu.VMEM((pad, channels), bf),
            pltpu.VMEM((pad, channels), bf),
            pltpu.VMEM((pad + all_rows, channels), f32),
            pltpu.VMEM((all_rows, channels), bf),
            pltpu.VMEM((2, rows, channels), bf),
            pltpu.VMEM((2, channels, width), bf),
            pltpu.VMEM((rows, width), bf),
            pltpu.VMEM((rows, width), bf),
            pltpu.VMEM((rows, width), f32),
            pltpu.VMEM((rows, width), bf),
            pltpu.VMEM((2, width, hid), bf),
            pltpu.VMEM((2, width, hid), bf),
            pltpu.VMEM((2 * hid, width), bf),
            pltpu.VMEM((width, shared_hid), bf),
            pltpu.VMEM((width, shared_hid), bf),
            pltpu.VMEM((shared_hid, width), bf),
            pltpu.VMEM((line, rows, width), bf),
            pltpu.VMEM((line, rows, lanes), f32),
            pltpu.VMEM((line, rows, 2 * hid), bf),
            pltpu.VMEM((rows, shared_hid), bf),
            pltpu.VMEM((rows, width), f32),
            pltpu.VMEM((line, rows, width), bf),
            pltpu.VMEM((line, rows, width), bf),
            pltpu.VMEM((line, rows, width), bf),
            dma((17,)),
        ]
        + [dma((1,))] * 6
        + [
            dma((2,)),
            dma((PIECES,)),
            dma((2, 2)),
            dma((PIECES + 1,)),
            dma((count,)),
            dma((2 + PIECES,)),
            dma((count,)),
            dma((2 + PIECES,)),
            dma((line - 1, HALVES + 1)),
            dma((HALVES + 1,)),
            dma((2, HALVES, PIECES)),
            dma((line - 1, HALVES, PIECES)),
        ],
        compiler_params=pltpu.CompilerParams(
            collective_id=0, has_side_effects=True, vmem_limit_bytes=46 * 1024 * 1024
        ),
    )(
        *(
            pltpu.with_memory_space_constraint(ref, pltpu.HBM)
            for ref in (
                x_in, gate_b, gate_c, conv_taps, resid, mix_gain, pre_gain, post_gain,
                routes.T, route_weights.T, out_proj, expert_gate, expert_up, expert_down,
                shared_gate, shared_up, shared_down,
            )
        )
    )


def passed_along(shard, axis, by):
    size = lax.axis_size(axis)
    pairs = [(i, i + by) for i in range(size) if 0 <= i + by < size]
    return lax.ppermute(shard, axis, pairs)


def body(
    x_in,
    gate_b,
    gate_c,
    conv_taps,
    out_proj,
    mix_gain,
    resid,
    pre_gain,
    expert_gate,
    expert_up,
    expert_down,
    shared_gate,
    shared_up,
    shared_down,
    post_gain,
    routes,
    route_weights,
):
    group = lax.axis_size("sp")
    wide_slots = 3 * resid.shape[0] * routes.shape[1] // group
    if wide_slots > resid.shape[0] and group == 2 * 2 * 2 and lax.axis_size("tp") == 2 * 2:
        return fused_layer(
            x_in, gate_b, gate_c, conv_taps, out_proj, mix_gain, resid, pre_gain, expert_gate,
            expert_up, expert_down, shared_gate, shared_up, shared_down, post_gain, routes,
            route_weights,
        )
    row_count = x_in.shape[0]
    channels = x_in.shape[1]
    reach = conv_taps.shape[0] - 1
    edge_rows = jnp.concatenate([x_in[row_count - reach :], gate_c[row_count - reach :]], 1)
    arrived_edge = passed_along(edge_rows, "sp", 1)
    inputs = jnp.concatenate([arrived_edge[:, :channels], x_in], 0).astype(jnp.float32)
    gate_rows = jnp.concatenate([arrived_edge[:, channels:], gate_c], 0).astype(jnp.float32)
    mixed_in = inputs * gate_rows
    taps = conv_taps.astype(jnp.float32)
    convolved = jnp.zeros((row_count, channels), jnp.float32)
    for index in range(reach + 1):
        convolved = convolved + taps[index][None, :] * mixed_in[index : index + row_count]
    conv_out = (gate_b.astype(jnp.float32) * convolved).astype(jnp.bfloat16)
    width_all = out_proj.shape[1]
    full_rows = lax.all_to_all(conv_out, "tp", split_axis=0, concat_axis=1, tiled=True)
    projected = jnp.dot(
        full_rows,
        lax.all_gather(out_proj, "tp", axis=0, tiled=True),
        preferred_element_type=jnp.float32,
    )
    row_scale = lax.rsqrt(jnp.mean(projected * projected, axis=1, keepdims=True) + epsilon)
    resid1 = (
        resid.astype(jnp.float32) + projected * row_scale * mix_gain.astype(jnp.float32)
    ).astype(jnp.bfloat16)
    wide_resid = resid1.astype(jnp.float32)
    normed = (
        wide_resid
        * lax.rsqrt(jnp.mean(wide_resid * wide_resid, axis=1, keepdims=True) + epsilon)
        * pre_gain.astype(jnp.float32)
    ).astype(jnp.bfloat16)
    experts = lax.axis_size("sp")
    local_rows = resid.shape[0]
    top_count = routes.shape[1]
    capacity = 3 * local_rows * top_count // (2 * experts)
    flat_ids = routes.reshape(-1)
    onehot = (flat_ids[:, None] == jnp.arange(experts, dtype=jnp.int32)[None, :]).astype(jnp.int32)
    before = jnp.cumsum(onehot, axis=0) - onehot
    position = jnp.sum(before * onehot, axis=1)
    slot_index = flat_ids * capacity + position
    outgoing = (
        jnp.zeros((experts * capacity, width_all), jnp.bfloat16)
        .at[slot_index]
        .set(jnp.repeat(normed, top_count, axis=0))
    )
    received = lax.all_to_all(
        outgoing.reshape(experts, capacity, width_all),
        "sp",
        split_axis=0,
        concat_axis=0,
        tiled=True,
    )
    arrived = received.reshape(experts * capacity, width_all)
    gate_h = jnp.dot(arrived, expert_gate[0], preferred_element_type=jnp.float32)
    up_h = jnp.dot(arrived, expert_up[0], preferred_element_type=jnp.float32)
    hidden = (jax.nn.silu(gate_h) * up_h).astype(jnp.bfloat16)
    expert_out = jnp.dot(hidden, expert_down[0], preferred_element_type=jnp.float32).astype(
        jnp.bfloat16
    )
    returned = lax.all_to_all(
        expert_out.reshape(experts, capacity, width_all),
        "sp",
        split_axis=0,
        concat_axis=0,
        tiled=True,
    )
    returned = returned.reshape(experts * capacity, width_all)
    picked = returned[slot_index].astype(jnp.float32).reshape(local_rows, top_count, width_all)
    routed = jnp.einsum("tk,tkd->td", route_weights, picked)
    shared_g = jnp.dot(normed, shared_gate, preferred_element_type=jnp.float32)
    shared_u = jnp.dot(normed, shared_up, preferred_element_type=jnp.float32)
    shared_hidden = (jax.nn.silu(shared_g) * shared_u).astype(jnp.bfloat16)
    shared_out = jnp.dot(shared_hidden, shared_down, preferred_element_type=jnp.float32)
    branch = routed + shared_out
    factor = lax.rsqrt(jnp.mean(branch * branch, axis=1, keepdims=True) + epsilon)
    return (wide_resid + branch * factor * post_gain.astype(jnp.float32)[None, :]).astype(
        jnp.bfloat16
    )


def solution(mesh):
    return jax.shard_map(
        body,
        mesh=mesh,
        in_specs=(
            P("sp", "tp"),
            P("sp", "tp"),
            P("sp", "tp"),
            P(None, "tp"),
            P("tp", None),
            P(),
            P(("sp", "tp"), None),
            P(),
            P("sp", None, None),
            P("sp", None, None),
            P("sp", None, None),
            P(),
            P(),
            P(),
            P(),
            P(("sp", "tp"), None),
            P(("sp", "tp"), None),
        ),
        out_specs=P(("sp", "tp"), None),
        check_vma=False,
    )
```

```python
import functools

import jax
import jax.numpy as jnp
from jax import lax
from jax.experimental import pallas as pl
from jax.experimental.pallas import tpu as pltpu

P = jax.sharding.PartitionSpec
MESH = pl.DeviceIdType.MESH
epsilon = 1e-06
PIECES = 4
HALVES = 2
DIRECT = (4, 5, 8)
ORDER = (0, 1, 2, 3, 4, -4, 6, 5, -5, 7, 8, -8)
CUTS = ((0, 0, 8), (0, 8, 8), (1, 0, 8), (1, 8, 5), (1, 13, 3))
SLICES = 16
TABLE = HALVES


def layer_kernel(
    line,
    x_hbm,
    gate_b_hbm,
    gate_c_hbm,
    taps_hbm,
    resid_hbm,
    mix_hbm,
    pre_hbm,
    post_hbm,
    routes_hbm,
    weights_hbm,
    proj_ref,
    eg_ref,
    eu_ref,
    ed_ref,
    sg_ref,
    su_ref,
    sd_ref,
    out_ref,
    x_ref,
    gate_b_ref,
    gate_c_ref,
    taps_ref,
    resid_ref,
    mix_ref,
    pre_ref,
    post_ref,
    routes_ref,
    weights_ref,
    edge_x,
    edge_c,
    mixed,
    conv,
    conv_near,
    proj,
    part_out,
    part_in,
    projected,
    resid1,
    w_gate,
    w_up,
    w_down,
    s_gate,
    s_up,
    s_down,
    blocks,
    shares,
    hidden,
    shared_hidden,
    branch,
    outgoing,
    from_out,
    from_in,
    load_sem,
    edge_send,
    misc_send,
    spread_send,
    relay_send,
    in_send,
    out_send,
    e_recv,
    p_recv,
    c_recv,
    f_recv,
    wx_recv,
    wn_recv,
    wf_recv,
    wr_recv,
    gi_recv,
    go_recv,
    ri_recv,
    ro_recv,
):
    sp = lax.axis_index("sp")
    tp = lax.axis_index("tp")
    sp_size = lax.axis_size("sp")
    tp_size = lax.axis_size("tp")
    z = sp // 2
    x = sp % 2
    last = line - 1
    mate = z * 2 + 1 - x
    near = (tp // 2) * 2 + 1 - tp % 2
    far = (tp + 2) % tp_size
    near_far = (near + 2) % tp_size
    upper = z // (line // 2)
    inward_step = 1 - 2 * upper
    level = upper * last + inward_step * z
    inward = ((z + inward_step) * 2 + x, tp)
    outward = ((z - inward_step) * 2 + x, tp)

    def rel(k):
        return upper * last + inward_step * k

    rows, width = resid_ref.shape
    half_rows = rows // HALVES
    hid = w_gate.shape[2]
    shared_hid = s_gate.shape[1]
    part_cols = width // PIECES

    barrier = pltpu.get_barrier_semaphore()

    def greet(device):
        pl.semaphore_signal(barrier, inc=1, device_id=device, device_id_type=MESH)

    greet((mate, tp))
    greet((sp, near))
    greet((sp, far))

    @pl.when(z > 0)
    def _():
        greet((sp - 2, tp))

    @pl.when(z < last)
    def _():
        greet((sp + 2, tp))

    @pl.when((x == 1) & (z < last))
    def _():
        greet((sp + 1, tp))

    @pl.when((x == 0) & (z > 0))
    def _():
        greet((sp - 1, tp))

    pairs = (
        (x_hbm, x_ref),
        (gate_c_hbm, gate_c_ref),
        (proj_ref, proj.at[0]),
        (gate_b_hbm, gate_b_ref),
        (taps_hbm, taps_ref),
        (routes_hbm, routes_ref),
        (weights_hbm, weights_ref),
        (resid_hbm, resid_ref),
        (mix_hbm, mix_ref),
        (pre_hbm, pre_ref),
        (eg_ref.at[0], w_gate.at[0]),
        (eu_ref.at[0], w_up.at[0]),
        (sg_ref, s_gate),
        (su_ref, s_up),
        (ed_ref.at[0], w_down.at[pl.ds(0, hid)]),
        (sd_ref, s_down),
        (post_hbm, post_ref),
    )
    loads = [pltpu.make_async_copy(src, dst, load_sem.at[n]) for n, (src, dst) in enumerate(pairs)]
    for load in loads:
        load.start()

    all_rows, channels = x_ref.shape
    reach = taps_ref.shape[0] - 1
    pad = edge_x.shape[0]

    def edge_copy(n):
        source, landing = ((x_hbm, edge_x), (gate_c_hbm, edge_c))[n]
        return pltpu.make_async_remote_copy(
            src_ref=source.at[pl.ds(all_rows - pad, pad)],
            dst_ref=landing,
            send_sem=edge_send.at[0],
            recv_sem=e_recv.at[n],
            device_id=((sp + 1) % sp_size, tp),
            device_id_type=MESH,
        )

    def block_rows(owner):
        return pl.ds(pl.multiple_of(owner * rows, rows), rows)

    def conv_copy(n, k):
        begin, size = ((pad, rows - pad), (0, pad))[k]
        return pltpu.make_async_remote_copy(
            src_ref=conv.at[pl.ds(pl.multiple_of((near, near_far)[n] * rows + begin, pad), size)],
            dst_ref=conv_near.at[n, pl.ds(begin, size)],
            send_sem=misc_send.at[0],
            recv_sem=c_recv.at[n, k],
            device_id=(sp, near),
            device_id_type=MESH,
        )

    def chunk(j):
        return pl.ds(pl.multiple_of(j * part_cols, part_cols), part_cols)

    def half(r):
        return pl.ds(r * half_rows, half_rows)

    def proj_copy(j):
        return pltpu.make_async_remote_copy(
            src_ref=proj.at[0, :, chunk(j)],
            dst_ref=proj.at[1, :, chunk(j)],
            send_sem=misc_send.at[0],
            recv_sem=p_recv.at[j],
            device_id=(sp, near),
            device_id_type=MESH,
        )

    def part_copy(j):
        where = (pl.ds(pad, rows - pad), chunk(j))
        return pltpu.make_async_remote_copy(
            src_ref=part_out.at[where],
            dst_ref=part_in.at[where],
            send_sem=misc_send.at[0],
            recv_sem=f_recv.at[j],
            device_id=(sp, far),
            device_id_type=MESH,
        )

    part_head = pltpu.make_async_remote_copy(
        src_ref=part_out.at[pl.ds(0, pad)],
        dst_ref=part_in.at[pl.ds(0, pad)],
        send_sem=misc_send.at[0],
        recv_sem=f_recv.at[PIECES],
        device_id=(sp, far),
        device_id_type=MESH,
    )

    pieces = [((eg_ref, w_gate), (eu_ref, w_up))[k] + (first, size) for k, first, size in CUTS]
    for j in range(PIECES):
        pieces.append((ed_ref, w_down, j, 1))
    count = len(pieces)

    def cut(n, owner):
        ref, held, first, steps = pieces[n]
        if held is w_down:
            size = hid // tp_size
            begin = pl.multiple_of(owner * size, size)
            return (
                ref.at[0, pl.ds(begin, size), chunk(first)],
                held.at[pl.ds(pl.multiple_of(hid + begin, size), size), chunk(first)],
            )
        size = ref.shape[1] // tp_size // SLICES
        where = pl.ds(pl.multiple_of((owner * SLICES + first) * size, size), size * steps)
        return ref.at[0, where], held.at[1, where]

    def hop(n, owner, target, send, recv, first=False):
        source, landing = cut(n, owner)
        return pltpu.make_async_remote_copy(
            src_ref=source if first else landing,
            dst_ref=landing,
            send_sem=send.at[0],
            recv_sem=recv,
            device_id=target,
            device_id_type=MESH,
        )

    def late(n):
        return min(n // 2, 1) + max(0, n - len(CUTS) + 1)

    def x_hop(n):
        return hop(n, tp, (mate, tp), spread_send, wx_recv.at[n], True)

    def near_hop(n, owner):
        return hop(n, owner, (sp, near), spread_send, wn_recv.at[late(n)])

    def far_hop(n, owner):
        return hop(n, owner, (sp, far), relay_send, wf_recv.at[n])

    def direct_hop(n):
        return hop(n, far, (mate, tp), relay_send, wf_recv.at[n], True)

    def relay_hop(n, owner):
        return hop(n, owner, (sp, near), relay_send, wr_recv.at[late(n)])

    def drain(send, recv, size):
        where = w_down.at[pl.ds(0, size)]
        return pltpu.make_async_remote_copy(
            src_ref=where,
            dst_ref=where,
            send_sem=send.at[0],
            recv_sem=recv.at[0],
            device_id=(sp, near),
            device_id_type=MESH,
        )

    def spread(n):
        with jax.named_scope("w_x"):
            x_hop(n).wait_recv()
        if n not in DIRECT:
            far_hop(n, tp).start()
        near_hop(n, tp).start()

    def relay(n):
        with jax.named_scope("w_far"):
            far_hop(n, far).wait_recv()
        relay_hop(n, far).start()

    def ready(n):
        with jax.named_scope("w_ready"):
            near_hop(n, near).wait_recv()
            relay_hop(n, near_far).wait_recv()

    def ready_part(k):
        with jax.named_scope("w_ready"):
            drain(spread_send, wn_recv.at[pl.ds(k, 1)], hid // tp_size).wait_recv()
            drain(relay_send, wr_recv.at[pl.ds(k, 1)], hid // tp_size).wait_recv()

    def block_copy(b, r, target, send, recv):
        ref = shares.at[b] if r == TABLE else blocks.at[b, half(r)]
        return pltpu.make_async_remote_copy(
            src_ref=ref,
            dst_ref=ref,
            send_sem=send.at[0],
            recv_sem=recv,
            device_id=target,
            device_id_type=MESH,
        )

    def edge_in(r):
        return block_copy(rel(0), r, inward, in_send, go_recv.at[r])

    def mid_in(k, r):
        return block_copy(rel(k), r, inward, in_send, gi_recv.at[last - k - 1, r])

    def mid_out(k, r):
        return block_copy(rel(k), r, outward, out_send, gi_recv.at[k - 1, r])

    def got_in(k, r):
        with jax.named_scope("w_gi"):
            block_copy(rel(k), r, inward, in_send, gi_recv.at[k - 1, r]).wait_recv()

    def got_out(r):
        with jax.named_scope("w_go"):
            block_copy(rel(0), r, outward, out_send, go_recv.at[r]).wait_recv()

    def sum_copy(k, r, j, landing, target, send, recv):
        return pltpu.make_async_remote_copy(
            src_ref=outgoing.at[rel(k), half(r), chunk(j)],
            dst_ref=landing.at[rel(k), half(r), chunk(j)],
            send_sem=send.at[0],
            recv_sem=recv.at[j],
            device_id=target,
            device_id_type=MESH,
        )

    def edge_give(k, r, j):
        return sum_copy(k, r, j, from_out, inward, in_send, ro_recv.at[k - 1, r])

    def mid_give_in(k, r, j):
        return sum_copy(k, r, j, from_in, inward, in_send, ri_recv.at[last - k, r])

    def mid_give_out(k, r, j):
        return sum_copy(k, r, j, from_in, outward, out_send, ri_recv.at[k, r])

    def sum_in(k, r, j):
        with jax.named_scope("w_ri"):
            sum_copy(k, r, j, from_in, inward, in_send, ri_recv.at[k, r]).wait_recv()

    def sum_out(k, r, j):
        with jax.named_scope("w_ro"):
            sum_copy(k, r, j, from_out, outward, out_send, ro_recv.at[k - 1, r]).wait_recv()

    with jax.named_scope("w_barrier"):
        met = 3 + jnp.where(z > 0, 1, 0) + jnp.where(z < last, 1, 0)
        met += jnp.where(jnp.where(x == 1, z < last, z > 0), 1, 0)
        pl.semaphore_wait(barrier, met)

    @pl.when(sp < sp_size - 1)
    def _():
        edge_copy(0).start()
        edge_copy(1).start()

    for n in ORDER:
        if n < 0:
            direct_hop(-n).start()
        else:
            x_hop(n).start()

    for n in (0, 1, 3, 4):
        loads[n].wait()
    mixed[:pad] = jnp.zeros((pad, channels), jnp.float32)
    mixed[pad:] = x_ref[...].astype(jnp.float32) * gate_c_ref[...].astype(jnp.float32)

    def convolve(size):
        convolved = jnp.zeros((size, channels), jnp.float32)
        for k in range(reach + 1):
            begin = pad - reach + k
            convolved += taps_ref[k : k + 1].astype(jnp.float32) * mixed[begin : begin + size]
        conv[:size] = (gate_b_ref[:size].astype(jnp.float32) * convolved).astype(jnp.bfloat16)

    convolve(all_rows)
    conv_copy(1, 0).start()
    loads[2].wait()
    for j in range(PIECES):
        proj_copy(j).start()
    conv_copy(0, 0).start()
    loads[5].wait()
    loads[6].wait()
    lanes = lax.broadcasted_iota(jnp.int32, (rows, shares.shape[2]), 1)
    names = lax.broadcasted_iota(jnp.int32, (shares.shape[2], rows), 0)
    table = jnp.zeros((shares.shape[2], rows), jnp.float32)
    for k in range(routes_ref.shape[0]):
        table += jnp.where(names == routes_ref[k : k + 1], weights_ref[k : k + 1], 0.0)
    own = z
    shares[own] = table.T

    def send_own(r):
        @pl.when(level == 0)
        def _():
            edge_in(r).start()

        @pl.when(level == 1)
        def _():
            if r != HALVES - 1:
                mid_in(1, r).start()
            mid_out(1, r).start()

    send_own(TABLE)

    def project(n, owner, cols, begin, size):
        mine = pl.ds(pl.multiple_of(owner * rows + begin, pad), size)
        return jnp.dot(
            conv[mine], proj[0, :, cols], preferred_element_type=jnp.float32
        ) + jnp.dot(
            conv_near[n, begin : begin + size], proj[1, :, cols], preferred_element_type=jnp.float32
        )

    with jax.named_scope("w_conv"):
        conv_copy(1, 0).wait_recv()

    @pl.loop(0, PIECES)
    def _(j):
        proj_copy(j).wait_recv()
        part_out[pad:, chunk(j)] = project(1, far, chunk(j), pad, rows - pad).astype(jnp.bfloat16)
        part_copy(j).start()

    with jax.named_scope("w_edge"):

        @pl.when(sp > 0)
        def _():
            edge_copy(0).wait_recv()
            edge_copy(1).wait_recv()
            mixed[:pad] = edge_x[...].astype(jnp.float32) * edge_c[...].astype(jnp.float32)

    convolve(pad)
    conv_copy(1, 1).start()
    conv_copy(0, 1).start()
    with jax.named_scope("w_head"):
        conv_copy(1, 1).wait_recv()

    @pl.loop(0, PIECES)
    def _(j):
        part_out[:pad, chunk(j)] = project(1, far, chunk(j), 0, pad).astype(jnp.bfloat16)

    part_head.start()
    conv_copy(0, 0).wait_recv()
    conv_copy(0, 1).wait_recv()

    @pl.loop(0, PIECES)
    def _(j):
        projected[:, chunk(j)] = project(0, tp, chunk(j), 0, rows)

    spread(0)
    spread(1)
    for load in loads[7:10]:
        load.wait()

    with jax.named_scope("w_part"):

        @pl.loop(0, PIECES)
        def _(j):
            part_copy(j).wait_recv()
            projected[pad:, chunk(j)] += part_in[pad:, chunk(j)].astype(jnp.float32)

        part_head.wait_recv()
        projected[:pad] += part_in[:pad].astype(jnp.float32)

    with jax.named_scope("norm"):
        for r in range(HALVES):
            part = half(r)
            block = projected[part]
            scale = lax.rsqrt(jnp.mean(block * block, axis=1, keepdims=True) + epsilon)
            mid = (
                resid_ref[part].astype(jnp.float32)
                + block * scale * mix_ref[...].astype(jnp.float32).reshape(1, width)
            ).astype(jnp.bfloat16)
            resid1[part] = mid
            wide = mid.astype(jnp.float32)
            normal = lax.rsqrt(jnp.mean(wide * wide, axis=1, keepdims=True) + epsilon)
            blocks[own, part] = (
                wide * normal * pre_ref[...].astype(jnp.float32).reshape(1, width)
            ).astype(jnp.bfloat16)

            send_own(r)

    spread(2)

    def hide(b, begin, size, e):
        part = pl.ds(begin, size)
        expert = z * 2 + x + e * (1 - 2 * x)
        share = jnp.sum(
            jnp.where(lanes[:size] == expert, shares[b, part], 0.0), axis=1, keepdims=True
        )

        def step(j):
            cols = pl.ds(pl.multiple_of(j * 256, 256), 256)
            gate = jnp.dot(blocks[b, part], w_gate[e, :, cols], preferred_element_type=jnp.float32)
            up = jnp.dot(blocks[b, part], w_up[e, :, cols], preferred_element_type=jnp.float32)
            kept = pl.ds(pl.multiple_of(e * hid + j * 256, 256), 256)
            hidden[b, part, kept] = (jax.nn.silu(gate) * up * share).astype(jnp.bfloat16)

        if size < rows:
            for j in range(hid // 256):
                step(j)
        else:
            pl.loop(0, hid // 256)(step)

    def share_of(b, e):
        expert = z * 2 + x + e * (1 - 2 * x)
        return jnp.sum(jnp.where(lanes == expert, shares[b], 0.0), axis=1, keepdims=True)

    def gate_ahead(b):
        share = share_of(b, 1)

        @pl.loop(0, hid // 256)
        def _(j):
            cols = pl.ds(pl.multiple_of(j * 256, 256), 256)
            gate = jnp.dot(blocks[b], w_gate[1, :, cols], preferred_element_type=jnp.float32)
            projected[:, cols] = jax.nn.silu(gate) * share

    def up_after(b):
        for j in range(hid // 256):
            cols = pl.ds(j * 256, 256)
            up = jnp.dot(blocks[b], w_up[1, :, cols], preferred_element_type=jnp.float32)
            kept = pl.ds(hid + j * 256, 256)
            hidden[b, :, kept] = (projected[:, cols] * up).astype(jnp.bfloat16)

    def hide_all(b, e):
        hide(b, 0, rows, e)

    def hide_half(b, r):
        hide(b, r * half_rows, half_rows, 0)
        hide(b, r * half_rows, half_rows, 1)

    def down(b, part, j):
        return jnp.dot(
            hidden[b, part], w_down[:, chunk(j)], preferred_element_type=jnp.float32
        )

    def give(k, r, j, arrived, send, landed=None):
        made = down(rel(k), half(r), j)
        if arrived is not None:
            landed(k, r, j)
            made += arrived[rel(k), half(r), chunk(j)].astype(jnp.float32)
        outgoing[rel(k), half(r), chunk(j)] = made.astype(jnp.bfloat16)
        send(k, r, j).start()

    def shared_up_to_hidden():
        s_g = jnp.dot(blocks[own], s_gate[...], preferred_element_type=jnp.float32)
        s_u = jnp.dot(blocks[own], s_up[...], preferred_element_type=jnp.float32)
        shared_hidden[...] = (jax.nn.silu(s_g) * s_u).astype(jnp.bfloat16)

    def own_branch():
        @pl.loop(0, PIECES)
        def _(j):
            branch[:, chunk(j)] = down(own, pl.ds(0, rows), j) + jnp.dot(
                shared_hidden[...], s_down[:, chunk(j)], preferred_element_type=jnp.float32
            )

    def yield_out(r, total):
        factor = lax.rsqrt(jnp.mean(total * total, axis=1, keepdims=True) + epsilon)
        out_ref[half(r)] = (
            resid1[half(r)].astype(jnp.float32)
            + total * factor * post_ref[...].astype(jnp.float32).reshape(1, width)
        ).astype(jnp.bfloat16)

    def settle():
        @pl.when(sp < sp_size - 1)
        def _():
            drain(edge_send, e_recv, 2 * pad * channels // width).wait_send()

        drain(misc_send, e_recv, channels + 2 * rows * channels // width + rows).wait_send()
        drain(spread_send, e_recv, 2 * 3 * hid // tp_size).wait_send()
        drain(relay_send, e_recv, 2 * 3 * hid // tp_size).wait_send()

    sent_block = rows + 2 * rows * shares.shape[2] // width
    sent_sums = rows

    for load in loads[10:14]:
        load.wait()
    hide_all(own, 0)
    shared_up_to_hidden()
    relay(0)
    spread(3)
    for load in loads[14:]:
        load.wait()

    @pl.when(level == 0)
    def _():
        got_in(1, TABLE)
        got_in(1, 0)
        hide(rel(1), 0, half_rows, 0)
        spread(4)
        relay(1)
        relay(4)
        spread(6)
        got_in(1, 1)
        hide(rel(1), half_rows, half_rows, 0)
        relay(2)
        ready_part(0)
        gate_ahead(rel(1))
        spread(5)
        relay(3)
        relay(5)
        ready_part(1)
        up_after(rel(1))
        ready(5)
        for r in range(HALVES):
            give(1, r, 0, None, edge_give)
        relay(6)
        spread(7)
        ready(6)
        for r in range(HALVES):
            give(1, r, 1, None, edge_give)
        got_in(2, TABLE)
        got_in(2, 0)
        hide_half(rel(2), 0)

        @pl.loop(0, 2)
        def _(j):
            give(2, 0, j, None, edge_give)

        spread(8)
        relay(7)
        relay(8)
        got_in(3, TABLE)
        got_in(3, 0)
        hide_half(rel(3), 0)

        @pl.loop(0, 2)
        def _(j):
            give(3, 0, j, None, edge_give)

        ready(7)
        ready(8)

        @pl.loop(2, PIECES)
        def _(j):
            give(3, 0, j, None, edge_give)

        got_in(3, 1)
        hide_half(rel(3), 1)

        @pl.loop(0, PIECES)
        def _(j):
            give(3, 1, j, None, edge_give)

        @pl.loop(2, PIECES)
        def _(j):
            give(2, 0, j, None, edge_give)

        hide_all(own, 1)
        got_in(2, 1)
        hide_half(rel(2), 1)

        @pl.loop(0, PIECES)
        def _(j):
            give(2, 1, j, None, edge_give)

        @pl.loop(2, PIECES)
        def _(j):
            for r in range(HALVES):
                give(1, r, j, None, edge_give)

        own_branch()
        settle()
        for r in range(HALVES):

            @pl.loop(0, PIECES)
            def _(j):
                sum_in(0, r, j)

            total = branch[half(r)] + from_in[own, half(r)].astype(jnp.float32)
            yield_out(r, total)

        drain(in_send, e_recv, sent_block + 3 * sent_sums).wait_send()

    @pl.when(level == 1)
    def _():
        def pass_in(r):
            got_out(r)
            mid_in(0, r).start()

        def pass_out(k, r):
            got_in(k, r)
            mid_out(k, r).start()

        pass_in(TABLE)
        pass_out(2, TABLE)
        pass_in(0)
        pass_out(2, 0)
        pass_out(3, TABLE)
        spread(4)
        relay(1)
        relay(4)
        spread(6)
        pass_in(1)
        mid_in(1, HALVES - 1).start()
        pass_out(3, 0)
        hide_all(rel(0), 0)
        relay(2)
        spread(5)
        relay(3)
        relay(5)
        ready_part(0)
        ready_part(1)
        hide_half(rel(2), 0)
        relay(6)
        spread(7)
        pass_out(3, 1)
        hide_all(own, 1)
        spread(8)
        hide_all(rel(3), 0)
        relay(7)
        relay(8)
        hide_all(rel(3), 1)
        pass_out(2, 1)
        hide_half(rel(2), 1)
        hide_all(rel(0), 1)
        for n in range(len(CUTS), count):
            ready(n)

        def give_in(k, r, j):
            give(k, r, j, from_out, mid_give_in, sum_out)

        def give_out(r, j):
            give(0, r, j, from_in, mid_give_out, sum_in)

        @pl.loop(0, 2)
        def _(j):
            give_in(2, 0, j)

        own_branch()

        @pl.loop(0, PIECES)
        def _(j):
            give_in(3, 0, j)

        settle()

        @pl.loop(0, PIECES)
        def _(j):
            give_out(0, j)
            give_in(3, 1, j)

        @pl.loop(0, 2)
        def _(j):
            give_out(1, j)

        @pl.loop(2, PIECES)
        def _(j):
            give_in(2, 0, j)
            give_out(1, j)

        @pl.loop(0, PIECES)
        def _(j):
            give_in(2, 1, j)

        for r in range(HALVES):

            @pl.loop(0, PIECES)
            def _(j):
                sum_in(1, r, j)
                sum_out(1, r, j)

            total = (
                branch[half(r)]
                + from_in[own, half(r)].astype(jnp.float32)
                + from_out[own, half(r)].astype(jnp.float32)
            )
            yield_out(r, total)

        drain(in_send, e_recv, 2 * sent_block + 2 * sent_sums).wait_send()
        drain(out_send, e_recv, 3 * sent_block + sent_sums).wait_send()


def fused_layer(
    x_in, gate_b, gate_c, conv_taps, out_proj, mix_gain, resid, pre_gain, expert_gate, expert_up,
    expert_down, shared_gate, shared_up, shared_down, post_gain, routes, route_weights,
):
    experts = lax.axis_size("sp")
    line = experts // 2
    all_rows, channels = x_in.shape
    rows, width = resid.shape
    hid = expert_gate.shape[2]
    shared_hid = shared_gate.shape[1]
    dma = pltpu.SemaphoreType.DMA
    count = len(CUTS) + PIECES
    bf, f32 = jnp.bfloat16, jnp.float32
    hbm = pl.BlockSpec(memory_space=pltpu.HBM)
    lanes = 128 * (-(-experts // 128))
    pad = 16 * (-(-(conv_taps.shape[0] - 1) // 16))
    top = routes.shape[1]
    return pl.pallas_call(
        functools.partial(layer_kernel, line),
        out_shape=jax.ShapeDtypeStruct((rows, width), bf),
        in_specs=[hbm] * 17,
        out_specs=pl.BlockSpec(memory_space=pltpu.VMEM),
        scratch_shapes=[
            pltpu.VMEM((all_rows, channels), bf),
            pltpu.VMEM((all_rows, channels), bf),
            pltpu.VMEM((all_rows, channels), bf),
            pltpu.VMEM(conv_taps.shape, bf),
            pltpu.VMEM((rows, width), bf),
            pltpu.VMEM((width,), bf),
            pltpu.VMEM((width,), bf),
            pltpu.VMEM((width,), bf),
            pltpu.VMEM((top, rows), jnp.int32),
            pltpu.VMEM((top, rows), f32),
            pltpu.VMEM((pad, channels), bf),
            pltpu.VMEM((pad, channels), bf),
            pltpu.VMEM((pad + all_rows, channels), f32),
            pltpu.VMEM((all_rows, channels), bf),
            pltpu.VMEM((2, rows, channels), bf),
            pltpu.VMEM((2, channels, width), bf),
            pltpu.VMEM((rows, width), bf),
            pltpu.VMEM((rows, width), bf),
            pltpu.VMEM((rows, width), f32),
            pltpu.VMEM((rows, width), bf),
            pltpu.VMEM((2, width, hid), bf),
            pltpu.VMEM((2, width, hid), bf),
            pltpu.VMEM((2 * hid, width), bf),
            pltpu.VMEM((width, shared_hid), bf),
            pltpu.VMEM((width, shared_hid), bf),
            pltpu.VMEM((shared_hid, width), bf),
            pltpu.VMEM((line, rows, width), bf),
            pltpu.VMEM((line, rows, lanes), f32),
            pltpu.VMEM((line, rows, 2 * hid), bf),
            pltpu.VMEM((rows, shared_hid), bf),
            pltpu.VMEM((rows, width), f32),
            pltpu.VMEM((line, rows, width), bf),
            pltpu.VMEM((line, rows, width), bf),
            pltpu.VMEM((line, rows, width), bf),
            dma((17,)),
        ]
        + [dma((1,))] * 6
        + [
            dma((2,)),
            dma((PIECES,)),
            dma((2, 2)),
            dma((PIECES + 1,)),
            dma((count,)),
            dma((2 + PIECES,)),
            dma((count,)),
            dma((2 + PIECES,)),
            dma((line - 1, HALVES + 1)),
            dma((HALVES + 1,)),
            dma((2, HALVES, PIECES)),
            dma((line - 1, HALVES, PIECES)),
        ],
        compiler_params=pltpu.CompilerParams(
            collective_id=0, has_side_effects=True, vmem_limit_bytes=46 * 1024 * 1024
        ),
    )(
        *(
            pltpu.with_memory_space_constraint(ref, pltpu.HBM)
            for ref in (
                x_in, gate_b, gate_c, conv_taps, resid, mix_gain, pre_gain, post_gain,
                routes.T, route_weights.T, out_proj, expert_gate, expert_up, expert_down,
                shared_gate, shared_up, shared_down,
            )
        )
    )


def passed_along(shard, axis, by):
    size = lax.axis_size(axis)
    pairs = [(i, i + by) for i in range(size) if 0 <= i + by < size]
    return lax.ppermute(shard, axis, pairs)


def body(
    x_in,
    gate_b,
    gate_c,
    conv_taps,
    out_proj,
    mix_gain,
    resid,
    pre_gain,
    expert_gate,
    expert_up,
    expert_down,
    shared_gate,
    shared_up,
    shared_down,
    post_gain,
    routes,
    route_weights,
):
    group = lax.axis_size("sp")
    wide_slots = 3 * resid.shape[0] * routes.shape[1] // group
    if wide_slots > resid.shape[0] and group == 2 * 2 * 2 and lax.axis_size("tp") == 2 * 2:
        return fused_layer(
            x_in, gate_b, gate_c, conv_taps, out_proj, mix_gain, resid, pre_gain, expert_gate,
            expert_up, expert_down, shared_gate, shared_up, shared_down, post_gain, routes,
            route_weights,
        )
    row_count = x_in.shape[0]
    channels = x_in.shape[1]
    reach = conv_taps.shape[0] - 1
    edge_rows = jnp.concatenate([x_in[row_count - reach :], gate_c[row_count - reach :]], 1)
    arrived_edge = passed_along(edge_rows, "sp", 1)
    inputs = jnp.concatenate([arrived_edge[:, :channels], x_in], 0).astype(jnp.float32)
    gate_rows = jnp.concatenate([arrived_edge[:, channels:], gate_c], 0).astype(jnp.float32)
    mixed_in = inputs * gate_rows
    taps = conv_taps.astype(jnp.float32)
    convolved = jnp.zeros((row_count, channels), jnp.float32)
    for index in range(reach + 1):
        convolved = convolved + taps[index][None, :] * mixed_in[index : index + row_count]
    conv_out = (gate_b.astype(jnp.float32) * convolved).astype(jnp.bfloat16)
    width_all = out_proj.shape[1]
    full_rows = lax.all_to_all(conv_out, "tp", split_axis=0, concat_axis=1, tiled=True)
    projected = jnp.dot(
        full_rows,
        lax.all_gather(out_proj, "tp", axis=0, tiled=True),
        preferred_element_type=jnp.float32,
    )
    row_scale = lax.rsqrt(jnp.mean(projected * projected, axis=1, keepdims=True) + epsilon)
    resid1 = (
        resid.astype(jnp.float32) + projected * row_scale * mix_gain.astype(jnp.float32)
    ).astype(jnp.bfloat16)
    wide_resid = resid1.astype(jnp.float32)
    normed = (
        wide_resid
        * lax.rsqrt(jnp.mean(wide_resid * wide_resid, axis=1, keepdims=True) + epsilon)
        * pre_gain.astype(jnp.float32)
    ).astype(jnp.bfloat16)
    experts = lax.axis_size("sp")
    local_rows = resid.shape[0]
    top_count = routes.shape[1]
    capacity = 3 * local_rows * top_count // (2 * experts)
    flat_ids = routes.reshape(-1)
    onehot = (flat_ids[:, None] == jnp.arange(experts, dtype=jnp.int32)[None, :]).astype(jnp.int32)
    before = jnp.cumsum(onehot, axis=0) - onehot
    position = jnp.sum(before * onehot, axis=1)
    slot_index = flat_ids * capacity + position
    outgoing = (
        jnp.zeros((experts * capacity, width_all), jnp.bfloat16)
        .at[slot_index]
        .set(jnp.repeat(normed, top_count, axis=0))
    )
    received = lax.all_to_all(
        outgoing.reshape(experts, capacity, width_all),
        "sp",
        split_axis=0,
        concat_axis=0,
        tiled=True,
    )
    arrived = received.reshape(experts * capacity, width_all)
    gate_h = jnp.dot(arrived, expert_gate[0], preferred_element_type=jnp.float32)
    up_h = jnp.dot(arrived, expert_up[0], preferred_element_type=jnp.float32)
    hidden = (jax.nn.silu(gate_h) * up_h).astype(jnp.bfloat16)
    expert_out = jnp.dot(hidden, expert_down[0], preferred_element_type=jnp.float32).astype(
        jnp.bfloat16
    )
    returned = lax.all_to_all(
        expert_out.reshape(experts, capacity, width_all),
        "sp",
        split_axis=0,
        concat_axis=0,
        tiled=True,
    )
    returned = returned.reshape(experts * capacity, width_all)
    picked = returned[slot_index].astype(jnp.float32).reshape(local_rows, top_count, width_all)
    routed = jnp.einsum("tk,tkd->td", route_weights, picked)
    shared_g = jnp.dot(normed, shared_gate, preferred_element_type=jnp.float32)
    shared_u = jnp.dot(normed, shared_up, preferred_element_type=jnp.float32)
    shared_hidden = (jax.nn.silu(shared_g) * shared_u).astype(jnp.bfloat16)
    shared_out = jnp.dot(shared_hidden, shared_down, preferred_element_type=jnp.float32)
    branch = routed + shared_out
    factor = lax.rsqrt(jnp.mean(branch * branch, axis=1, keepdims=True) + epsilon)
    return (wide_resid + branch * factor * post_gain.astype(jnp.float32)[None, :]).astype(
        jnp.bfloat16
    )


def solution(mesh):
    return jax.shard_map(
        body,
        mesh=mesh,
        in_specs=(
            P("sp", "tp"),
            P("sp", "tp"),
            P("sp", "tp"),
            P(None, "tp"),
            P("tp", None),
            P(),
            P(("sp", "tp"), None),
            P(),
            P("sp", None, None),
            P("sp", None, None),
            P("sp", None, None),
            P(),
            P(),
            P(),
            P(),
            P(("sp", "tp"), None),
            P(("sp", "tp"), None),
        ),
        out_specs=P(("sp", "tp"), None),
        check_vma=False,
    )
```
